256 devices in a mesh: kv: 32 (over z, y), tp: 8 (over x, core).
Axes of the slice: x: 4, y: 4, z: 8, core: 2. Of those that a mesh axis runs over, the one named last changes fastest.
Arguments:
- tokens: bfloat16 [16, 4096], P(None, 'tp'), may hold values from -6 to 6
- norm_gain: float32 [4096], P('tp'), may hold values from 0.1 to 1.9
- w_query: bfloat16 [4096, 32, 96], P('tp', 'kv'), as said below
- w_latent: bfloat16 [4096, 1024], P('tp', 'kv'), may hold values from -0.09375 to 0.09375
- w_rotary: bfloat16 [4096, 32], P('tp'), may hold values from -0.09375 to 0.09375
- latent_gain: float32 [1024], replicated, may hold values from 0.1 to 1.9
- w_key_up: bfloat16 [1024, 32, 64], P('tp', 'kv'), may hold values from -0.1875 to 0.1875
- w_value_up: bfloat16 [1024, 32, 128], replicated, may hold values from -0.1875 to 0.1875
- w_out: bfloat16 [4096, 4096], P('kv', 'tp'), may hold values from -0.09375 to 0.09375
- cache_latent: bfloat16 [16, 32768, 1024], P(None, ('kv', 'tp')), may hold values from -6 to 6
- cache_rotary: bfloat16 [16, 32768, 32], P(None, ('kv', 'tp')), may hold values from -6 to 6
- lengths: int32 [16], replicated, may hold values from 8192 to 32768
Outputs:
- mixed_out: bfloat16 [16, 4096], P(None, 'tp')
- new_latent: bfloat16 [16, 1024], P(None, ('kv', 'tp'))
- new_rotary: bfloat16 [16, 32], replicated
The draws below stay inside these ranges and needn't reach their ends.
Inputs may be any that keep to these rules, and one draw needn't show every extreme that they name: `w_query`: finite.
All inputs are finite; a program needn't handle non-finite values.
Results may differ from the reference program's by a relative error of at most 0.012.
The reference program's roundings to bfloat16 on the way count: a program that leaves them out, or rounds other values in their place, can miss the bound.
Values may be sent and summed in bfloat16 or wider, within the bound.
No kernel may reach another device: no remote copies, remote signals or barrier semaphores. Data moves between devices by JAX's collectives and lax.ppermute only.
A program may use at most 64 MiB of HBM per device.

```python
import jax
import jax.numpy as jnp
from jax import lax

D = 4096
HEADS = 32
NOPE = 64
ROPE = 32
VH = 128
LATENT = 1024
SEQS = 16
CACHE = 32768


def draw_w_query(key, part):
    base_key = jax.random.fold_in(key, 11)
    pick_key = jax.random.fold_in(key, 12)
    order = jax.random.permutation(pick_key, HEADS)
    values = jax.random.truncated_normal(base_key, -6.0, 6.0, (D, HEADS, NOPE + ROPE), jnp.float32) * D ** (-0.5)
    strengths = jnp.array([30.0, 60.0], jnp.float32)
    factor = jnp.full((HEADS,), 5.0, jnp.float32)
    factor = factor.at[order[:strengths.shape[0]]].set(strengths)
    return (values * factor[None, :, None]).astype(jnp.bfloat16)


def touch_ends(result, key, smallest, high):
    longest = result.shape.index(max(result.shape))
    spots = []
    for shift in (0, 1):
        where = [jax.random.randint(jax.random.fold_in(key, axis), (), 0, length) for axis, length in enumerate(result.shape)]
        where[longest] = (where[longest] + shift) % result.shape[longest]
        spots.append(tuple(where))
    return result.at[spots[0]].set(smallest).at[spots[1]].set(high)


def block_levels(rng, dims, split, low, largest):
    def one(dim, shards_of):
        heights = jax.random.uniform(jax.random.fold_in(jax.random.fold_in(rng, 6), dim), (shards_of,), jnp.float32, low / len(split), largest / len(split))
        return jnp.repeat(jnp.exp(heights), dims[dim] // shards_of).reshape((-1,) + (1,) * (len(dims) - dim - 1))

    level = one(*split[0])
    for cut in split[1:]:
        level = level * one(*cut)
    return level


def gaussian(key, shape, spread, bound, shards=(), kind=jnp.bfloat16):
    result = jax.random.normal(key, shape, jnp.float32) * spread
    if len(shards) > 0:
        result = block_levels(key, shape, shards, -0.22, 0.18) * result
    return jnp.clip(result, min=-bound, max=bound).astype(kind)


def setup_inputs(seed: int = 0) -> dict:
    splits = jax.random.split(jax.random.key(seed), 13)
    return {
        "tokens": gaussian(splits[0], (SEQS, D), 1.0, 6.0, ((1, 8),)),
        "norm_gain": jnp.clip(1.0 + 0.18 * jax.random.normal(splits[1], (D,), jnp.float32), 0.1, 1.9),
        "w_query": draw_w_query(jax.random.fold_in(splits[12], 71), 0),
        "w_latent": gaussian(splits[3], (D, LATENT), D ** -0.5, 0.09375, ((0, 8), (1, 32))),
        "w_rotary": gaussian(splits[4], (D, ROPE), D ** -0.5, 0.09375, ((0, 8),)),
        "latent_gain": jnp.clip(1.0 + 0.18 * jax.random.normal(splits[5], (LATENT,), jnp.float32), 0.1, 1.9),
        "w_key_up": gaussian(splits[6], (LATENT, HEADS, NOPE), LATENT ** -0.5, 0.1875, ((0, 8), (1, 32))),
        "w_value_up": gaussian(splits[7], (LATENT, HEADS, VH), LATENT ** -0.5, 0.1875),
        "w_out": gaussian(splits[8], (HEADS * VH, D), (HEADS * VH) ** -0.5, 0.09375, ((0, 32), (1, 8))),
        "cache_latent": gaussian(splits[9], (SEQS, CACHE, LATENT), 1.0, 6.0, ((1, 256),)),
        "cache_rotary": gaussian(splits[10], (SEQS, CACHE, ROPE), 1.0, 6.0, ((1, 256),)),
        "lengths": touch_ends(jax.random.randint(splits[11], (SEQS,), CACHE // 4, CACHE + 1), jax.random.fold_in(splits[11], 1), CACHE // 4, CACHE).astype(jnp.int32),
    }


THETA = 10000.0
EPS = 1e-06

def rotate(values, position):
    full_width = values.shape[-1]
    half_width = full_width // 2
    frequency = THETA ** (-jnp.arange(0, full_width, 2, dtype=jnp.float32) / full_width)
    angles = position.astype(jnp.float32)[:, None] * frequency[None, :]
    angles = angles.reshape((angles.shape[0],) + (1,) * (values.ndim - 2) + (half_width,))
    cosine = jnp.cos(angles)
    sine_part = jnp.sin(angles)
    first_half = values[..., :half_width]
    second_half = values[..., half_width:]
    return jnp.concatenate([first_half * cosine - second_half * sine_part, first_half * sine_part + second_half * cosine], axis=-1)

def reference(tokens, norm_gain, w_query, w_latent, w_rotary, latent_gain, w_key_up, w_value_up, w_out, cache_latent, cache_rotary, lengths):
    tokens_f = tokens.astype(jnp.float32)
    scaled = (tokens_f * norm_gain).astype(jnp.bfloat16)
    inverse = lax.rsqrt(lax.optimization_barrier(jnp.mean(tokens_f * tokens_f, axis=1)) + EPS)
    query_sum = jnp.einsum('bd,dhn->bhn', scaled.astype(jnp.float32), w_query.astype(jnp.float32))
    latent_sum = jnp.dot(scaled, w_latent, preferred_element_type=jnp.float32)
    rotary_sum = jnp.dot(scaled, w_rotary, preferred_element_type=jnp.float32)
    query_heads = (query_sum * inverse[:, None, None]).astype(jnp.bfloat16)
    compressed = (latent_sum * inverse[:, None]).astype(jnp.bfloat16)
    new_rotary = rotate(rotary_sum * inverse[:, None], lengths).astype(jnp.bfloat16)
    query_rope = rotate(query_heads[:, :, NOPE:].astype(jnp.float32), lengths).astype(jnp.bfloat16)
    query_latent = jnp.einsum('bhn,rhn->bhr', query_heads[:, :, :NOPE].astype(jnp.float32), w_key_up.astype(jnp.float32)).astype(jnp.bfloat16)
    compressed_f = compressed.astype(jnp.float32)
    new_latent = (compressed_f * lax.rsqrt(lax.optimization_barrier(jnp.mean(compressed_f * compressed_f, axis=1, keepdims=True)) + EPS) * latent_gain).astype(jnp.bfloat16)
    score_scale = (NOPE + ROPE) ** (-0.5)
    own_score = (jnp.einsum('bhr,br->bh', query_latent.astype(jnp.float32), new_latent.astype(jnp.float32)) + jnp.einsum('bhq,bq->bh', query_rope.astype(jnp.float32), new_rotary.astype(jnp.float32))) * score_scale

    def attend(items):
        latent_query, rope_query, past_latent, past_rotary, length, own, fresh = items
        scores = (jnp.dot(latent_query, past_latent.T, preferred_element_type=jnp.float32) + jnp.dot(rope_query, past_rotary.T, preferred_element_type=jnp.float32)) * score_scale
        valid = jnp.arange(CACHE, dtype=jnp.int32) < length
        masked = jnp.where(valid[None, :], scores, -jnp.inf)
        top_score = jnp.maximum(lax.optimization_barrier(jnp.max(masked, axis=1)), own)
        weights = jnp.where(valid[None, :], jnp.exp(scores - top_score[:, None]), 0.0)
        own_weight = jnp.exp(own - top_score)
        total = lax.optimization_barrier(jnp.sum(weights, axis=1)) + own_weight
        summed = jnp.dot(weights.astype(jnp.bfloat16), past_latent, preferred_element_type=jnp.float32)
        summed = summed + own_weight[:, None] * fresh.astype(jnp.float32)[None, :]
        return summed / total[:, None]
    latent_out = lax.map(attend, (query_latent, query_rope, cache_latent, cache_rotary, lengths, own_score, new_latent))
    head_out = jnp.einsum('bhr,rhv->bhv', latent_out, w_value_up.astype(jnp.float32), precision=lax.Precision.HIGHEST).astype(jnp.bfloat16)
    mixed_out = jnp.dot(head_out.reshape(head_out.shape[0], -1), w_out, preferred_element_type=jnp.float32).astype(jnp.bfloat16)
    return (mixed_out, new_latent, new_rotary)
```

```python
import functools

import jax
import jax.numpy as jnp
from jax import lax
from jax.experimental import pallas as pl
from jax.experimental.pallas import tpu as pltpu
from jax.sharding import Mesh
from jax.sharding import PartitionSpec as P

KV = ("kv_0", "kv_1")
TP = ("tp_0", "tp_1")
KV_TP = ("kv_0", "kv_1", "tp_0", "tp_1")


THETA = 10000.0
EPS = 1e-06
F32 = jnp.float32
BF16 = jnp.bfloat16
FLOOR = -(2.0**127)
LANES = 128


def whole(count):
    return [pl.BlockSpec(memory_space=pltpu.VMEM)] * count


def lane_ids(rows):
    return lax.broadcasted_iota(jnp.int32, (rows, LANES), 1)


def swapped(value, axis, step):
    count = lax.axis_size(axis)
    return lax.ppermute(value, axis, [(i, i ^ step) for i in range(count)])


def project_kernel(tokens_ref, gain_ref, query_ref, latent_ref, rotary_ref, out_ref):
    tokens = tokens_ref[...].astype(F32)
    scaled = (tokens * gain_ref[...]).astype(BF16)
    squares = jnp.sum(tokens * tokens, axis=1, keepdims=True)
    query = jnp.dot(scaled, query_ref[...], preferred_element_type=F32)
    latent = jnp.dot(scaled, latent_ref[...], preferred_element_type=F32)
    rotary = jnp.dot(scaled, rotary_ref[...], preferred_element_type=F32)
    out_ref[0:16, 0:96] = query
    out_ref[0:16, 96:128] = latent
    out_ref[16:32, :] = jnp.broadcast_to(squares, (16, LANES))
    out_ref[16:32, 0:32] = rotary


def query_kernel(
    model_width, a_ref, b_ref, c_ref, d_ref, cos_ref, left_ref, right_ref, key_ref,
    block_ref, rotary_ref, slice_ref, dot_ref,
):
    total = (a_ref[...] + b_ref[...]) + (c_ref[...] + d_ref[...])
    lane = lane_ids(16)
    first, second = total[0:16], total[16:32]
    squares = jnp.sum(jnp.where(lane == 64, second, 0.0), axis=1, keepdims=True)
    inverse = lax.rsqrt(squares / model_width + EPS)

    def rotated(v):
        return (
            v * cos_ref[...]
            + pltpu.roll(v, LANES - 16, 1) * left_ref[...]
            + pltpu.roll(v, 16, 1) * right_ref[...]
        )

    query = (first * inverse).astype(BF16)
    query_f = query.astype(F32)
    rope = rotated(query_f)
    fresh = rotated(second * inverse).astype(BF16)
    latent_query = lax.dot_general(
        query[:, 0:64], key_ref[...], (((1,), (1,)), ((), ())), preferred_element_type=F32
    ).astype(BF16)
    side = jnp.where(lane < 96, rope, query_f)
    side = pltpu.roll(jnp.where(lane < 64, 0.0, side), 64, 1).astype(BF16)
    for peer in range(block_ref.shape[0]):
        block_ref[peer, 0:16, :] = latent_query
        block_ref[peer, 16:32, :] = side
    rotary_ref[...] = fresh[:, 0:32]
    slice_ref[...] = latent_query.astype(F32)
    both = jnp.where(lane < 32, side.astype(F32) * fresh.astype(F32), 0.0)
    dot_ref[...] = jnp.broadcast_to(jnp.sum(both, axis=1, keepdims=True), (16, LANES))


def attend_kernel(scale, info_ref, *refs):
    pieces = refs[0:8]
    (side_ref, fresh_ref, rot_ref, cache_hbm, value_hbm, out_ref, own_ref) = refs[8:15]
    (q_s, r_s, cache_s, value_s, valuef_s, o_s, m_s, l_s, cache_sem, value_sem) = refs[15:]
    seqs, heads = 16, 32
    chunks = cache_sem.shape[0]
    per = seqs // chunks
    depth = value_s.shape[0]
    part = depth // chunks
    pairs, blocks = seqs * heads, depth // LANES

    def cache_copy(i):
        rows = pl.ds(i * per, per)
        return pltpu.make_async_copy(cache_hbm.at[rows], cache_s.at[rows], cache_sem.at[i])

    def value_copy(i):
        rows = pl.ds(i * part, part)
        return pltpu.make_async_copy(value_hbm.at[rows], value_s.at[rows], value_sem.at[i])

    for i in range(chunks):
        cache_copy(i).start()
    for i in range(chunks):
        value_copy(i).start()

    first_pos, chip, core = info_ref[0], info_ref[1], info_ref[2]
    for j in range(4):
        at = ((chip ^ j) * 2 + core) * pairs
        other = ((chip ^ j) * 2 + 1 - core) * pairs
        q_s[pl.ds(pl.multiple_of(at, pairs), pairs), :] = pieces[j][...].astype(F32)
        q_s[pl.ds(pl.multiple_of(other, pairs), pairs), :] = pieces[4 + j][...].astype(F32)
    r_s[...] = side_ref[...].astype(F32)
    position = first_pos + lane_ids(heads)
    for i in range(chunks):
        cache_copy(i).wait()
        for b in range(i * per, (i + 1) * per):
            query = jnp.concatenate(
                [q_s[pl.ds(n * pairs + b, heads, stride=seqs), :] for n in range(blocks)], axis=1
            ).astype(BF16)
            rope = r_s[pl.ds(b, heads, stride=seqs), :][:, 0:32].astype(BF16)
            past = cache_s[b]
            nt = (((1,), (1,)), ((), ()))
            scores = lax.dot_general(query, past, nt, preferred_element_type=F32)
            scores += lax.dot_general(rope, rot_ref[b], nt, preferred_element_type=F32)
            scores = scores * scale
            valid = position < info_ref[8 + b]
            top = jnp.max(jnp.where(valid, scores, FLOOR), axis=1, keepdims=True)
            weights = jnp.where(valid, jnp.exp(scores - top), 0.0)
            total = jnp.sum(weights, axis=1, keepdims=True)
            rows = slice(b * heads, (b + 1) * heads)
            summed = jnp.dot(weights.astype(BF16), past, preferred_element_type=F32)
            for n in range(blocks):
                o_s[n * pairs + b * heads : n * pairs + (b + 1) * heads, :] = summed[
                    :, n * LANES : (n + 1) * LANES
                ]
            m_s[rows, :] = jnp.broadcast_to(top, (heads, LANES))
            l_s[rows, :] = jnp.broadcast_to(total, (heads, LANES))
    for i in range(chunks):
        value_copy(i).wait()
        rows = slice(i * part, (i + 1) * part)
        valuef_s[i * part * heads : (i + 1) * part * heads, :] = (
            value_s[rows].astype(F32).reshape(part * heads, LANES)
        )
    lane = lane_ids(seqs)
    for h in range(heads):
        latent = jnp.concatenate(
            [o_s[pl.ds(n * pairs + h, seqs, stride=heads), :] for n in range(blocks)], axis=1
        ).astype(BF16)
        weight = valuef_s[pl.ds(h, depth, stride=heads), :].astype(BF16)
        out_ref[h, 0:16, :] = jnp.dot(latent, weight, preferred_element_type=F32).astype(BF16)
        stats = jnp.zeros((seqs, LANES), F32)
        for at, ref in ((0, m_s), (3, l_s)):
            left = ref[pl.ds(h, seqs, stride=heads), :]
            for n in range(3):
                piece = left.astype(BF16).astype(F32)
                stats = jnp.where(lane == at + n, piece, stats)
                left = left - piece
        out_ref[h, 16:32, :] = stats.astype(BF16)
    weight = valuef_s[pl.ds(info_ref[3], depth, stride=heads), :].astype(BF16)
    own_ref[...] = jnp.dot(fresh_ref[...], weight, preferred_element_type=F32)


def gather_kernel(parts_ref, slice_ref, fresh_ref, out_ref, m_s, l_s):
    count = parts_ref.shape[0]
    lane = lane_ids(16)
    top = jnp.full((16, LANES), FLOOR, F32)
    for k in range(count):
        stats = parts_ref[k, 16:32, :].astype(F32)
        m = jnp.sum(jnp.where(lane < 3, stats, 0.0), axis=1, keepdims=True)
        l = jnp.sum(jnp.where((lane >= 3) & (lane < 6), stats, 0.0), axis=1, keepdims=True)
        m = jnp.broadcast_to(m, (16, LANES))
        m_s[k] = m
        l_s[k] = jnp.broadcast_to(l, (16, LANES))
        top = jnp.maximum(top, m)
    total = jnp.zeros((16, LANES), F32)
    summed = jnp.zeros((16, LANES), F32)
    for k in range(count):
        factor = jnp.exp(m_s[k] - top)
        total += factor * l_s[k]
        summed += factor * parts_ref[k, 0:16, :].astype(F32)
    out_ref[0:16, :] = summed
    out_ref[16:32, :] = top
    out_ref[32:48, :] = total
    out_ref[48:64, :] = slice_ref[...] * fresh_ref[...]


def merged(a, b):
    top = jnp.maximum(a[1], b[1])
    wa, wb = jnp.exp(a[1] - top), jnp.exp(b[1] - top)
    return (wa * a[0] + wb * b[0], top, wa * a[2] + wb * b[2], a[3] + b[3])


def parts_of(ref):
    return tuple(ref[16 * i : 16 * (i + 1), :] for i in range(4))


def pair_kernel(a_ref, b_ref, out_ref):
    for i, piece in enumerate(merged(parts_of(a_ref), parts_of(b_ref))):
        out_ref[16 * i : 16 * (i + 1), :] = piece


def finish_kernel(scale, a_ref, b_ref, c_ref, d_ref, dot_ref, own_ref, weight_ref, out_ref):
    left = merged(parts_of(a_ref), parts_of(b_ref))
    summed, top, total, product = merged(left, merged(parts_of(c_ref), parts_of(d_ref)))
    own = (jnp.sum(product, axis=1, keepdims=True) + dot_ref[...]) * scale
    highest = jnp.maximum(top, own)
    factor, own_weight = jnp.exp(top - highest), jnp.exp(own - highest)
    head = (factor * summed + own_weight * own_ref[...]) / (factor * total + own_weight)
    term = jnp.dot(head.astype(BF16), weight_ref[...], preferred_element_type=F32).astype(BF16)
    for peer in range(out_ref.shape[0]):
        out_ref[peer] = term


def shards(
    tokens, norm_gain, w_query, w_latent, w_rotary, latent_gain, w_key_up, w_value_up, w_out,
    cache_latent, cache_rotary, lengths,
):
    seqs = tokens.shape[0]
    kv_count, tp_count = lax.axis_size(KV), lax.axis_size(TP)
    kv_index, tp_index = lax.axis_index(KV), lax.axis_index(TP)
    chip, core = lax.axis_index("tp_0"), lax.axis_index("tp_1")
    heads = kv_count
    rope_width = cache_rotary.shape[2]
    rank = cache_latent.shape[2]
    pos_dev = cache_latent.shape[1]
    model_width = tokens.shape[1] * tp_count
    out_cols = w_out.shape[1]
    score_scale = w_query.shape[2] ** (-0.5)
    sds = jax.ShapeDtypeStruct

    partial = pl.pallas_call(
        project_kernel,
        out_shape=sds((32, LANES), F32),
        in_specs=whole(5),
        out_specs=whole(1)[0],
    )(tokens, norm_gain[None], w_query[:, 0], w_latent, w_rotary)

    half = rope_width // 2
    frequency = THETA ** (-jnp.arange(0, rope_width, 2, dtype=F32) / rope_width)
    angles = lengths.astype(F32)[:, None] * frequency[None, :]
    cosine, sine = jnp.cos(angles), jnp.sin(angles)
    zero = jnp.zeros_like(cosine)
    cos_table = jnp.tile(cosine, (1, LANES // half))
    left_table = jnp.tile(jnp.concatenate([-sine, zero], axis=1), (1, LANES // rope_width))
    right_table = jnp.tile(jnp.concatenate([zero, sine], axis=1), (1, LANES // rope_width))

    partial = partial + swapped(partial, "tp_1", 1)
    sums = [partial] + [swapped(partial, "tp_0", j) for j in (1, 2, 3)]
    block, new_rotary, own_slice, rope_dot = pl.pallas_call(
        functools.partial(query_kernel, float(model_width)),
        out_shape=(
            sds((heads, 32, LANES), BF16),
            sds((seqs, rope_width), BF16),
            sds((seqs, LANES), F32),
            sds((seqs, LANES), F32),
        ),
        in_specs=whole(8),
        out_specs=tuple(whole(4)),
    )(*sums, cos_table, left_table, right_table, w_key_up[:, 0])

    got = lax.all_to_all(block, KV, 0, 0, tiled=True)
    mine = got[:, 0:16, :].reshape(heads * seqs, LANES)
    side = got[:, 16:32, :]
    pieces = [mine] + [swapped(mine, "tp_0", j) for j in (1, 2, 3)]
    pieces = pieces + [swapped(piece, "tp_1", 1) for piece in pieces]

    fresh_f = side[:, :, rope_width : 2 * rope_width].astype(F32)
    inverse = lax.rsqrt(jnp.mean(fresh_f * fresh_f, axis=(0, 2)) + EPS)
    new_latent = (
        fresh_f * inverse[None, :, None] * latent_gain.reshape(heads, 1, rope_width)
    ).astype(BF16)
    new_latent = new_latent.transpose(1, 0, 2).reshape(seqs, rank)
    column_slice = rank // tp_count
    latent_width = rank // (kv_count * tp_count)
    latent_piece = lax.dynamic_slice_in_dim(
        new_latent, (kv_index * tp_count + tp_index) * latent_width, latent_width, 1
    )
    fresh_slice = lax.dynamic_slice_in_dim(
        new_latent, tp_index * column_slice, column_slice, 1
    ).astype(F32)

    first_pos = (kv_index * tp_count + tp_index) * pos_dev
    info = jnp.stack([first_pos, chip, core, kv_index] + [first_pos] * 4).astype(jnp.int32)
    info = jnp.concatenate([info, lengths])
    chunks = 4
    values, own_value = pl.pallas_call(
        functools.partial(attend_kernel, score_scale),
        out_shape=(sds((heads, 32, LANES), BF16), sds((seqs, LANES), F32)),
        in_specs=[pl.BlockSpec(memory_space=pltpu.SMEM)]
        + whole(11)
        + [pl.BlockSpec(memory_space=pl.ANY)] * 2,
        out_specs=tuple(whole(2)),
        scratch_shapes=[
            pltpu.VMEM((heads * seqs * (rank // LANES), LANES), F32),
            pltpu.VMEM((heads * seqs, LANES), F32),
            pltpu.VMEM(cache_latent.shape, BF16),
            pltpu.VMEM(w_value_up.shape, BF16),
            pltpu.VMEM((rank * heads, LANES), F32),
            pltpu.VMEM((heads * seqs * (rank // LANES), LANES), F32),
            pltpu.VMEM((heads * seqs, LANES), F32),
            pltpu.VMEM((heads * seqs, LANES), F32),
            pltpu.SemaphoreType.DMA((chunks,)),
            pltpu.SemaphoreType.DMA((chunks,)),
        ],
        compiler_params=pltpu.CompilerParams(vmem_limit_bytes=56 * 1024 * 1024),
    )(
        info, *pieces, side.reshape(heads * seqs, LANES), new_latent, cache_rotary,
        cache_latent, w_value_up,
    )

    arrived = lax.all_to_all(values, KV, 0, 0, tiled=True)
    state = pl.pallas_call(
        gather_kernel,
        out_shape=sds((64, LANES), F32),
        in_specs=whole(3),
        out_specs=whole(1)[0],
        scratch_shapes=[pltpu.VMEM((kv_count, 16, LANES), F32)] * 2,
    )(arrived, own_slice, fresh_slice)
    state = pl.pallas_call(
        pair_kernel, out_shape=sds((64, LANES), F32), in_specs=whole(2), out_specs=whole(1)[0]
    )(state, swapped(state, "tp_1", 1))
    states = [state] + [swapped(state, "tp_0", j) for j in (1, 2, 3)]
    terms = pl.pallas_call(
        functools.partial(finish_kernel, score_scale),
        out_shape=sds((kv_count, seqs, out_cols), BF16),
        in_specs=whole(7),
        out_specs=whole(1)[0],
    )(*states, rope_dot, own_value, w_out)
    terms = lax.all_to_all(terms, KV, 0, 0, tiled=True)
    mixed_out = jnp.sum(terms.astype(F32), axis=0).astype(BF16)
    return (mixed_out, latent_piece, new_rotary)


def solution(mesh):
    torus = Mesh(mesh.devices.reshape(8, 4, 4, 2), KV_TP)
    in_specs = (
        P(None, TP),
        P(TP),
        P(TP, KV, None),
        P(TP, KV),
        P(TP, None),
        P(),
        P(TP, KV, None),
        P(),
        P(KV, TP),
        P(None, KV_TP, None),
        P(None, KV_TP, None),
        P(),
    )
    out_specs = (P(None, TP), P(None, KV_TP), P())
    return jax.shard_map(
        shards, mesh=torus, in_specs=in_specs, out_specs=out_specs, check_vma=False
    )
```

```python
import functools

import jax
import jax.numpy as jnp
from jax import lax
from jax.experimental import pallas as pl
from jax.experimental.pallas import tpu as pltpu
from jax.sharding import Mesh
from jax.sharding import PartitionSpec as P

KV = ("kv_0", "kv_1")
TP = ("tp_0", "tp_1")
KV_TP = ("kv_0", "kv_1", "tp_0", "tp_1")


THETA = 10000.0
EPS = 1e-06
F32 = jnp.float32
BF16 = jnp.bfloat16
SMALL = pltpu.CompilerParams(vmem_limit_bytes=4 * 1024 * 1024)
FLOOR = -(2.0**127)
LANES = 128
NT = (((1,), (1,)), ((), ()))


def whole(count):
    return [pl.BlockSpec(memory_space=pltpu.VMEM)] * count


def lane_ids(rows):
    return lax.broadcasted_iota(jnp.int32, (rows, LANES), 1)


def swapped(value, axis, step):
    count = lax.axis_size(axis)
    return lax.ppermute(value, axis, [(i, i ^ step) for i in range(count)])


def project_kernel(tokens_ref, gain_ref, query_ref, latent_ref, rotary_ref, out_ref, sum_s):
    tokens = tokens_ref[...].astype(F32)
    scaled = (tokens * gain_ref[...]).astype(BF16)
    squares = jnp.sum(tokens * tokens, axis=1, keepdims=True)
    sum_s[0:16, 0:96] = lax.dot_general(scaled, query_ref[...], NT, preferred_element_type=F32)
    sum_s[0:16, 96:128] = lax.dot_general(scaled, latent_ref[...], NT, preferred_element_type=F32)
    sum_s[16:32, :] = jnp.broadcast_to(squares, (16, LANES))
    sum_s[16:32, 0:32] = lax.dot_general(scaled, rotary_ref[...], NT, preferred_element_type=F32)
    for peer in range(out_ref.shape[0]):
        out_ref[peer] = sum_s[...]


def query_kernel(
    model_width, parts_ref, cos_ref, left_ref, right_ref, key_ref,
    block_ref, rotary_ref, slice_ref, dot_ref,
):
    total = parts_ref[0]
    for peer in range(1, parts_ref.shape[0]):
        total = total + parts_ref[peer]
    lane = lane_ids(16)
    first, second = total[0:16], total[16:32]
    squares = jnp.sum(jnp.where(lane == 64, second, 0.0), axis=1, keepdims=True)
    inverse = lax.rsqrt(squares / model_width + EPS)

    def rotated(v):
        return (
            v * cos_ref[...]
            + pltpu.roll(v, LANES - 16, 1) * left_ref[...]
            + pltpu.roll(v, 16, 1) * right_ref[...]
        )

    query = (first * inverse).astype(BF16)
    query_f = query.astype(F32)
    rope = rotated(query_f)
    fresh = rotated(second * inverse).astype(BF16)
    latent_query = jnp.dot(query[:, 0:64], key_ref[...], preferred_element_type=F32).astype(BF16)
    side = jnp.where(lane < 96, rope, query_f)
    side = pltpu.roll(jnp.where(lane < 64, 0.0, side), 64, 1).astype(BF16)
    for peer in range(block_ref.shape[0]):
        block_ref[peer, 0:16, :] = latent_query
        block_ref[peer, 16:32, :] = side
    rotary_ref[...] = fresh[:, 0:32]
    slice_ref[...] = latent_query.astype(F32)
    both = jnp.where(lane < 32, side.astype(F32) * fresh.astype(F32), 0.0)
    dot_ref[...] = jnp.broadcast_to(jnp.sum(both, axis=1, keepdims=True), (16, LANES))


def attend_kernel(scale, info_ref, *refs):
    pieces = refs[0:8]
    (side_ref, fresh_ref, rot_ref, cache_hbm, value_hbm, out_ref, own_ref) = refs[8:15]
    (q_s, r_s, cache_s, value_s, valuef_s, o_s, m_s, l_s, cache_sem, value_sem) = refs[15:]
    seqs, heads = 16, 32
    chunks = cache_sem.shape[0]
    per = seqs // chunks
    depth = value_s.shape[0]
    part = depth // chunks
    blocks, gap = depth // LANES, heads + 1

    def cache_copy(i):
        rows = pl.ds(i * per, per)
        return pltpu.make_async_copy(cache_hbm.at[rows], cache_s.at[rows], cache_sem.at[i])

    def value_copy(i):
        rows = pl.ds(i * part, part)
        return pltpu.make_async_copy(value_hbm.at[rows], value_s.at[rows], value_sem.at[i])

    for i in range(chunks):
        cache_copy(i).start()
    for i in range(chunks):
        value_copy(i).start()

    first_pos, chip, core = info_ref[0], info_ref[1], info_ref[2]
    for j in range(4):
        at, other = (chip ^ j) * 2 + core, (chip ^ j) * 2 + 1 - core
        q_s[at] = pltpu.einshape("hbr->bhr", pieces[j][...].reshape(heads, seqs, LANES))
        q_s[other] = pltpu.einshape("hbr->bhr", pieces[4 + j][...].reshape(heads, seqs, LANES))
    r_s[...] = pltpu.einshape("hbr->bhr", side_ref[...].reshape(heads, seqs, LANES))
    position = first_pos + lane_ids(heads)
    for i in range(chunks):
        cache_copy(i).wait()
        for b in range(i * per, (i + 1) * per):
            query = jnp.concatenate([q_s[n, b] for n in range(blocks)], axis=1)
            rope = r_s[b][:, 0:32]
            past = cache_s[b]
            scores = lax.dot_general(query, past, NT, preferred_element_type=F32)
            scores += jnp.dot(rope, rot_ref[b], preferred_element_type=F32)
            scores = scores * scale
            valid = position < info_ref[8 + b]
            top = jnp.max(jnp.where(valid, scores, FLOOR), axis=1, keepdims=True)
            weights = jnp.where(valid, jnp.exp(scores - top), 0.0)
            total = jnp.sum(weights, axis=1, keepdims=True)
            rows = slice(b * gap, b * gap + heads)
            summed = jnp.dot(weights.astype(BF16), past, preferred_element_type=F32)
            for n in range(blocks):
                at = (n * seqs + b) * gap
                o_s[at : at + heads, :] = summed[:, n * LANES : (n + 1) * LANES]
            m_s[rows, :] = jnp.broadcast_to(top, (heads, LANES))
            l_s[rows, :] = jnp.broadcast_to(total, (heads, LANES))
    for i in range(chunks):
        value_copy(i).wait()

        def spread(step, _):
            for n in range(8):
                r = i * part + step * 8 + n
                valuef_s[pl.ds(r * gap, heads), :] = value_s[r].astype(F32)
            return 0

        lax.fori_loop(0, part // 8, spread, 0)
    lane = lane_ids(seqs)
    for h in range(heads):
        latent = jnp.concatenate(
            [o_s[pl.ds(n * seqs * gap + h, seqs, stride=gap), :] for n in range(blocks)], axis=1
        ).astype(BF16)
        weight = valuef_s[pl.ds(h, depth, stride=gap), :].astype(BF16)
        out_ref[h, 0:16, :] = jnp.dot(latent, weight, preferred_element_type=F32).astype(BF16)
        stats = jnp.zeros((seqs, LANES), F32)
        for at, ref in ((0, m_s), (3, l_s)):
            left = ref[pl.ds(h, seqs, stride=gap), :]
            for n in range(3):
                piece = left.astype(BF16).astype(F32)
                stats = jnp.where(lane == at + n, piece, stats)
                left = left - piece
        out_ref[h, 16:32, :] = stats.astype(BF16)
    weight = valuef_s[pl.ds(info_ref[3], depth, stride=gap), :].astype(BF16)
    own_ref[...] = jnp.dot(fresh_ref[...], weight, preferred_element_type=F32)


def gather_kernel(parts_ref, slice_ref, fresh_ref, out_ref, m_s, l_s):
    count = parts_ref.shape[0]
    lane = lane_ids(16)
    top = jnp.full((16, LANES), FLOOR, F32)
    for k in range(count):
        stats = parts_ref[k, 16:32, :].astype(F32)
        m = jnp.sum(jnp.where(lane < 3, stats, 0.0), axis=1, keepdims=True)
        l = jnp.sum(jnp.where((lane >= 3) & (lane < 6), stats, 0.0), axis=1, keepdims=True)
        m = jnp.broadcast_to(m, (16, LANES))
        m_s[k] = m
        l_s[k] = jnp.broadcast_to(l, (16, LANES))
        top = jnp.maximum(top, m)
    total = jnp.zeros((16, LANES), F32)
    summed = jnp.zeros((16, LANES), F32)
    for k in range(count):
        factor = jnp.exp(m_s[k] - top)
        total += factor * l_s[k]
        summed += factor * parts_ref[k, 0:16, :].astype(F32)
    own = jnp.sum(slice_ref[...] * fresh_ref[...], axis=1, keepdims=True)
    stats = jnp.where(lane == 0, top, jnp.where(lane == 1, total, own))
    for peer in range(out_ref.shape[0]):
        out_ref[peer, 0:16, :] = summed
        out_ref[peer, 16:32, :] = stats


def lane_of(stats, n):
    return jnp.sum(jnp.where(lane_ids(stats.shape[0]) == n, stats, 0.0), axis=1, keepdims=True)


def finish_kernel(scale, parts_ref, dot_ref, own_ref, weight_ref, out_ref):
    peers = range(parts_ref.shape[0])
    stats = [parts_ref[peer, 16:32, :] for peer in peers]
    tops = [lane_of(s, 0) for s in stats]
    own = (functools.reduce(jnp.add, [lane_of(s, 2) for s in stats]) + dot_ref[...]) * scale
    highest = functools.reduce(jnp.maximum, tops, own)
    total = jnp.exp(own - highest)
    summed = total * own_ref[...]
    for peer in peers:
        factor = jnp.exp(tops[peer] - highest)
        total += factor * lane_of(stats[peer], 1)
        summed += factor * parts_ref[peer, 0:16, :]
    head = (summed / total).astype(BF16)
    term = jnp.dot(head, weight_ref[...], preferred_element_type=F32).astype(BF16)
    for peer in range(out_ref.shape[0]):
        out_ref[peer] = term


def shards(
    tokens, norm_gain, w_query, w_latent, w_rotary, latent_gain, w_key_up, w_value_up, w_out,
    cache_latent, cache_rotary, lengths,
):
    seqs = tokens.shape[0]
    kv_count, tp_count = lax.axis_size(KV), lax.axis_size(TP)
    kv_index, tp_index = lax.axis_index(KV), lax.axis_index(TP)
    chip, core = lax.axis_index("tp_0"), lax.axis_index("tp_1")
    heads = kv_count
    rope_width = cache_rotary.shape[2]
    rank = cache_latent.shape[2]
    pos_dev = cache_latent.shape[1]
    model_width = tokens.shape[1] * tp_count
    out_cols = w_out.shape[1]
    score_scale = w_query.shape[2] ** (-0.5)
    sds = jax.ShapeDtypeStruct

    partial = pl.pallas_call(
        project_kernel,
        out_shape=sds((tp_count, 32, LANES), F32),
        in_specs=whole(5),
        out_specs=whole(1)[0],
        scratch_shapes=[pltpu.VMEM((32, LANES), F32)],
        compiler_params=SMALL,
    )(tokens, norm_gain[None], w_query[:, 0].T, w_latent.T, w_rotary.T)

    lane = lax.broadcasted_iota(jnp.int32, (seqs, LANES), 1)
    pair = lane % (rope_width // 2)
    frequency = THETA ** (-(2 * pair).astype(F32) / rope_width)
    angles = lengths.astype(F32)[:, None] * frequency
    cosine, sine = jnp.cos(angles), jnp.sin(angles)
    low = lane % rope_width < rope_width // 2
    left, right = jnp.where(low, -sine, 0.0), jnp.where(low, 0.0, sine)

    first_pos = (kv_index * tp_count + tp_index) * pos_dev
    info = jnp.stack([first_pos, chip, core, kv_index] + [first_pos] * 4).astype(jnp.int32)
    info = jnp.concatenate([info, lengths])
    partial, cosine, left, right, info = lax.optimization_barrier(
        (partial, cosine, left, right, info)
    )

    sums = lax.all_to_all(partial, TP, 0, 0, tiled=True)
    block, new_rotary, own_slice, rope_dot = pl.pallas_call(
        functools.partial(query_kernel, float(model_width)),
        out_shape=(
            sds((heads, 32, LANES), BF16),
            sds((seqs, rope_width), BF16),
            sds((seqs, LANES), F32),
            sds((seqs, LANES), F32),
        ),
        in_specs=whole(5),
        out_specs=tuple(whole(4)),
        compiler_params=SMALL,
    )(sums, cosine, left, right, w_key_up[:, 0].T)

    got = lax.all_to_all(block, KV, 0, 0, tiled=True)
    mine = got[:, 0:16, :].reshape(heads * seqs, LANES)
    side = got[:, 16:32, :]
    pieces = [mine] + [swapped(mine, "tp_0", j) for j in (1, 2, 3)]
    pieces = pieces + [swapped(piece, "tp_1", 1) for piece in pieces]

    fresh_f = side[:, :, rope_width : 2 * rope_width].astype(F32)
    inverse = lax.rsqrt(jnp.mean(fresh_f * fresh_f, axis=(0, 2)) + EPS)
    new_latent = (
        fresh_f * inverse[None, :, None] * latent_gain.reshape(heads, 1, rope_width)
    ).astype(BF16)
    new_latent = new_latent.transpose(1, 0, 2).reshape(seqs, rank)
    column_slice = rank // tp_count
    latent_width = rank // (kv_count * tp_count)
    latent_piece = lax.dynamic_slice_in_dim(
        new_latent, (kv_index * tp_count + tp_index) * latent_width, latent_width, 1
    )
    fresh_slice = lax.dynamic_slice_in_dim(
        new_latent, tp_index * column_slice, column_slice, 1
    ).astype(F32)

    chunks = 4
    values, own_value = pl.pallas_call(
        functools.partial(attend_kernel, score_scale),
        out_shape=(sds((heads, 32, LANES), BF16), sds((seqs, LANES), F32)),
        in_specs=[pl.BlockSpec(memory_space=pltpu.SMEM)]
        + whole(11)
        + [pl.BlockSpec(memory_space=pl.ANY)] * 2,
        out_specs=tuple(whole(2)),
        scratch_shapes=[
            pltpu.VMEM((rank // LANES, seqs, heads, LANES), BF16),
            pltpu.VMEM((seqs, heads, LANES), BF16),
            pltpu.VMEM(cache_latent.shape, BF16),
            pltpu.VMEM(w_value_up.shape, BF16),
            pltpu.VMEM((rank * (heads + 1), LANES), F32),
            pltpu.VMEM(((heads + 1) * seqs * (rank // LANES), LANES), F32),
            pltpu.VMEM(((heads + 1) * seqs, LANES), F32),
            pltpu.VMEM(((heads + 1) * seqs, LANES), F32),
            pltpu.SemaphoreType.DMA((chunks,)),
            pltpu.SemaphoreType.DMA((chunks,)),
        ],
        compiler_params=pltpu.CompilerParams(vmem_limit_bytes=48 * 1024 * 1024),
    )(
        info, *pieces, side.reshape(heads * seqs, LANES), new_latent,
        cache_rotary.transpose(0, 2, 1), cache_latent, w_value_up,
    )

    values, own_value, latent_piece, fresh_slice = lax.optimization_barrier(
        (values, own_value, latent_piece, fresh_slice)
    )
    arrived = lax.all_to_all(values, KV, 0, 0, tiled=True)
    states = pl.pallas_call(
        gather_kernel,
        out_shape=sds((tp_count, 32, LANES), F32),
        in_specs=whole(3),
        out_specs=whole(1)[0],
        scratch_shapes=[pltpu.VMEM((kv_count, 16, LANES), F32)] * 2,
        compiler_params=SMALL,
    )(arrived, own_slice, fresh_slice)
    states = lax.all_to_all(states, TP, 0, 0, tiled=True)
    terms = pl.pallas_call(
        functools.partial(finish_kernel, score_scale),
        out_shape=sds((kv_count, seqs, out_cols), BF16),
        in_specs=whole(4),
        out_specs=whole(1)[0],
        compiler_params=SMALL,
    )(states, rope_dot, own_value, w_out)
    terms = lax.all_to_all(terms, KV, 0, 0, tiled=True)
    mixed_out = jnp.sum(terms.astype(F32), axis=0).astype(BF16)
    return (mixed_out, latent_piece, new_rotary)


def solution(mesh):
    torus = Mesh(mesh.devices.reshape(8, 4, 4, 2), KV_TP)
    in_specs = (
        P(None, TP),
        P(TP),
        P(TP, KV, None),
        P(TP, KV),
        P(TP, None),
        P(),
        P(TP, KV, None),
        P(),
        P(KV, TP),
        P(None, KV_TP, None),
        P(None, KV_TP, None),
        P(),
    )
    out_specs = (P(None, TP), P(None, KV_TP), P())
    return jax.shard_map(
        shards, mesh=torus, in_specs=in_specs, out_specs=out_specs, check_vma=False
    )
```

```python
import functools

import jax
import jax.numpy as jnp
from jax import lax
from jax.experimental import pallas as pl
from jax.experimental.pallas import tpu as pltpu
from jax.sharding import Mesh
from jax.sharding import PartitionSpec as P

KV = ("kv_0", "kv_1")
TP = ("tp_0", "tp_1")
KV_TP = ("kv_0", "kv_1", "tp_0", "tp_1")


THETA = 10000.0
EPS = 1e-06
F32 = jnp.float32
BF16 = jnp.bfloat16
SMALL = pltpu.CompilerParams(vmem_limit_bytes=4 * 1024 * 1024)
FLOOR = -(2.0**127)
LANES = 128
NT = (((1,), (1,)), ((), ()))


def whole(count):
    return [pl.BlockSpec(memory_space=pltpu.VMEM)] * count


def lane_ids(rows):
    return lax.broadcasted_iota(jnp.int32, (rows, LANES), 1)


def swapped(value, axis, step):
    count = lax.axis_size(axis)
    return lax.ppermute(value, axis, [(i, i ^ step) for i in range(count)])


def fetch(pairs, sems):
    copies = [pltpu.make_async_copy(src, dst, sems.at[i]) for i, (src, dst) in enumerate(pairs)]
    for copy in copies:
        copy.start()
    return copies


def project_kernel(
    tokens_hbm, gain_hbm, query_hbm, latent_hbm, rotary_hbm, out_ref,
    tokens_s, gain_s, query_s, latent_s, rotary_s, sum_s, sems,
):
    copies = fetch(
        [
            (tokens_hbm, tokens_s), (gain_hbm, gain_s), (query_hbm, query_s),
            (latent_hbm, latent_s), (rotary_hbm, rotary_s),
        ],
        sems,
    )
    for copy in copies:
        copy.wait()
    tokens = tokens_s[...].astype(F32)
    scaled = (tokens * gain_s[...]).astype(BF16)
    squares = jnp.sum(tokens * tokens, axis=1, keepdims=True)
    sum_s[0:16, 0:96] = lax.dot_general(scaled, query_s[...], NT, preferred_element_type=F32)
    sum_s[0:16, 96:128] = lax.dot_general(scaled, latent_s[...], NT, preferred_element_type=F32)
    sum_s[16:32, :] = jnp.broadcast_to(squares, (16, LANES))
    sum_s[16:32, 0:32] = lax.dot_general(scaled, rotary_s[...], NT, preferred_element_type=F32)
    for peer in range(out_ref.shape[0]):
        out_ref[peer] = sum_s[...]


def table_kernel(lengths_ref, frequency_ref, key_in_ref, cos_ref, sin_ref, key_ref):
    row = lax.broadcasted_iota(jnp.int32, (16, LANES), 0)
    position = jnp.zeros((16, LANES), jnp.int32)
    for b in range(16):
        position = jnp.where(row == b, lengths_ref[b], position)
    angles = position.astype(F32) * frequency_ref[...]
    cos_ref[...] = jnp.cos(angles)
    sin_ref[...] = jnp.sin(angles)
    key_ref[...] = key_in_ref[...]


def query_kernel(
    model_width, parts_ref, cos_ref, sin_ref, key_ref,
    block_ref, rotary_ref, slice_ref, dot_ref,
):
    total = parts_ref[0]
    for peer in range(1, parts_ref.shape[0]):
        total = total + parts_ref[peer]
    lane = lane_ids(16)
    low = (lane & 31) < 16
    first, second = total[0:16], total[16:32]
    squares = jnp.sum(jnp.where(lane == 64, second, 0.0), axis=1, keepdims=True)
    inverse = lax.rsqrt(squares / model_width + EPS)

    def rotated(v):
        turned = jnp.where(low, -pltpu.roll(v, LANES - 16, 1), pltpu.roll(v, 16, 1))
        return v * cos_ref[...] + turned * sin_ref[...]

    query = (first * inverse).astype(BF16)
    query_f = query.astype(F32)
    rope = rotated(query_f)
    fresh = rotated(second * inverse).astype(BF16)
    latent_query = jnp.dot(query[:, 0:64], key_ref[...], preferred_element_type=F32).astype(BF16)
    side = jnp.where(lane < 96, rope, query_f)
    side = pltpu.roll(jnp.where(lane < 64, 0.0, side), 64, 1).astype(BF16)
    for peer in range(block_ref.shape[0]):
        block_ref[peer, 0:16, :] = latent_query
        block_ref[peer, 16:32, :] = side
    rotary_ref[...] = fresh[:, 0:32]
    slice_ref[...] = latent_query.astype(F32)
    both = jnp.where(lane < 32, side.astype(F32) * fresh.astype(F32), 0.0)
    dot_ref[...] = jnp.broadcast_to(jnp.sum(both, axis=1, keepdims=True), (16, LANES))


def sort_kernel(block_ref, mine_ref, side_ref):
    mine_ref[...] = pltpu.einshape("hbr->bhr", block_ref[:, 0:16, :])
    side_ref[...] = pltpu.einshape("hbr->bhr", block_ref[:, 16:32, :])


def fresh_kernel(side_ref, gain_ref, fresh_ref, slice_ref, piece_ref, row_s):
    heads, width, rank = side_ref.shape[1], 32, gain_ref.shape[1]
    square = jnp.zeros((16, width), F32)
    for k in range(heads):
        block = side_ref[:, k, width : 2 * width].astype(F32)
        row_s[:, k * width : (k + 1) * width] = block
        square += block * block
    mean = jnp.sum(square, axis=1, keepdims=True) / rank
    fresh = (row_s[...] * lax.rsqrt(mean + EPS) * gain_ref[...]).astype(BF16)
    fresh_ref[...] = fresh
    row_s[...] = fresh.astype(F32)
    tp = lax.axis_index("tp_0") * 2 + lax.axis_index("tp_1")
    kv = lax.axis_index("kv_0") * 4 + lax.axis_index("kv_1")
    slice_ref[...] = row_s[:, pl.ds(pl.multiple_of(tp * LANES, LANES), LANES)]
    column = (kv * 8 + tp) * 4
    base = column // LANES
    held = row_s[:, pl.ds(pl.multiple_of(base * LANES, LANES), LANES)]
    held = pltpu.roll(held, (LANES - (column - base * LANES)) % LANES, 1)
    piece_ref[...] = held.T[0:4, :].astype(BF16)


def values_kernel(order_ref, value_ref, out_ref):
    step = 64

    def turn(j, _):
        at = pl.ds(pl.multiple_of(j * step, step), step)
        out_ref[:, at, :] = pltpu.einshape("rhv->hrv", value_ref[at])
        return 0

    lax.fori_loop(0, value_ref.shape[0] // step, turn, 0)


def attend_kernel(scale, lengths_ref, *refs):
    pieces = refs[0:8]
    (side_ref, fresh_ref, rot_ref, value_ref, cache_ref, out_ref, own_ref) = refs[8:15]
    (q_s, o_s, m_s, l_s) = refs[15:]
    seqs, heads = 16, 32
    blocks, gap = q_s.shape[0], heads + 1

    chip, core = lax.axis_index("tp_0"), lax.axis_index("tp_1")
    kv = lax.axis_index("kv_0") * 4 + lax.axis_index("kv_1")
    first_pos = (kv * 8 + chip * 2 + core) * LANES
    for j in range(4):
        q_s[(chip ^ j) * 2 + core] = pieces[j][...]
        q_s[(chip ^ j) * 2 + 1 - core] = pieces[4 + j][...]
    position = first_pos + lane_ids(heads)
    for b in range(seqs):
        query = jnp.concatenate([q_s[n, b] for n in range(blocks)], axis=1)
        rope = side_ref[b][:, 0:32]
        past = cache_ref[b]
        scores = lax.dot_general(query, past, NT, preferred_element_type=F32)
        scores += jnp.dot(rope, rot_ref[b], preferred_element_type=F32)
        scores = scores * scale
        valid = position < lengths_ref[b]
        top = jnp.max(jnp.where(valid, scores, FLOOR), axis=1, keepdims=True)
        weights = jnp.where(valid, jnp.exp(scores - top), 0.0)
        total = jnp.sum(weights, axis=1, keepdims=True)
        rows = slice(b * gap, b * gap + heads)
        summed = jnp.dot(weights.astype(BF16), past, preferred_element_type=F32)
        for n in range(blocks):
            at = (n * seqs + b) * gap
            o_s[at : at + heads, :] = summed[:, n * LANES : (n + 1) * LANES]
        m_s[rows, :] = jnp.broadcast_to(top, (heads, LANES))
        l_s[rows, :] = jnp.broadcast_to(total, (heads, LANES))
    lane = lane_ids(seqs)
    for h in range(heads):
        latent = jnp.concatenate(
            [o_s[pl.ds(n * seqs * gap + h, seqs, stride=gap), :] for n in range(blocks)], axis=1
        ).astype(BF16)
        out_ref[h, 0:16, :] = jnp.dot(
            latent, value_ref[h], preferred_element_type=F32
        ).astype(BF16)
        stats = jnp.zeros((seqs, LANES), F32)
        for at, ref in ((0, m_s), (3, l_s)):
            left = ref[pl.ds(h, seqs, stride=gap), :]
            for n in range(3):
                piece = left.astype(BF16).astype(F32)
                stats = jnp.where(lane == at + n, piece, stats)
                left = left - piece
        out_ref[h, 16:32, :] = stats.astype(BF16)
    own_ref[...] = jnp.dot(fresh_ref[...], value_ref[kv], preferred_element_type=F32)


def gather_kernel(parts_ref, slice_ref, fresh_ref, out_ref, m_s, l_s):
    count = parts_ref.shape[0]
    lane = lane_ids(16)
    top = jnp.full((16, LANES), FLOOR, F32)
    for k in range(count):
        stats = parts_ref[k, 16:32, :].astype(F32)
        m = jnp.sum(jnp.where(lane < 3, stats, 0.0), axis=1, keepdims=True)
        l = jnp.sum(jnp.where((lane >= 3) & (lane < 6), stats, 0.0), axis=1, keepdims=True)
        m = jnp.broadcast_to(m, (16, LANES))
        m_s[k] = m
        l_s[k] = jnp.broadcast_to(l, (16, LANES))
        top = jnp.maximum(top, m)
    total = jnp.zeros((16, LANES), F32)
    summed = jnp.zeros((16, LANES), F32)
    for k in range(count):
        factor = jnp.exp(m_s[k] - top)
        total += factor * l_s[k]
        summed += factor * parts_ref[k, 0:16, :].astype(F32)
    own = jnp.sum(slice_ref[...] * fresh_ref[...], axis=1, keepdims=True)
    stats = jnp.where(lane == 0, top, jnp.where(lane == 1, total, own))
    for peer in range(out_ref.shape[0]):
        out_ref[peer, 0:16, :] = summed
        out_ref[peer, 16:32, :] = stats


def lane_of(stats, n):
    return jnp.sum(jnp.where(lane_ids(stats.shape[0]) == n, stats, 0.0), axis=1, keepdims=True)


def finish_kernel(scale, parts_ref, dot_ref, own_ref, weight_ref, out_ref):
    peers = range(parts_ref.shape[0])
    stats = [parts_ref[peer, 16:32, :] for peer in peers]
    tops = [lane_of(s, 0) for s in stats]
    own = (functools.reduce(jnp.add, [lane_of(s, 2) for s in stats]) + dot_ref[...]) * scale
    highest = functools.reduce(jnp.maximum, tops, own)
    total = jnp.exp(own - highest)
    summed = total * own_ref[...]
    for peer in peers:
        factor = jnp.exp(tops[peer] - highest)
        total += factor * lane_of(stats[peer], 1)
        summed += factor * parts_ref[peer, 0:16, :]
    head = (summed / total).astype(BF16)
    term = jnp.dot(head, weight_ref[...], preferred_element_type=F32).astype(BF16)
    for peer in range(out_ref.shape[0]):
        out_ref[peer] = term


def shards(
    tokens, norm_gain, w_query, w_latent, w_rotary, latent_gain, w_key_up, w_value_up, w_out,
    cache_latent, cache_rotary, lengths,
):
    seqs = tokens.shape[0]
    kv_count, tp_count = lax.axis_size(KV), lax.axis_size(TP)
    heads = kv_count
    rope_width = cache_rotary.shape[2]
    rank = cache_latent.shape[2]
    pos_dev = cache_latent.shape[1]
    model_width = tokens.shape[1] * tp_count
    out_cols = w_out.shape[1]
    score_scale = w_query.shape[2] ** (-0.5)
    sds = jax.ShapeDtypeStruct

    hbm = pl.BlockSpec(memory_space=pltpu.HBM)
    smem = pl.BlockSpec(memory_space=pltpu.SMEM)
    width = tokens.shape[1]
    query_width = w_query.shape[2]
    partial = pl.pallas_call(
        project_kernel,
        out_shape=sds((tp_count, 32, LANES), F32),
        in_specs=[hbm] * 5,
        out_specs=whole(1)[0],
        scratch_shapes=[
            pltpu.VMEM((seqs, width), BF16),
            pltpu.VMEM((1, width), F32),
            pltpu.VMEM((query_width, width), BF16),
            pltpu.VMEM((rope_width, width), BF16),
            pltpu.VMEM((rope_width, width), BF16),
            pltpu.VMEM((32, LANES), F32),
            pltpu.SemaphoreType.DMA((5,)),
        ],
    )(tokens, norm_gain[None], w_query[:, 0].T, w_latent.T, w_rotary.T)

    pair = lax.broadcasted_iota(jnp.int32, (1, LANES), 1) % (rope_width // 2)
    frequency = THETA ** (-(2 * pair).astype(F32) / rope_width)
    cosine, sine, key_up = pl.pallas_call(
        table_kernel,
        out_shape=(sds((seqs, LANES), F32),) * 2 + (sds((w_key_up.shape[2], LANES), BF16),),
        in_specs=[smem] + whole(2),
        out_specs=tuple(whole(3)),
        compiler_params=SMALL,
    )(lengths, frequency, w_key_up[:, 0].T)
    partial, cosine, sine, key_up = lax.optimization_barrier((partial, cosine, sine, key_up))

    sums = lax.all_to_all(partial, TP, 0, 0, tiled=True)
    block, new_rotary, own_slice, rope_dot = pl.pallas_call(
        functools.partial(query_kernel, float(model_width)),
        out_shape=(
            sds((heads, 32, LANES), BF16),
            sds((seqs, rope_width), BF16),
            sds((seqs, LANES), F32),
            sds((seqs, LANES), F32),
        ),
        in_specs=whole(4),
        out_specs=tuple(whole(4)),
        compiler_params=SMALL,
    )(sums, cosine, sine, key_up)

    got = lax.all_to_all(block, KV, 0, 0, tiled=True)
    mine, side = pl.pallas_call(
        sort_kernel,
        out_shape=(sds((seqs, heads, LANES), BF16),) * 2,
        in_specs=whole(1),
        out_specs=tuple(whole(2)),
        compiler_params=SMALL,
    )(got)
    pieces = [swapped(mine, "tp_0", j) for j in (1, 2, 3)]

    new_latent, fresh_slice, latent_piece = pl.pallas_call(
        fresh_kernel,
        out_shape=(sds((seqs, rank), BF16), sds((seqs, LANES), F32), sds((4, seqs), BF16)),
        in_specs=whole(2),
        out_specs=tuple(whole(3)),
        scratch_shapes=[pltpu.VMEM((seqs, rank), F32)],
        compiler_params=SMALL,
    )(side, latent_gain[None])
    value_up = pl.pallas_call(
        values_kernel,
        out_shape=sds((heads, rank, LANES), BF16),
        in_specs=whole(2),
        out_specs=whole(1)[0],
        compiler_params=pltpu.CompilerParams(vmem_limit_bytes=20 * 1024 * 1024),
    )(fresh_slice, w_value_up)
    pieces, value_up = lax.optimization_barrier((pieces, value_up))
    pieces = [mine] + pieces
    pieces = pieces + [swapped(piece, "tp_1", 1) for piece in pieces]

    pairs_gap = seqs * (heads + 1)
    values, own_value = pl.pallas_call(
        functools.partial(attend_kernel, score_scale),
        out_shape=(sds((heads, 32, LANES), BF16), sds((seqs, LANES), F32)),
        in_specs=[smem] + whole(13),
        out_specs=tuple(whole(2)),
        scratch_shapes=[
            pltpu.VMEM((rank // LANES, seqs, heads, LANES), BF16),
            pltpu.VMEM((pairs_gap * (rank // LANES), LANES), F32),
            pltpu.VMEM((pairs_gap, LANES), F32),
            pltpu.VMEM((pairs_gap, LANES), F32),
        ],
        compiler_params=pltpu.CompilerParams(vmem_limit_bytes=20 * 1024 * 1024),
    )(
        lengths, *pieces, side, new_latent, cache_rotary.transpose(0, 2, 1), value_up, cache_latent
    )

    arrived = lax.all_to_all(values, KV, 0, 0, tiled=True)
    states = pl.pallas_call(
        gather_kernel,
        out_shape=sds((tp_count, 32, LANES), F32),
        in_specs=whole(3),
        out_specs=whole(1)[0],
        scratch_shapes=[pltpu.VMEM((kv_count, 16, LANES), F32)] * 2,
        compiler_params=SMALL,
    )(arrived, own_slice, fresh_slice)
    states = lax.all_to_all(states, TP, 0, 0, tiled=True)
    terms = pl.pallas_call(
        functools.partial(finish_kernel, score_scale),
        out_shape=sds((kv_count, seqs, out_cols), BF16),
        in_specs=whole(4),
        out_specs=whole(1)[0],
        compiler_params=SMALL,
    )(states, rope_dot, own_value, w_out)
    terms = lax.all_to_all(terms, KV, 0, 0, tiled=True)
    mixed_out = jnp.sum(terms.astype(F32), axis=0).astype(BF16)
    return (mixed_out, latent_piece.T, new_rotary)


def solution(mesh):
    torus = Mesh(mesh.devices.reshape(8, 4, 4, 2), KV_TP)
    in_specs = (
        P(None, TP),
        P(TP),
        P(TP, KV, None),
        P(TP, KV),
        P(TP, None),
        P(),
        P(TP, KV, None),
        P(),
        P(KV, TP),
        P(None, KV_TP, None),
        P(None, KV_TP, None),
        P(),
    )
    out_specs = (P(None, TP), P(None, KV_TP), P())
    return jax.shard_map(
        shards, mesh=torus, in_specs=in_specs, out_specs=out_specs, check_vma=False
    )
```

```python
import functools

import jax
import jax.numpy as jnp
from jax import lax
from jax.experimental import pallas as pl
from jax.experimental.pallas import tpu as pltpu
from jax.sharding import Mesh
from jax.sharding import PartitionSpec as P

KV = ("kv_0", "kv_1")
TP = ("tp_0", "tp_1")
KV_TP = ("kv_0", "kv_1", "tp_0", "tp_1")


THETA = 10000.0
EPS = 1e-06
F32 = jnp.float32
BF16 = jnp.bfloat16
SMALL = pltpu.CompilerParams(vmem_limit_bytes=4 * 1024 * 1024)
FLOOR = -(2.0**127)
LANES = 128
NT = (((1,), (1,)), ((), ()))


def whole(count):
    return [pl.BlockSpec(memory_space=pltpu.VMEM)] * count


def lane_ids(rows):
    return lax.broadcasted_iota(jnp.int32, (rows, LANES), 1)


def swapped(value, axis, step):
    count = lax.axis_size(axis)
    return lax.ppermute(value, axis, [(i, i ^ step) for i in range(count)])


def fetch(pairs, sems):
    copies = [pltpu.make_async_copy(src, dst, sems.at[i]) for i, (src, dst) in enumerate(pairs)]
    for copy in copies:
        copy.start()
    return copies


def project_kernel(
    tokens_hbm, gain_hbm, query_hbm, latent_hbm, rotary_hbm, out_ref,
    tokens_s, gain_s, query_s, latent_s, rotary_s, sum_s, sems,
):
    copies = fetch(
        [
            (tokens_hbm, tokens_s), (gain_hbm, gain_s), (query_hbm, query_s),
            (latent_hbm, latent_s), (rotary_hbm, rotary_s),
        ],
        sems,
    )
    for copy in copies:
        copy.wait()
    tokens = tokens_s[...].astype(F32)
    scaled = (tokens * gain_s[...]).astype(BF16)
    squares = jnp.sum(tokens * tokens, axis=1, keepdims=True)
    sum_s[0:16, 0:96] = lax.dot_general(scaled, query_s[...], NT, preferred_element_type=F32)
    sum_s[0:16, 96:128] = lax.dot_general(scaled, latent_s[...], NT, preferred_element_type=F32)
    sum_s[16:32, :] = jnp.broadcast_to(squares, (16, LANES))
    sum_s[16:32, 0:32] = lax.dot_general(scaled, rotary_s[...], NT, preferred_element_type=F32)
    for peer in range(out_ref.shape[0]):
        out_ref[peer] = sum_s[...]


def table_kernel(lengths_ref, frequency_ref, key_in_ref, cos_ref, sin_ref, key_ref):
    row = lax.broadcasted_iota(jnp.int32, (16, LANES), 0)
    position = jnp.zeros((16, LANES), jnp.int32)
    for b in range(16):
        position = jnp.where(row == b, lengths_ref[b], position)
    angles = position.astype(F32) * frequency_ref[...]
    cos_ref[...] = jnp.cos(angles)
    sin_ref[...] = jnp.sin(angles)
    key_ref[...] = key_in_ref[...]


def query_kernel(
    model_width, parts_ref, cos_ref, sin_ref, key_ref,
    block_ref, rotary_ref, slice_ref, dot_ref,
):
    total = parts_ref[0]
    for peer in range(1, parts_ref.shape[0]):
        total = total + parts_ref[peer]
    lane = lane_ids(16)
    low = (lane & 31) < 16
    first, second = total[0:16], total[16:32]
    squares = jnp.sum(jnp.where(lane == 64, second, 0.0), axis=1, keepdims=True)
    inverse = lax.rsqrt(squares / model_width + EPS)

    def rotated(v):
        turned = jnp.where(low, -pltpu.roll(v, LANES - 16, 1), pltpu.roll(v, 16, 1))
        return v * cos_ref[...] + turned * sin_ref[...]

    query = (first * inverse).astype(BF16)
    query_f = query.astype(F32)
    rope = rotated(query_f)
    fresh = rotated(second * inverse).astype(BF16)
    latent_query = jnp.dot(query[:, 0:64], key_ref[...], preferred_element_type=F32).astype(BF16)
    side = jnp.where(lane < 96, rope, query_f)
    side = pltpu.roll(jnp.where(lane < 64, 0.0, side), 64, 1).astype(BF16)
    for peer in range(block_ref.shape[0]):
        block_ref[peer, 0:16, :] = latent_query
        block_ref[peer, 16:32, :] = side
    rotary_ref[...] = fresh[:, 0:32]
    slice_ref[...] = latent_query.astype(F32)
    both = jnp.where(lane < 32, side.astype(F32) * fresh.astype(F32), 0.0)
    dot_ref[...] = jnp.broadcast_to(jnp.sum(both, axis=1, keepdims=True), (16, LANES))


def sort_kernel(block_ref, mine_ref, side_ref):
    mine_ref[...] = pltpu.einshape("hbr->bhr", block_ref[:, 0:16, :])
    side_ref[...] = pltpu.einshape("hbr->bhr", block_ref[:, 16:32, :])


def fresh_kernel(side_ref, gain_ref, fresh_ref, slice_ref, piece_ref, row_s):
    heads, width, rank = side_ref.shape[1], 32, gain_ref.shape[1]
    square = jnp.zeros((16, width), F32)
    for k in range(heads):
        block = side_ref[:, k, width : 2 * width].astype(F32)
        row_s[:, k * width : (k + 1) * width] = block
        square += block * block
    mean = jnp.sum(square, axis=1, keepdims=True) / rank
    fresh = (row_s[...] * lax.rsqrt(mean + EPS) * gain_ref[...]).astype(BF16)
    fresh_ref[...] = fresh
    row_s[...] = fresh.astype(F32)
    tp = lax.axis_index("tp_0") * 2 + lax.axis_index("tp_1")
    kv = lax.axis_index("kv_0") * 4 + lax.axis_index("kv_1")
    slice_ref[...] = row_s[:, pl.ds(pl.multiple_of(tp * LANES, LANES), LANES)]
    column = (kv * 8 + tp) * 4
    base = column // LANES
    held = row_s[:, pl.ds(pl.multiple_of(base * LANES, LANES), LANES)]
    held = pltpu.roll(held, (LANES - (column - base * LANES)) % LANES, 1)
    piece_ref[...] = held.T[0:4, :].astype(BF16)


def values_kernel(order_ref, value_ref, out_ref):
    step = 64

    def turn(j, _):
        at = pl.ds(pl.multiple_of(j * step, step), step)
        out_ref[:, at, :] = pltpu.einshape("rhv->hrv", value_ref[at])
        return 0

    lax.fori_loop(0, value_ref.shape[0] // step, turn, 0)


def attend_kernel(scale, lengths_ref, *refs):
    pieces = refs[0:8]
    (side_ref, fresh_ref, rot_ref, value_hbm, cache_hbm, out_ref, own_ref) = refs[8:15]
    (q_s, cache_ref, value_ref, o_s, m_s, l_s, sems) = refs[15:]
    seqs, heads = 16, 32
    chunks = sems.shape[0] // 2
    per, group = seqs // chunks, heads // chunks
    cut = lambda ref, i, size: ref.at[pl.ds(i * size, size)]
    copies = fetch(
        [(cut(cache_hbm, i, per), cut(cache_ref, i, per)) for i in range(chunks)]
        + [(cut(value_hbm, i, group), cut(value_ref, i, group)) for i in range(chunks)],
        sems,
    )
    blocks, gap = q_s.shape[0], heads + 1

    chip, core = lax.axis_index("tp_0"), lax.axis_index("tp_1")
    kv = lax.axis_index("kv_0") * 4 + lax.axis_index("kv_1")
    first_pos = (kv * 8 + chip * 2 + core) * LANES
    for j in range(4):
        q_s[(chip ^ j) * 2 + core] = pieces[j][...]
        q_s[(chip ^ j) * 2 + 1 - core] = pieces[4 + j][...]
    position = first_pos + lane_ids(heads)
    for b in range(seqs):
        if b % per == 0:
            copies[b // per].wait()
        query = jnp.concatenate([q_s[n, b] for n in range(blocks)], axis=1)
        rope = side_ref[b][:, 0:32]
        past = cache_ref[b]
        scores = lax.dot_general(query, past, NT, preferred_element_type=F32)
        scores += jnp.dot(rope, rot_ref[b], preferred_element_type=F32)
        scores = scores * scale
        valid = position < lengths_ref[b]
        top = jnp.max(jnp.where(valid, scores, FLOOR), axis=1, keepdims=True)
        weights = jnp.where(valid, jnp.exp(scores - top), 0.0)
        total = jnp.sum(weights, axis=1, keepdims=True)
        rows = slice(b * gap, b * gap + heads)
        summed = jnp.dot(weights.astype(BF16), past, preferred_element_type=F32)
        for n in range(blocks):
            at = (n * seqs + b) * gap
            o_s[at : at + heads, :] = summed[:, n * LANES : (n + 1) * LANES]
        m_s[rows, :] = jnp.broadcast_to(top, (heads, LANES))
        l_s[rows, :] = jnp.broadcast_to(total, (heads, LANES))
    lane = lane_ids(seqs)
    for h in range(heads):
        if h % group == 0:
            copies[chunks + h // group].wait()
        latent = jnp.concatenate(
            [o_s[pl.ds(n * seqs * gap + h, seqs, stride=gap), :] for n in range(blocks)], axis=1
        ).astype(BF16)
        out_ref[h, 0:16, :] = jnp.dot(
            latent, value_ref[h], preferred_element_type=F32
        ).astype(BF16)
        stats = jnp.zeros((seqs, LANES), F32)
        for at, ref in ((0, m_s), (3, l_s)):
            left = ref[pl.ds(h, seqs, stride=gap), :]
            for n in range(3):
                piece = left.astype(BF16).astype(F32)
                stats = jnp.where(lane == at + n, piece, stats)
                left = left - piece
        out_ref[h, 16:32, :] = stats.astype(BF16)
    own_ref[...] = jnp.dot(fresh_ref[...], value_ref[kv], preferred_element_type=F32)


def gather_kernel(parts_ref, slice_ref, fresh_ref, out_ref, m_s, l_s):
    count = parts_ref.shape[0]
    lane = lane_ids(16)
    top = jnp.full((16, LANES), FLOOR, F32)
    for k in range(count):
        stats = parts_ref[k, 16:32, :].astype(F32)
        m = jnp.sum(jnp.where(lane < 3, stats, 0.0), axis=1, keepdims=True)
        l = jnp.sum(jnp.where((lane >= 3) & (lane < 6), stats, 0.0), axis=1, keepdims=True)
        m = jnp.broadcast_to(m, (16, LANES))
        m_s[k] = m
        l_s[k] = jnp.broadcast_to(l, (16, LANES))
        top = jnp.maximum(top, m)
    total = jnp.zeros((16, LANES), F32)
    summed = jnp.zeros((16, LANES), F32)
    for k in range(count):
        factor = jnp.exp(m_s[k] - top)
        total += factor * l_s[k]
        summed += factor * parts_ref[k, 0:16, :].astype(F32)
    own = jnp.sum(slice_ref[...] * fresh_ref[...], axis=1, keepdims=True)
    stats = jnp.where(lane == 0, top, jnp.where(lane == 1, total, own))
    for peer in range(out_ref.shape[0]):
        out_ref[peer, 0:16, :] = summed
        out_ref[peer, 16:32, :] = stats


def lane_of(stats, n):
    return jnp.sum(jnp.where(lane_ids(stats.shape[0]) == n, stats, 0.0), axis=1, keepdims=True)


def finish_kernel(scale, parts_ref, dot_ref, own_ref, weight_ref, out_ref):
    peers = range(parts_ref.shape[0])
    stats = [parts_ref[peer, 16:32, :] for peer in peers]
    tops = [lane_of(s, 0) for s in stats]
    own = (functools.reduce(jnp.add, [lane_of(s, 2) for s in stats]) + dot_ref[...]) * scale
    highest = functools.reduce(jnp.maximum, tops, own)
    total = jnp.exp(own - highest)
    summed = total * own_ref[...]
    for peer in peers:
        factor = jnp.exp(tops[peer] - highest)
        total += factor * lane_of(stats[peer], 1)
        summed += factor * parts_ref[peer, 0:16, :]
    head = (summed / total).astype(BF16)
    term = jnp.dot(head, weight_ref[...], preferred_element_type=F32).astype(BF16)
    for peer in range(out_ref.shape[0]):
        out_ref[peer] = term


def shards(
    tokens, norm_gain, w_query, w_latent, w_rotary, latent_gain, w_key_up, w_value_up, w_out,
    cache_latent, cache_rotary, lengths,
):
    seqs = tokens.shape[0]
    kv_count, tp_count = lax.axis_size(KV), lax.axis_size(TP)
    heads = kv_count
    rope_width = cache_rotary.shape[2]
    rank = cache_latent.shape[2]
    pos_dev = cache_latent.shape[1]
    model_width = tokens.shape[1] * tp_count
    out_cols = w_out.shape[1]
    score_scale = w_query.shape[2] ** (-0.5)
    sds = jax.ShapeDtypeStruct

    hbm = pl.BlockSpec(memory_space=pltpu.HBM)
    smem = pl.BlockSpec(memory_space=pltpu.SMEM)
    width = tokens.shape[1]
    query_width = w_query.shape[2]
    partial = pl.pallas_call(
        project_kernel,
        out_shape=sds((tp_count, 32, LANES), F32),
        in_specs=[hbm] * 5,
        out_specs=whole(1)[0],
        scratch_shapes=[
            pltpu.VMEM((seqs, width), BF16),
            pltpu.VMEM((1, width), F32),
            pltpu.VMEM((query_width, width), BF16),
            pltpu.VMEM((rope_width, width), BF16),
            pltpu.VMEM((rope_width, width), BF16),
            pltpu.VMEM((32, LANES), F32),
            pltpu.SemaphoreType.DMA((5,)),
        ],
    )(tokens, norm_gain[None], w_query[:, 0].T, w_latent.T, w_rotary.T)

    pair = lax.broadcasted_iota(jnp.int32, (1, LANES), 1) % (rope_width // 2)
    frequency = THETA ** (-(2 * pair).astype(F32) / rope_width)
    cosine, sine, key_up = pl.pallas_call(
        table_kernel,
        out_shape=(sds((seqs, LANES), F32),) * 2 + (sds((w_key_up.shape[2], LANES), BF16),),
        in_specs=[smem] + whole(2),
        out_specs=tuple(whole(3)),
        compiler_params=SMALL,
    )(lengths, frequency, w_key_up[:, 0].T)

    sums = lax.all_to_all(partial, TP, 0, 0, tiled=True)
    block, new_rotary, own_slice, rope_dot = pl.pallas_call(
        functools.partial(query_kernel, float(model_width)),
        out_shape=(
            sds((heads, 32, LANES), BF16),
            sds((seqs, rope_width), BF16),
            sds((seqs, LANES), F32),
            sds((seqs, LANES), F32),
        ),
        in_specs=whole(4),
        out_specs=tuple(whole(4)),
        compiler_params=SMALL,
    )(sums, cosine, sine, key_up)

    got = lax.all_to_all(block, KV, 0, 0, tiled=True)
    steps = 8
    value_up = pl.pallas_call(
        values_kernel,
        grid=(steps,),
        out_shape=sds((heads, rank, LANES), BF16),
        in_specs=[
            pl.BlockSpec((seqs, LANES), lambda i: (0, 0)),
            pl.BlockSpec((rank // steps, heads, LANES), lambda i: (i, 0, 0)),
        ],
        out_specs=pl.BlockSpec((heads, rank // steps, LANES), lambda i: (0, i, 0)),
    )(own_slice, w_value_up)
    got, value_up = lax.optimization_barrier((got, value_up))
    mine, side = pl.pallas_call(
        sort_kernel,
        out_shape=(sds((seqs, heads, LANES), BF16),) * 2,
        in_specs=whole(1),
        out_specs=tuple(whole(2)),
        compiler_params=SMALL,
    )(got)
    pieces = [swapped(mine, "tp_0", j) for j in (1, 2, 3)]

    new_latent, fresh_slice, latent_piece = pl.pallas_call(
        fresh_kernel,
        out_shape=(sds((seqs, rank), BF16), sds((seqs, LANES), F32), sds((4, seqs), BF16)),
        in_specs=whole(2),
        out_specs=tuple(whole(3)),
        scratch_shapes=[pltpu.VMEM((seqs, rank), F32)],
        compiler_params=SMALL,
    )(side, latent_gain[None])
    pieces = [mine] + pieces
    pieces = pieces + [swapped(piece, "tp_1", 1) for piece in pieces]

    pairs_gap = seqs * (heads + 1)
    values, own_value = pl.pallas_call(
        functools.partial(attend_kernel, score_scale),
        out_shape=(sds((heads, 32, LANES), BF16), sds((seqs, LANES), F32)),
        in_specs=[smem] + whole(11) + [hbm] * 2,
        out_specs=tuple(whole(2)),
        scratch_shapes=[
            pltpu.VMEM((rank // LANES, seqs, heads, LANES), BF16),
            pltpu.VMEM(cache_latent.shape, BF16),
            pltpu.VMEM((heads, rank, LANES), BF16),
            pltpu.VMEM((pairs_gap * (rank // LANES), LANES), F32),
            pltpu.VMEM((pairs_gap, LANES), F32),
            pltpu.VMEM((pairs_gap, LANES), F32),
            pltpu.SemaphoreType.DMA((8,)),
        ],
        compiler_params=pltpu.CompilerParams(vmem_limit_bytes=52 * 1024 * 1024),
    )(
        lengths, *pieces, side, new_latent, cache_rotary.transpose(0, 2, 1), value_up, cache_latent
    )

    arrived = lax.all_to_all(values, KV, 0, 0, tiled=True)
    states = pl.pallas_call(
        gather_kernel,
        out_shape=sds((tp_count, 32, LANES), F32),
        in_specs=whole(3),
        out_specs=whole(1)[0],
        scratch_shapes=[pltpu.VMEM((kv_count, 16, LANES), F32)] * 2,
        compiler_params=SMALL,
    )(arrived, own_slice, fresh_slice)
    states = lax.all_to_all(states, TP, 0, 0, tiled=True)
    terms = pl.pallas_call(
        functools.partial(finish_kernel, score_scale),
        out_shape=sds((kv_count, seqs, out_cols), BF16),
        in_specs=whole(4),
        out_specs=whole(1)[0],
        compiler_params=SMALL,
    )(states, rope_dot, own_value, w_out)
    terms = lax.all_to_all(terms, KV, 0, 0, tiled=True)
    mixed_out = jnp.sum(terms.astype(F32), axis=0).astype(BF16)
    return (mixed_out, latent_piece.T, new_rotary)


def solution(mesh):
    torus = Mesh(mesh.devices.reshape(8, 4, 4, 2), KV_TP)
    in_specs = (
        P(None, TP),
        P(TP),
        P(TP, KV, None),
        P(TP, KV),
        P(TP, None),
        P(),
        P(TP, KV, None),
        P(),
        P(KV, TP),
        P(None, KV_TP, None),
        P(None, KV_TP, None),
        P(),
    )
    out_specs = (P(None, TP), P(None, KV_TP), P())
    return jax.shard_map(
        shards, mesh=torus, in_specs=in_specs, out_specs=out_specs, check_vma=False
    )
```

```python
import functools

import jax
import jax.numpy as jnp
from jax import lax
from jax.experimental import pallas as pl
from jax.experimental.pallas import tpu as pltpu
from jax.sharding import Mesh
from jax.sharding import PartitionSpec as P

KV = ("kv_0", "kv_1")
TP = ("tp_0", "tp_1")
KV_TP = ("kv_0", "kv_1", "tp_0", "tp_1")


THETA = 10000.0
EPS = 1e-06
F32 = jnp.float32
BF16 = jnp.bfloat16
SMALL = pltpu.CompilerParams(vmem_limit_bytes=4 * 1024 * 1024)
FLOOR = -(2.0**127)
LANES = 128
NT = (((1,), (1,)), ((), ()))


def whole(count):
    return [pl.BlockSpec(memory_space=pltpu.VMEM)] * count


def lane_ids(rows):
    return lax.broadcasted_iota(jnp.int32, (rows, LANES), 1)


def swapped(value, axis, step):
    count = lax.axis_size(axis)
    return lax.ppermute(value, axis, [(i, i ^ step) for i in range(count)])


def fetch(pairs, sems):
    copies = [pltpu.make_async_copy(src, dst, sems.at[i]) for i, (src, dst) in enumerate(pairs)]
    for copy in copies:
        copy.start()
    return copies


def project_kernel(
    tokens_hbm, gain_hbm, query_hbm, latent_hbm, rotary_hbm, out_ref,
    tokens_s, gain_s, query_s, latent_s, rotary_s, sum_s, sems,
):
    copies = fetch(
        [
            (tokens_hbm, tokens_s), (gain_hbm, gain_s), (query_hbm, query_s),
            (latent_hbm, latent_s), (rotary_hbm, rotary_s),
        ],
        sems,
    )
    for copy in copies:
        copy.wait()
    tokens = tokens_s[...].astype(F32)
    scaled = (tokens * gain_s[...]).astype(BF16)
    squares = jnp.sum(tokens * tokens, axis=1, keepdims=True)
    sum_s[0:16, 0:96] = lax.dot_general(scaled, query_s[...], NT, preferred_element_type=F32)
    sum_s[0:16, 96:128] = lax.dot_general(scaled, latent_s[...], NT, preferred_element_type=F32)
    sum_s[16:32, :] = jnp.broadcast_to(squares, (16, LANES))
    sum_s[16:32, 0:32] = lax.dot_general(scaled, rotary_s[...], NT, preferred_element_type=F32)
    for peer in range(out_ref.shape[0]):
        out_ref[peer] = sum_s[...]


def table_kernel(
    lengths_ref, frequency_ref, key_in_ref, rot_in_ref, gain_in_ref,
    cos_ref, sin_ref, limit_ref, key_ref, rot_ref, gain_ref,
):
    row = lax.broadcasted_iota(jnp.int32, (16, LANES), 0)
    position = jnp.zeros((16, LANES), jnp.int32)
    for b in range(16):
        position = jnp.where(row == b, lengths_ref[b], position)
    angles = position.astype(F32) * frequency_ref[...]
    cos_ref[...] = jnp.cos(angles)
    sin_ref[...] = jnp.sin(angles)
    limit_ref[...] = position
    key_ref[...] = key_in_ref[...]
    rot_ref[...] = rot_in_ref[...]
    gain_ref[...] = gain_in_ref[...]


def query_kernel(
    model_width, parts_ref, cos_ref, sin_ref, key_ref,
    block_ref, rotary_ref, slice_ref, dot_ref,
):
    total = parts_ref[0]
    for peer in range(1, parts_ref.shape[0]):
        total = total + parts_ref[peer]
    lane = lane_ids(16)
    low = (lane & 31) < 16
    first, second = total[0:16], total[16:32]
    squares = jnp.sum(jnp.where(lane == 64, second, 0.0), axis=1, keepdims=True)
    inverse = lax.rsqrt(squares / model_width + EPS)

    def rotated(v):
        turned = jnp.where(low, -pltpu.roll(v, LANES - 16, 1), pltpu.roll(v, 16, 1))
        return v * cos_ref[...] + turned * sin_ref[...]

    query = (first * inverse).astype(BF16)
    query_f = query.astype(F32)
    rope = rotated(query_f)
    fresh = rotated(second * inverse).astype(BF16)
    latent_query = jnp.dot(query[:, 0:64], key_ref[...], preferred_element_type=F32).astype(BF16)
    side = jnp.where(lane < 96, rope, query_f)
    side = pltpu.roll(jnp.where(lane < 64, 0.0, side), 64, 1).astype(BF16)
    for peer in range(block_ref.shape[0]):
        block_ref[peer, 0:16, :] = latent_query
        block_ref[peer, 16:32, :] = side
    rotary_ref[...] = fresh[:, 0:32]
    slice_ref[...] = latent_query.astype(F32)
    both = jnp.where(lane < 32, side.astype(F32) * fresh.astype(F32), 0.0)
    dot_ref[...] = jnp.broadcast_to(jnp.sum(both, axis=1, keepdims=True), (16, LANES))


def sort_kernel(block_ref, mine_ref, side_ref):
    mine_ref[...] = pltpu.einshape("hbr->bhr", block_ref[:, 0:16, :])
    side_ref[...] = pltpu.einshape("hbr->bhr", block_ref[:, 16:32, :])


def fresh_kernel(side_ref, gain_ref, fresh_ref, slice_ref, piece_ref, row_s):
    heads, width, rank = side_ref.shape[1], 32, gain_ref.shape[1]
    square = jnp.zeros((16, width), F32)
    for k in range(heads):
        block = side_ref[:, k, width : 2 * width].astype(F32)
        row_s[:, k * width : (k + 1) * width] = block
        square += block * block
    mean = jnp.sum(square, axis=1, keepdims=True) / rank
    fresh = (row_s[...] * lax.rsqrt(mean + EPS) * gain_ref[...]).astype(BF16)
    fresh_ref[...] = fresh
    row_s[...] = fresh.astype(F32)
    tp = lax.axis_index("tp_0") * 2 + lax.axis_index("tp_1")
    kv = lax.axis_index("kv_0") * 4 + lax.axis_index("kv_1")
    slice_ref[...] = row_s[:, pl.ds(pl.multiple_of(tp * LANES, LANES), LANES)]
    column = (kv * 8 + tp) * 4
    base = column // LANES
    held = row_s[:, pl.ds(pl.multiple_of(base * LANES, LANES), LANES)]
    held = pltpu.roll(held, (LANES - (column - base * LANES)) % LANES, 1)
    piece_ref[...] = held.T[0:4, :].astype(BF16)


def attend_kernel(scale, limit_ref, *refs):
    pieces = refs[0:8]
    (side_ref, fresh_ref, rot_ref, value_hbm, cache_hbm, out_ref, own_ref) = refs[8:15]
    (q_s, cache_ref, value_ref, spread_s, o_s, m_s, l_s, sems) = refs[15:]
    seqs, heads = 16, 32
    chunks = sems.shape[0] // 2
    depth = value_ref.shape[0]
    per, part = seqs // chunks, depth // chunks
    cut = lambda ref, i, size: ref.at[pl.ds(i * size, size)]
    copies = fetch(
        [(cut(cache_hbm, i, per), cut(cache_ref, i, per)) for i in range(chunks)]
        + [(cut(value_hbm, i, part), cut(value_ref, i, part)) for i in range(chunks)],
        sems,
    )
    blocks, gap = q_s.shape[0], heads + 1

    chip, core = lax.axis_index("tp_0"), lax.axis_index("tp_1")
    kv = lax.axis_index("kv_0") * 4 + lax.axis_index("kv_1")
    first_pos = (kv * 8 + chip * 2 + core) * LANES
    for j in range(4):
        q_s[(chip ^ j) * 2 + core] = pieces[j][...]
        q_s[(chip ^ j) * 2 + 1 - core] = pieces[4 + j][...]
    position = first_pos + lane_ids(heads)
    for b in range(seqs):
        if b % per == 0:
            copies[b // per].wait()
        query = jnp.concatenate([q_s[n, b] for n in range(blocks)], axis=1)
        rope = side_ref[b][:, 0:32]
        past = cache_ref[b]
        scores = lax.dot_general(query, past, NT, preferred_element_type=F32)
        scores += jnp.dot(rope, rot_ref[b], preferred_element_type=F32)
        scores = scores * scale
        valid = position < limit_ref[b : b + 1, :]
        top = jnp.max(jnp.where(valid, scores, FLOOR), axis=1, keepdims=True)
        weights = jnp.where(valid, jnp.exp(scores - top), 0.0)
        total = jnp.sum(weights, axis=1, keepdims=True)
        rows = slice(b * gap, b * gap + heads)
        summed = jnp.dot(weights.astype(BF16), past, preferred_element_type=F32)
        for n in range(blocks):
            at = (n * seqs + b) * gap
            o_s[at : at + heads, :] = summed[:, n * LANES : (n + 1) * LANES]
        m_s[rows, :] = jnp.broadcast_to(top, (heads, LANES))
        l_s[rows, :] = jnp.broadcast_to(total, (heads, LANES))
    for i in range(chunks):
        copies[chunks + i].wait()

        def spread(step, _):
            for n in range(8):
                r = i * part + step * 8 + n
                spread_s[pl.ds(r * gap, heads), :] = value_ref[r].astype(F32)
            return 0

        lax.fori_loop(0, part // 8, spread, 0)
    lane = lane_ids(seqs)
    for h in range(heads):
        latent = jnp.concatenate(
            [o_s[pl.ds(n * seqs * gap + h, seqs, stride=gap), :] for n in range(blocks)], axis=1
        ).astype(BF16)
        weight = spread_s[pl.ds(h, depth, stride=gap), :].astype(BF16)
        out_ref[h, 0:16, :] = jnp.dot(latent, weight, preferred_element_type=F32).astype(BF16)
        stats = jnp.zeros((seqs, LANES), F32)
        for at, ref in ((0, m_s), (3, l_s)):
            left = ref[pl.ds(h, seqs, stride=gap), :]
            for n in range(3):
                piece = left.astype(BF16).astype(F32)
                stats = jnp.where(lane == at + n, piece, stats)
                left = left - piece
        out_ref[h, 16:32, :] = stats.astype(BF16)
    weight = spread_s[pl.ds(kv, depth, stride=gap), :].astype(BF16)
    own_ref[...] = jnp.dot(fresh_ref[...], weight, preferred_element_type=F32)


def gather_kernel(parts_ref, slice_ref, fresh_ref, out_ref, m_s, l_s):
    count = parts_ref.shape[0]
    lane = lane_ids(16)
    top = jnp.full((16, LANES), FLOOR, F32)
    for k in range(count):
        stats = parts_ref[k, 16:32, :].astype(F32)
        m = jnp.sum(jnp.where(lane < 3, stats, 0.0), axis=1, keepdims=True)
        l = jnp.sum(jnp.where((lane >= 3) & (lane < 6), stats, 0.0), axis=1, keepdims=True)
        m = jnp.broadcast_to(m, (16, LANES))
        m_s[k] = m
        l_s[k] = jnp.broadcast_to(l, (16, LANES))
        top = jnp.maximum(top, m)
    total = jnp.zeros((16, LANES), F32)
    summed = jnp.zeros((16, LANES), F32)
    for k in range(count):
        factor = jnp.exp(m_s[k] - top)
        total += factor * l_s[k]
        summed += factor * parts_ref[k, 0:16, :].astype(F32)
    own = jnp.sum(slice_ref[...] * fresh_ref[...], axis=1, keepdims=True)
    stats = jnp.where(lane == 0, top, jnp.where(lane == 1, total, own))
    for peer in range(out_ref.shape[0]):
        out_ref[peer, 0:16, :] = summed
        out_ref[peer, 16:32, :] = stats


def lane_of(stats, n):
    return jnp.sum(jnp.where(lane_ids(stats.shape[0]) == n, stats, 0.0), axis=1, keepdims=True)


def finish_kernel(scale, parts_ref, dot_ref, own_ref, weight_ref, out_ref):
    peers = range(parts_ref.shape[0])
    stats = [parts_ref[peer, 16:32, :] for peer in peers]
    tops = [lane_of(s, 0) for s in stats]
    own = (functools.reduce(jnp.add, [lane_of(s, 2) for s in stats]) + dot_ref[...]) * scale
    highest = functools.reduce(jnp.maximum, tops, own)
    total = jnp.exp(own - highest)
    summed = total * own_ref[...]
    for peer in peers:
        factor = jnp.exp(tops[peer] - highest)
        total += factor * lane_of(stats[peer], 1)
        summed += factor * parts_ref[peer, 0:16, :]
    head = (summed / total).astype(BF16)
    term = jnp.dot(head, weight_ref[...], preferred_element_type=F32).astype(BF16)
    for peer in range(out_ref.shape[0]):
        for n in range(4):
            out_ref[peer, 16 * n : 16 * (n + 1), :] = term[:, LANES * n : LANES * (n + 1)]


def total_kernel(terms_ref, out_ref):
    for n in range(4):
        rows = slice(16 * n, 16 * (n + 1))
        total = terms_ref[0, rows, :].astype(F32)
        for k in range(1, terms_ref.shape[0]):
            total += terms_ref[k, rows, :].astype(F32)
        out_ref[:, LANES * n : LANES * (n + 1)] = total.astype(BF16)


def shards(
    tokens, norm_gain, w_query, w_latent, w_rotary, latent_gain, w_key_up, w_value_up, w_out,
    cache_latent, cache_rotary, lengths,
):
    seqs = tokens.shape[0]
    kv_count, tp_count = lax.axis_size(KV), lax.axis_size(TP)
    heads = kv_count
    rope_width = cache_rotary.shape[2]
    rank = cache_latent.shape[2]
    pos_dev = cache_latent.shape[1]
    model_width = tokens.shape[1] * tp_count
    out_cols = w_out.shape[1]
    score_scale = w_query.shape[2] ** (-0.5)
    sds = jax.ShapeDtypeStruct

    hbm = pl.BlockSpec(memory_space=pltpu.HBM)
    smem = pl.BlockSpec(memory_space=pltpu.SMEM)
    width = tokens.shape[1]
    query_width = w_query.shape[2]
    partial = pl.pallas_call(
        project_kernel,
        out_shape=sds((tp_count, 32, LANES), F32),
        in_specs=[hbm] * 5,
        out_specs=whole(1)[0],
        scratch_shapes=[
            pltpu.VMEM((seqs, width), BF16),
            pltpu.VMEM((1, width), F32),
            pltpu.VMEM((query_width, width), BF16),
            pltpu.VMEM((rope_width, width), BF16),
            pltpu.VMEM((rope_width, width), BF16),
            pltpu.VMEM((32, LANES), F32),
            pltpu.SemaphoreType.DMA((5,)),
        ],
    )(tokens, norm_gain[None], w_query[:, 0].T, w_latent.T, w_rotary.T)

    pair = lax.broadcasted_iota(jnp.int32, (1, LANES), 1) % (rope_width // 2)
    frequency = THETA ** (-(2 * pair).astype(F32) / rope_width)
    cosine, sine, limits, key_up, rotary_keys, gain = pl.pallas_call(
        table_kernel,
        out_shape=(
            sds((seqs, LANES), F32),
            sds((seqs, LANES), F32),
            sds((seqs, LANES), jnp.int32),
            sds((w_key_up.shape[2], LANES), BF16),
            sds((seqs, rope_width, pos_dev), BF16),
            sds((1, rank), F32),
        ),
        in_specs=[smem] + whole(4),
        out_specs=tuple(whole(6)),
        compiler_params=SMALL,
    )(
        lengths, frequency, w_key_up[:, 0].T, cache_rotary.transpose(0, 2, 1), latent_gain[None]
    )

    sums = lax.all_to_all(partial, TP, 0, 0, tiled=True)
    block, new_rotary, own_slice, rope_dot = pl.pallas_call(
        functools.partial(query_kernel, float(model_width)),
        out_shape=(
            sds((heads, 32, LANES), BF16),
            sds((seqs, rope_width), BF16),
            sds((seqs, LANES), F32),
            sds((seqs, LANES), F32),
        ),
        in_specs=whole(4),
        out_specs=tuple(whole(4)),
        compiler_params=SMALL,
    )(sums, cosine, sine, key_up)

    got = lax.all_to_all(block, KV, 0, 0, tiled=True)
    mine, side = pl.pallas_call(
        sort_kernel,
        out_shape=(sds((seqs, heads, LANES), BF16),) * 2,
        in_specs=whole(1),
        out_specs=tuple(whole(2)),
        compiler_params=SMALL,
    )(got)
    pieces = [swapped(mine, "tp_0", j) for j in (1, 2, 3)]

    new_latent, fresh_slice, latent_piece = pl.pallas_call(
        fresh_kernel,
        out_shape=(sds((seqs, rank), BF16), sds((seqs, LANES), F32), sds((4, seqs), BF16)),
        in_specs=whole(2),
        out_specs=tuple(whole(3)),
        scratch_shapes=[pltpu.VMEM((seqs, rank), F32)],
        compiler_params=SMALL,
    )(side, gain)
    pieces = [mine] + pieces
    pieces = pieces + [swapped(piece, "tp_1", 1) for piece in pieces]

    pairs_gap = seqs * (heads + 1)
    values, own_value = pl.pallas_call(
        functools.partial(attend_kernel, score_scale),
        out_shape=(sds((heads, 32, LANES), BF16), sds((seqs, LANES), F32)),
        in_specs=whole(12) + [hbm] * 2,
        out_specs=tuple(whole(2)),
        scratch_shapes=[
            pltpu.VMEM((rank // LANES, seqs, heads, LANES), BF16),
            pltpu.VMEM(cache_latent.shape, BF16),
            pltpu.VMEM(w_value_up.shape, BF16),
            pltpu.VMEM((rank * (heads + 1), LANES), F32),
            pltpu.VMEM((pairs_gap * (rank // LANES), LANES), F32),
            pltpu.VMEM((pairs_gap, LANES), F32),
            pltpu.VMEM((pairs_gap, LANES), F32),
            pltpu.SemaphoreType.DMA((8,)),
        ],
        compiler_params=pltpu.CompilerParams(vmem_limit_bytes=52 * 1024 * 1024),
    )(
        limits, *pieces, side, new_latent, rotary_keys, w_value_up, cache_latent
    )

    arrived = lax.all_to_all(values, KV, 0, 0, tiled=True)
    states = pl.pallas_call(
        gather_kernel,
        out_shape=sds((tp_count, 32, LANES), F32),
        in_specs=whole(3),
        out_specs=whole(1)[0],
        scratch_shapes=[pltpu.VMEM((kv_count, 16, LANES), F32)] * 2,
        compiler_params=SMALL,
    )(arrived, own_slice, fresh_slice)
    states = lax.all_to_all(states, TP, 0, 0, tiled=True)
    terms = pl.pallas_call(
        functools.partial(finish_kernel, score_scale),
        out_shape=sds((kv_count, seqs * out_cols // LANES, LANES), BF16),
        in_specs=whole(4),
        out_specs=whole(1)[0],
        compiler_params=SMALL,
    )(states, rope_dot, own_value, w_out)
    terms = lax.all_to_all(terms, KV, 0, 0, tiled=True)
    mixed_out = pl.pallas_call(
        total_kernel,
        out_shape=sds((seqs, out_cols), BF16),
        in_specs=whole(1),
        out_specs=whole(1)[0],
        compiler_params=SMALL,
    )(terms)
    return (mixed_out, latent_piece.T, new_rotary)


def solution(mesh):
    torus = Mesh(mesh.devices.reshape(8, 4, 4, 2), KV_TP)
    in_specs = (
        P(None, TP),
        P(TP),
        P(TP, KV, None),
        P(TP, KV),
        P(TP, None),
        P(),
        P(TP, KV, None),
        P(),
        P(KV, TP),
        P(None, KV_TP, None),
        P(None, KV_TP, None),
        P(),
    )
    out_specs = (P(None, TP), P(None, KV_TP), P())
    return jax.shard_map(
        shards, mesh=torus, in_specs=in_specs, out_specs=out_specs, check_vma=False
    )
```

```python
import functools

import jax
import jax.numpy as jnp
from jax import lax
from jax.experimental import pallas as pl
from jax.experimental.pallas import tpu as pltpu
from jax.sharding import Mesh
from jax.sharding import PartitionSpec as P

KV = ("kv_0", "kv_1")
TP = ("tp_0", "tp_1")
KV_TP = ("kv_0", "kv_1", "tp_0", "tp_1")


THETA = 10000.0
EPS = 1e-06
F32 = jnp.float32
BF16 = jnp.bfloat16
SMALL = pltpu.CompilerParams(vmem_limit_bytes=4 * 1024 * 1024)
FLOOR = -(2.0**127)
LANES = 128
NT = (((1,), (1,)), ((), ()))


def whole(count):
    return [pl.BlockSpec(memory_space=pltpu.VMEM)] * count


def lane_ids(rows):
    return lax.broadcasted_iota(jnp.int32, (rows, LANES), 1)


def swapped(value, axis, step):
    count = lax.axis_size(axis)
    return lax.ppermute(value, axis, [(i, i ^ step) for i in range(count)])


def fetch(pairs, sems):
    copies = [pltpu.make_async_copy(src, dst, sems.at[i]) for i, (src, dst) in enumerate(pairs)]
    for copy in copies:
        copy.start()
    return copies


def project_kernel(
    tokens_hbm, gain_hbm, query_hbm, latent_hbm, rotary_hbm, out_ref,
    tokens_s, gain_s, query_s, latent_s, rotary_s, sum_s, sems,
):
    copies = fetch(
        [
            (tokens_hbm, tokens_s), (gain_hbm, gain_s), (query_hbm, query_s),
            (latent_hbm, latent_s), (rotary_hbm, rotary_s),
        ],
        sems,
    )
    for copy in copies:
        copy.wait()
    tokens = tokens_s[...].astype(F32)
    scaled = (tokens * gain_s[...]).astype(BF16)
    squares = jnp.sum(tokens * tokens, axis=1, keepdims=True)
    sum_s[0:16, 0:96] = lax.dot_general(scaled, query_s[...], NT, preferred_element_type=F32)
    sum_s[0:16, 96:128] = lax.dot_general(scaled, latent_s[...], NT, preferred_element_type=F32)
    sum_s[16:32, :] = jnp.broadcast_to(squares, (16, LANES))
    sum_s[16:32, 0:32] = lax.dot_general(scaled, rotary_s[...], NT, preferred_element_type=F32)
    for peer in range(out_ref.shape[0]):
        out_ref[peer] = sum_s[...]


def table_kernel(
    lengths_ref, frequency_ref, key_in_ref, rot_in_ref, gain_in_ref,
    cos_ref, sin_ref, limit_ref, key_ref, rot_ref, gain_ref,
):
    row = lax.broadcasted_iota(jnp.int32, (16, LANES), 0)
    position = jnp.zeros((16, LANES), jnp.int32)
    for b in range(16):
        position = jnp.where(row == b, lengths_ref[b], position)
    angles = position.astype(F32) * frequency_ref[...]
    cos_ref[...] = jnp.cos(angles)
    sin_ref[...] = jnp.sin(angles)
    limit_ref[...] = position
    key_ref[...] = key_in_ref[...]
    rot_ref[...] = rot_in_ref[...]
    gain_ref[...] = gain_in_ref[...]


def query_kernel(
    model_width, parts_ref, cos_ref, sin_ref, key_ref,
    block_ref, rotary_ref, slice_ref, dot_ref,
):
    total = parts_ref[0]
    for peer in range(1, parts_ref.shape[0]):
        total = total + parts_ref[peer]
    lane = lane_ids(16)
    low = (lane & 31) < 16
    first, second = total[0:16], total[16:32]
    squares = jnp.sum(jnp.where(lane == 64, second, 0.0), axis=1, keepdims=True)
    inverse = lax.rsqrt(squares / model_width + EPS)

    def rotated(v):
        turned = jnp.where(low, -pltpu.roll(v, LANES - 16, 1), pltpu.roll(v, 16, 1))
        return v * cos_ref[...] + turned * sin_ref[...]

    query = (first * inverse).astype(BF16)
    query_f = query.astype(F32)
    rope = rotated(query_f)
    fresh = rotated(second * inverse).astype(BF16)
    latent_query = jnp.dot(query[:, 0:64], key_ref[...], preferred_element_type=F32).astype(BF16)
    side = jnp.where(lane < 96, rope, query_f)
    side = pltpu.roll(jnp.where(lane < 64, 0.0, side), 64, 1).astype(BF16)
    for peer in range(block_ref.shape[0]):
        block_ref[peer, 0:16, :] = latent_query
        block_ref[peer, 16:32, :] = side
    rotary_ref[...] = fresh[:, 0:32]
    slice_ref[...] = latent_query.astype(F32)
    both = jnp.where(lane < 32, side.astype(F32) * fresh.astype(F32), 0.0)
    dot_ref[...] = jnp.broadcast_to(jnp.sum(both, axis=1, keepdims=True), (16, LANES))


def sort_kernel(block_ref, mine_ref, side_ref):
    mine_ref[...] = pltpu.einshape("hbr->bhr", block_ref[:, 0:16, :])
    side_ref[...] = pltpu.einshape("hbr->bhr", block_ref[:, 16:32, :])


def fresh_kernel(side_ref, gain_ref, fresh_ref, slice_ref, piece_ref, row_s):
    heads, width, rank = side_ref.shape[1], 32, gain_ref.shape[1]
    square = jnp.zeros((16, width), F32)
    for k in range(heads):
        block = side_ref[:, k, width : 2 * width].astype(F32)
        row_s[:, k * width : (k + 1) * width] = block
        square += block * block
    mean = jnp.sum(square, axis=1, keepdims=True) / rank
    fresh = (row_s[...] * lax.rsqrt(mean + EPS) * gain_ref[...]).astype(BF16)
    fresh_ref[...] = fresh
    row_s[...] = fresh.astype(F32)
    tp = lax.axis_index("tp_0") * 2 + lax.axis_index("tp_1")
    kv = lax.axis_index("kv_0") * 4 + lax.axis_index("kv_1")
    slice_ref[...] = row_s[:, pl.ds(pl.multiple_of(tp * LANES, LANES), LANES)]
    column = (kv * 8 + tp) * 4
    base = column // LANES
    held = row_s[:, pl.ds(pl.multiple_of(base * LANES, LANES), LANES)]
    held = pltpu.roll(held, (LANES - (column - base * LANES)) % LANES, 1)
    piece_ref[...] = held.T[0:4, :].astype(BF16)


def attend_kernel(scale, limit_ref, *refs):
    pieces = refs[0:8]
    (side_ref, fresh_ref, rot_ref, value_hbm, cache_hbm, out_ref, own_ref) = refs[8:15]
    (q_s, cache_ref, value_ref, spread_s, o_s, m_s, l_s, sems) = refs[15:]
    seqs, heads = 16, 32
    chunks = sems.shape[0] // 2
    depth = value_ref.shape[0]
    per, part = seqs // chunks, depth // chunks
    cut = lambda ref, i, size: ref.at[pl.ds(i * size, size)]
    copies = fetch(
        [(cut(cache_hbm, i, per), cut(cache_ref, i, per)) for i in range(chunks)]
        + [(cut(value_hbm, i, part), cut(value_ref, i, part)) for i in range(chunks)],
        sems,
    )
    blocks, gap = q_s.shape[0], heads + 1

    chip, core = lax.axis_index("tp_0"), lax.axis_index("tp_1")
    kv = lax.axis_index("kv_0") * 4 + lax.axis_index("kv_1")
    first_pos = (kv * 8 + chip * 2 + core) * LANES
    for j in range(4):
        q_s[(chip ^ j) * 2 + core] = pieces[j][...]
        q_s[(chip ^ j) * 2 + 1 - core] = pieces[4 + j][...]
    group = 8
    for first in range(0, seqs, group):
        members = range(first, first + group)
        for i in range(first // per, (first + group) // per):
            copies[i].wait()
        scores = []
        for b in members:
            query = jnp.concatenate([q_s[n, b] for n in range(blocks)], axis=1)
            term = lax.dot_general(query, cache_ref[b], NT, preferred_element_type=F32)
            term += jnp.dot(side_ref[b][:, 0:32], rot_ref[b], preferred_element_type=F32)
            scores.append(term)
        scores = jnp.concatenate(scores, axis=0) * scale
        limit = jnp.concatenate(
            [jnp.broadcast_to(limit_ref[b : b + 1, :], (heads, LANES)) for b in members], axis=0
        )
        valid = first_pos + lane_ids(heads * group) < limit
        top = jnp.max(jnp.where(valid, scores, FLOOR), axis=1, keepdims=True)
        weights = jnp.where(valid, jnp.exp(scores - top), 0.0)
        total = jnp.sum(weights, axis=1, keepdims=True)
        weights = weights.astype(BF16)
        for k, b in enumerate(members):
            part_rows = slice(k * heads, (k + 1) * heads)
            rows = slice(b * gap, b * gap + heads)
            summed = jnp.dot(weights[part_rows], cache_ref[b], preferred_element_type=F32)
            for n in range(blocks):
                at = (n * seqs + b) * gap
                o_s[at : at + heads, :] = summed[:, n * LANES : (n + 1) * LANES]
            m_s[rows, :] = jnp.broadcast_to(top[part_rows], (heads, LANES))
            l_s[rows, :] = jnp.broadcast_to(total[part_rows], (heads, LANES))
    for i in range(chunks):
        copies[chunks + i].wait()

        def spread(step, _):
            for n in range(8):
                r = i * part + step * 8 + n
                spread_s[pl.ds(r * gap, heads), :] = value_ref[r].astype(F32)
            return 0

        lax.fori_loop(0, part // 8, spread, 0)
    lane = lane_ids(seqs)
    for h in range(heads):
        latent = jnp.concatenate(
            [o_s[pl.ds(n * seqs * gap + h, seqs, stride=gap), :] for n in range(blocks)], axis=1
        ).astype(BF16)
        weight = spread_s[pl.ds(h, depth, stride=gap), :].astype(BF16)
        out_ref[h, 0:16, :] = jnp.dot(latent, weight, preferred_element_type=F32).astype(BF16)
        stats = jnp.zeros((seqs, LANES), F32)
        for at, ref in ((0, m_s), (3, l_s)):
            left = ref[pl.ds(h, seqs, stride=gap), :]
            for n in range(3):
                piece = left.astype(BF16).astype(F32)
                stats = jnp.where(lane == at + n, piece, stats)
                left = left - piece
        out_ref[h, 16:32, :] = stats.astype(BF16)
    weight = spread_s[pl.ds(kv, depth, stride=gap), :].astype(BF16)
    own_ref[...] = jnp.dot(fresh_ref[...], weight, preferred_element_type=F32)


def gather_kernel(parts_ref, slice_ref, fresh_ref, out_ref, m_s, l_s):
    count = parts_ref.shape[0]
    lane = lane_ids(16)
    top = jnp.full((16, LANES), FLOOR, F32)
    for k in range(count):
        stats = parts_ref[k, 16:32, :].astype(F32)
        m = jnp.sum(jnp.where(lane < 3, stats, 0.0), axis=1, keepdims=True)
        l = jnp.sum(jnp.where((lane >= 3) & (lane < 6), stats, 0.0), axis=1, keepdims=True)
        m = jnp.broadcast_to(m, (16, LANES))
        m_s[k] = m
        l_s[k] = jnp.broadcast_to(l, (16, LANES))
        top = jnp.maximum(top, m)
    total = jnp.zeros((16, LANES), F32)
    summed = jnp.zeros((16, LANES), F32)
    for k in range(count):
        factor = jnp.exp(m_s[k] - top)
        total += factor * l_s[k]
        summed += factor * parts_ref[k, 0:16, :].astype(F32)
    own = jnp.sum(slice_ref[...] * fresh_ref[...], axis=1, keepdims=True)
    stats = jnp.where(lane == 0, top, jnp.where(lane == 1, total, own))
    for peer in range(out_ref.shape[0]):
        out_ref[peer, 0:16, :] = summed
        out_ref[peer, 16:32, :] = stats


def lane_of(stats, n):
    return jnp.sum(jnp.where(lane_ids(stats.shape[0]) == n, stats, 0.0), axis=1, keepdims=True)


def finish_kernel(scale, parts_ref, dot_ref, own_ref, weight_ref, out_ref):
    peers = range(parts_ref.shape[0])
    stats = [parts_ref[peer, 16:32, :] for peer in peers]
    tops = [lane_of(s, 0) for s in stats]
    own = (functools.reduce(jnp.add, [lane_of(s, 2) for s in stats]) + dot_ref[...]) * scale
    highest = functools.reduce(jnp.maximum, tops, own)
    total = jnp.exp(own - highest)
    summed = total * own_ref[...]
    for peer in peers:
        factor = jnp.exp(tops[peer] - highest)
        total += factor * lane_of(stats[peer], 1)
        summed += factor * parts_ref[peer, 0:16, :]
    head = (summed / total).astype(BF16)
    term = jnp.dot(head, weight_ref[...], preferred_element_type=F32).astype(BF16)
    for peer in range(out_ref.shape[0]):
        for n in range(4):
            out_ref[peer, 16 * n : 16 * (n + 1), :] = term[:, LANES * n : LANES * (n + 1)]


def total_kernel(terms_ref, out_ref):
    for n in range(4):
        rows = slice(16 * n, 16 * (n + 1))
        total = terms_ref[0, rows, :].astype(F32)
        for k in range(1, terms_ref.shape[0]):
            total += terms_ref[k, rows, :].astype(F32)
        out_ref[:, LANES * n : LANES * (n + 1)] = total.astype(BF16)


def shards(
    tokens, norm_gain, w_query, w_latent, w_rotary, latent_gain, w_key_up, w_value_up, w_out,
    cache_latent, cache_rotary, lengths,
):
    seqs = tokens.shape[0]
    kv_count, tp_count = lax.axis_size(KV), lax.axis_size(TP)
    heads = kv_count
    rope_width = cache_rotary.shape[2]
    rank = cache_latent.shape[2]
    pos_dev = cache_latent.shape[1]
    model_width = tokens.shape[1] * tp_count
    out_cols = w_out.shape[1]
    score_scale = w_query.shape[2] ** (-0.5)
    sds = jax.ShapeDtypeStruct

    hbm = pl.BlockSpec(memory_space=pltpu.HBM)
    smem = pl.BlockSpec(memory_space=pltpu.SMEM)
    width = tokens.shape[1]
    query_width = w_query.shape[2]
    partial = pl.pallas_call(
        project_kernel,
        out_shape=sds((tp_count, 32, LANES), F32),
        in_specs=[hbm] * 5,
        out_specs=whole(1)[0],
        scratch_shapes=[
            pltpu.VMEM((seqs, width), BF16),
            pltpu.VMEM((1, width), F32),
            pltpu.VMEM((query_width, width), BF16),
            pltpu.VMEM((rope_width, width), BF16),
            pltpu.VMEM((rope_width, width), BF16),
            pltpu.VMEM((32, LANES), F32),
            pltpu.SemaphoreType.DMA((5,)),
        ],
    )(tokens, norm_gain[None], w_query[:, 0].T, w_latent.T, w_rotary.T)

    pair = lax.broadcasted_iota(jnp.int32, (1, LANES), 1) % (rope_width // 2)
    frequency = THETA ** (-(2 * pair).astype(F32) / rope_width)
    cosine, sine, limits, key_up, rotary_keys, gain = pl.pallas_call(
        table_kernel,
        out_shape=(
            sds((seqs, LANES), F32),
            sds((seqs, LANES), F32),
            sds((seqs, LANES), jnp.int32),
            sds((w_key_up.shape[2], LANES), BF16),
            sds((seqs, rope_width, pos_dev), BF16),
            sds((1, rank), F32),
        ),
        in_specs=[smem] + whole(4),
        out_specs=tuple(whole(6)),
        compiler_params=SMALL,
    )(
        lengths, frequency, w_key_up[:, 0].T, cache_rotary.transpose(0, 2, 1), latent_gain[None]
    )

    sums = lax.all_to_all(partial, TP, 0, 0, tiled=True)
    block, new_rotary, own_slice, rope_dot = pl.pallas_call(
        functools.partial(query_kernel, float(model_width)),
        out_shape=(
            sds((heads, 32, LANES), BF16),
            sds((seqs, rope_width), BF16),
            sds((seqs, LANES), F32),
            sds((seqs, LANES), F32),
        ),
        in_specs=whole(4),
        out_specs=tuple(whole(4)),
        compiler_params=SMALL,
    )(sums, cosine, sine, key_up)

    got = lax.all_to_all(block, KV, 0, 0, tiled=True)
    mine, side = pl.pallas_call(
        sort_kernel,
        out_shape=(sds((seqs, heads, LANES), BF16),) * 2,
        in_specs=whole(1),
        out_specs=tuple(whole(2)),
        compiler_params=SMALL,
    )(got)
    pieces = [swapped(mine, "tp_0", j) for j in (1, 2, 3)]

    new_latent, fresh_slice, latent_piece = pl.pallas_call(
        fresh_kernel,
        out_shape=(sds((seqs, rank), BF16), sds((seqs, LANES), F32), sds((4, seqs), BF16)),
        in_specs=whole(2),
        out_specs=tuple(whole(3)),
        scratch_shapes=[pltpu.VMEM((seqs, rank), F32)],
        compiler_params=SMALL,
    )(side, gain)
    pieces = [mine] + pieces
    pieces = pieces + [swapped(piece, "tp_1", 1) for piece in pieces]

    pairs_gap = seqs * (heads + 1)
    values, own_value = pl.pallas_call(
        functools.partial(attend_kernel, score_scale),
        out_shape=(sds((heads, 32, LANES), BF16), sds((seqs, LANES), F32)),
        in_specs=whole(12) + [hbm] * 2,
        out_specs=tuple(whole(2)),
        scratch_shapes=[
            pltpu.VMEM((rank // LANES, seqs, heads, LANES), BF16),
            pltpu.VMEM(cache_latent.shape, BF16),
            pltpu.VMEM(w_value_up.shape, BF16),
            pltpu.VMEM((rank * (heads + 1), LANES), F32),
            pltpu.VMEM((pairs_gap * (rank // LANES), LANES), F32),
            pltpu.VMEM((pairs_gap, LANES), F32),
            pltpu.VMEM((pairs_gap, LANES), F32),
            pltpu.SemaphoreType.DMA((8,)),
        ],
        compiler_params=pltpu.CompilerParams(vmem_limit_bytes=52 * 1024 * 1024),
    )(
        limits, *pieces, side, new_latent, rotary_keys, w_value_up, cache_latent
    )

    arrived = lax.all_to_all(values, KV, 0, 0, tiled=True)
    states = pl.pallas_call(
        gather_kernel,
        out_shape=sds((tp_count, 32, LANES), F32),
        in_specs=whole(3),
        out_specs=whole(1)[0],
        scratch_shapes=[pltpu.VMEM((kv_count, 16, LANES), F32)] * 2,
        compiler_params=SMALL,
    )(arrived, own_slice, fresh_slice)
    states = lax.all_to_all(states, TP, 0, 0, tiled=True)
    terms = pl.pallas_call(
        functools.partial(finish_kernel, score_scale),
        out_shape=sds((kv_count, seqs * out_cols // LANES, LANES), BF16),
        in_specs=whole(4),
        out_specs=whole(1)[0],
        compiler_params=SMALL,
    )(states, rope_dot, own_value, w_out)
    terms = lax.all_to_all(terms, KV, 0, 0, tiled=True)
    mixed_out = pl.pallas_call(
        total_kernel,
        out_shape=sds((seqs, out_cols), BF16),
        in_specs=whole(1),
        out_specs=whole(1)[0],
        compiler_params=SMALL,
    )(terms)
    return (mixed_out, latent_piece.T, new_rotary)


def solution(mesh):
    torus = Mesh(mesh.devices.reshape(8, 4, 4, 2), KV_TP)
    in_specs = (
        P(None, TP),
        P(TP),
        P(TP, KV, None),
        P(TP, KV),
        P(TP, None),
        P(),
        P(TP, KV, None),
        P(),
        P(KV, TP),
        P(None, KV_TP, None),
        P(None, KV_TP, None),
        P(),
    )
    out_specs = (P(None, TP), P(None, KV_TP), P())
    return jax.shard_map(
        shards, mesh=torus, in_specs=in_specs, out_specs=out_specs, check_vma=False
    )
```

```python
import functools

import jax
import jax.numpy as jnp
from jax import lax
from jax.experimental import pallas as pl
from jax.experimental.pallas import tpu as pltpu
from jax.sharding import Mesh
from jax.sharding import PartitionSpec as P

KV = ("kv_0", "kv_1")
TP = ("tp_0", "tp_1")
KV_TP = ("kv_0", "kv_1", "tp_0", "tp_1")


THETA = 10000.0
EPS = 1e-06
F32 = jnp.float32
BF16 = jnp.bfloat16
SMALL = pltpu.CompilerParams(vmem_limit_bytes=4 * 1024 * 1024)
FLOOR = -(2.0**127)
LANES = 128
NT = (((1,), (1,)), ((), ()))


def whole(count):
    return [pl.BlockSpec(memory_space=pltpu.VMEM)] * count


def lane_ids(rows):
    return lax.broadcasted_iota(jnp.int32, (rows, LANES), 1)


def swapped(value, axis, step):
    count = lax.axis_size(axis)
    return lax.ppermute(value, axis, [(i, i ^ step) for i in range(count)])


def fetch(pairs, sems):
    copies = [pltpu.make_async_copy(src, dst, sems.at[i]) for i, (src, dst) in enumerate(pairs)]
    for copy in copies:
        copy.start()
    return copies


def project_kernel(
    tokens_hbm, gain_hbm, query_hbm, latent_hbm, rotary_hbm, out_ref,
    tokens_s, gain_s, query_s, latent_s, rotary_s, sum_s, sems,
):
    copies = fetch(
        [
            (tokens_hbm, tokens_s), (gain_hbm, gain_s), (query_hbm, query_s),
            (latent_hbm, latent_s), (rotary_hbm, rotary_s),
        ],
        sems,
    )
    for copy in copies:
        copy.wait()
    tokens = tokens_s[...].astype(F32)
    scaled = (tokens * gain_s[...]).astype(BF16)
    squares = jnp.sum(tokens * tokens, axis=1, keepdims=True)
    sum_s[0:16, 0:96] = lax.dot_general(scaled, query_s[...], NT, preferred_element_type=F32)
    sum_s[0:16, 96:128] = lax.dot_general(scaled, latent_s[...], NT, preferred_element_type=F32)
    sum_s[16:32, :] = jnp.broadcast_to(squares, (16, LANES))
    sum_s[16:32, 0:32] = lax.dot_general(scaled, rotary_s[...], NT, preferred_element_type=F32)
    for peer in range(out_ref.shape[0]):
        out_ref[peer] = sum_s[...]


def table_kernel(
    lengths_ref, frequency_ref, key_in_ref, rot_in_ref, gain_in_ref,
    cos_ref, sin_ref, limit_ref, key_ref, rot_ref, gain_ref,
):
    row = lax.broadcasted_iota(jnp.int32, (16, LANES), 0)
    position = jnp.zeros((16, LANES), jnp.int32)
    for b in range(16):
        position = jnp.where(row == b, lengths_ref[b], position)
    angles = position.astype(F32) * frequency_ref[...]
    cos_ref[...] = jnp.cos(angles)
    sin_ref[...] = jnp.sin(angles)
    limit_ref[...] = position
    key_ref[...] = key_in_ref[...]
    rot_ref[...] = rot_in_ref[...]
    gain_ref[...] = gain_in_ref[...]


def query_kernel(
    model_width, parts_ref, cos_ref, sin_ref, key_ref,
    block_ref, rotary_ref, slice_ref, dot_ref,
):
    total = parts_ref[0]
    for peer in range(1, parts_ref.shape[0]):
        total = total + parts_ref[peer]
    lane = lane_ids(16)
    low = (lane & 31) < 16
    first, second = total[0:16], total[16:32]
    squares = jnp.sum(jnp.where(lane == 64, second, 0.0), axis=1, keepdims=True)
    inverse = lax.rsqrt(squares / model_width + EPS)

    def rotated(v):
        turned = jnp.where(low, -pltpu.roll(v, LANES - 16, 1), pltpu.roll(v, 16, 1))
        return v * cos_ref[...] + turned * sin_ref[...]

    query = (first * inverse).astype(BF16)
    query_f = query.astype(F32)
    rope = rotated(query_f)
    fresh = rotated(second * inverse).astype(BF16)
    latent_query = jnp.dot(query[:, 0:64], key_ref[...], preferred_element_type=F32).astype(BF16)
    side = jnp.where(lane < 96, rope, query_f)
    side = pltpu.roll(jnp.where(lane < 64, 0.0, side), 64, 1).astype(BF16)
    for peer in range(block_ref.shape[0]):
        block_ref[peer, 0:16, :] = latent_query
        block_ref[peer, 16:32, :] = side
    rotary_ref[...] = fresh[:, 0:32]
    slice_ref[...] = latent_query.astype(F32)
    both = jnp.where(lane < 32, side.astype(F32) * fresh.astype(F32), 0.0)
    dot_ref[...] = jnp.broadcast_to(jnp.sum(both, axis=1, keepdims=True), (16, LANES))


def sort_kernel(block_ref, mine_ref, side_ref):
    mine_ref[...] = pltpu.einshape("hbr->bhr", block_ref[:, 0:16, :])
    side_ref[...] = pltpu.einshape("hbr->bhr", block_ref[:, 16:32, :])


def fresh_kernel(
    side_ref, gain_ref, value_hbm, cache_hbm,
    fresh_ref, slice_ref, piece_ref, value_ref, cache_ref, row_s, sems,
):
    copies = fetch(
        [(cache_hbm, cache_ref), (value_hbm.at[pl.ds(0, value_ref.shape[0])], value_ref)], sems
    )
    heads, width, rank = side_ref.shape[1], 32, gain_ref.shape[1]
    square = jnp.zeros((16, width), F32)
    for k in range(heads):
        block = side_ref[:, k, width : 2 * width].astype(F32)
        row_s[:, k * width : (k + 1) * width] = block
        square += block * block
    mean = jnp.sum(square, axis=1, keepdims=True) / rank
    fresh = (row_s[...] * lax.rsqrt(mean + EPS) * gain_ref[...]).astype(BF16)
    fresh_ref[...] = fresh
    row_s[...] = fresh.astype(F32)
    tp = lax.axis_index("tp_0") * 2 + lax.axis_index("tp_1")
    kv = lax.axis_index("kv_0") * 4 + lax.axis_index("kv_1")
    slice_ref[...] = row_s[:, pl.ds(pl.multiple_of(tp * LANES, LANES), LANES)]
    column = (kv * 8 + tp) * 4
    base = column // LANES
    held = row_s[:, pl.ds(pl.multiple_of(base * LANES, LANES), LANES)]
    held = pltpu.roll(held, (LANES - (column - base * LANES)) % LANES, 1)
    piece_ref[...] = held.T[0:4, :].astype(BF16)
    for copy in copies:
        copy.wait()


def attend_kernel(scale, limit_ref, *refs):
    pieces = refs[0:8]
    (side_ref, fresh_ref, rot_ref, cache_ref, early_ref, value_hbm, out_ref, own_ref) = refs[8:16]
    (q_s, late_s, spread_s, o_s, m_s, l_s, sems) = refs[16:]
    seqs, heads = 16, 32
    depth, half = value_hbm.shape[0], late_s.shape[0]
    copy = pltpu.make_async_copy(value_hbm.at[pl.ds(half, half)], late_s, sems.at[0])
    copy.start()
    blocks, gap = q_s.shape[0], heads + 1

    chip, core = lax.axis_index("tp_0"), lax.axis_index("tp_1")
    kv = lax.axis_index("kv_0") * 4 + lax.axis_index("kv_1")
    first_pos = (kv * 8 + chip * 2 + core) * LANES
    for j in range(4):
        q_s[(chip ^ j) * 2 + core] = pieces[j][...]
        q_s[(chip ^ j) * 2 + 1 - core] = pieces[4 + j][...]
    group = 8
    for first in range(0, seqs, group):
        members = range(first, first + group)
        scores = []
        for b in members:
            query = jnp.concatenate([q_s[n, b] for n in range(blocks)], axis=1)
            term = lax.dot_general(query, cache_ref[b], NT, preferred_element_type=F32)
            term += jnp.dot(side_ref[b][:, 0:32], rot_ref[b], preferred_element_type=F32)
            scores.append(term)
        scores = jnp.concatenate(scores, axis=0) * scale
        limit = jnp.concatenate(
            [jnp.broadcast_to(limit_ref[b : b + 1, :], (heads, LANES)) for b in members], axis=0
        )
        valid = first_pos + lane_ids(heads * group) < limit
        top = jnp.max(jnp.where(valid, scores, FLOOR), axis=1, keepdims=True)
        weights = jnp.where(valid, jnp.exp(scores - top), 0.0)
        total = jnp.sum(weights, axis=1, keepdims=True)
        weights = weights.astype(BF16)
        for k, b in enumerate(members):
            part_rows = slice(k * heads, (k + 1) * heads)
            rows = slice(b * gap, b * gap + heads)
            summed = jnp.dot(weights[part_rows], cache_ref[b], preferred_element_type=F32)
            for n in range(blocks):
                at = (n * seqs + b) * gap
                o_s[at : at + heads, :] = summed[:, n * LANES : (n + 1) * LANES]
            m_s[rows, :] = jnp.broadcast_to(top[part_rows], (heads, LANES))
            l_s[rows, :] = jnp.broadcast_to(total[part_rows], (heads, LANES))
    for base, ref in ((0, early_ref), (half, late_s)):
        if base > 0:
            copy.wait()

        def spread(step, _):
            for n in range(8):
                r = step * 8 + n
                spread_s[pl.ds((base + r) * gap, heads), :] = ref[r].astype(F32)
            return 0

        lax.fori_loop(0, half // 8, spread, 0)
    lane = lane_ids(seqs)
    for h in range(heads):
        latent = jnp.concatenate(
            [o_s[pl.ds(n * seqs * gap + h, seqs, stride=gap), :] for n in range(blocks)], axis=1
        ).astype(BF16)
        weight = spread_s[pl.ds(h, depth, stride=gap), :].astype(BF16)
        out_ref[h, 0:16, :] = jnp.dot(latent, weight, preferred_element_type=F32).astype(BF16)
        stats = jnp.zeros((seqs, LANES), F32)
        for at, ref in ((0, m_s), (3, l_s)):
            left = ref[pl.ds(h, seqs, stride=gap), :]
            for n in range(3):
                piece = left.astype(BF16).astype(F32)
                stats = jnp.where(lane == at + n, piece, stats)
                left = left - piece
        out_ref[h, 16:32, :] = stats.astype(BF16)
    weight = spread_s[pl.ds(kv, depth, stride=gap), :].astype(BF16)
    own_ref[...] = jnp.dot(fresh_ref[...], weight, preferred_element_type=F32)


def gather_kernel(parts_ref, slice_ref, fresh_ref, out_ref, m_s, l_s):
    count = parts_ref.shape[0]
    lane = lane_ids(16)
    top = jnp.full((16, LANES), FLOOR, F32)
    for k in range(count):
        stats = parts_ref[k, 16:32, :].astype(F32)
        m = jnp.sum(jnp.where(lane < 3, stats, 0.0), axis=1, keepdims=True)
        l = jnp.sum(jnp.where((lane >= 3) & (lane < 6), stats, 0.0), axis=1, keepdims=True)
        m = jnp.broadcast_to(m, (16, LANES))
        m_s[k] = m
        l_s[k] = jnp.broadcast_to(l, (16, LANES))
        top = jnp.maximum(top, m)
    total = jnp.zeros((16, LANES), F32)
    summed = jnp.zeros((16, LANES), F32)
    for k in range(count):
        factor = jnp.exp(m_s[k] - top)
        total += factor * l_s[k]
        summed += factor * parts_ref[k, 0:16, :].astype(F32)
    own = jnp.sum(slice_ref[...] * fresh_ref[...], axis=1, keepdims=True)
    stats = jnp.where(lane == 0, top, jnp.where(lane == 1, total, own))
    for peer in range(out_ref.shape[0]):
        out_ref[peer, 0:16, :] = summed
        out_ref[peer, 16:32, :] = stats


def lane_of(stats, n):
    return jnp.sum(jnp.where(lane_ids(stats.shape[0]) == n, stats, 0.0), axis=1, keepdims=True)


def finish_kernel(scale, parts_ref, dot_ref, own_ref, weight_ref, out_ref):
    peers = range(parts_ref.shape[0])
    stats = [parts_ref[peer, 16:32, :] for peer in peers]
    tops = [lane_of(s, 0) for s in stats]
    own = (functools.reduce(jnp.add, [lane_of(s, 2) for s in stats]) + dot_ref[...]) * scale
    highest = functools.reduce(jnp.maximum, tops, own)
    total = jnp.exp(own - highest)
    summed = total * own_ref[...]
    for peer in peers:
        factor = jnp.exp(tops[peer] - highest)
        total += factor * lane_of(stats[peer], 1)
        summed += factor * parts_ref[peer, 0:16, :]
    head = (summed / total).astype(BF16)
    term = jnp.dot(head, weight_ref[...], preferred_element_type=F32).astype(BF16)
    for n in range(4):
        out_ref[16 * n : 16 * (n + 1), :] = term[:, LANES * n : LANES * (n + 1)]


def ring_kernel(a_ref, b_ref, c_ref, d_ref, out_ref):
    a, b, c, d = (ref[...].astype(F32) for ref in (a_ref, b_ref, c_ref, d_ref))
    term = ((a + b) + (c + d)).astype(BF16)
    for peer in range(out_ref.shape[0]):
        out_ref[peer] = term


def total_kernel(terms_ref, out_ref):
    for n in range(4):
        rows = slice(16 * n, 16 * (n + 1))
        total = terms_ref[0, rows, :].astype(F32)
        for k in range(1, terms_ref.shape[0]):
            total += terms_ref[k, rows, :].astype(F32)
        out_ref[:, LANES * n : LANES * (n + 1)] = total.astype(BF16)


def shards(
    tokens, norm_gain, w_query, w_latent, w_rotary, latent_gain, w_key_up, w_value_up, w_out,
    cache_latent, cache_rotary, lengths,
):
    seqs = tokens.shape[0]
    kv_count, tp_count = lax.axis_size(KV), lax.axis_size(TP)
    heads = kv_count
    rope_width = cache_rotary.shape[2]
    rank = cache_latent.shape[2]
    pos_dev = cache_latent.shape[1]
    model_width = tokens.shape[1] * tp_count
    out_cols = w_out.shape[1]
    score_scale = w_query.shape[2] ** (-0.5)
    sds = jax.ShapeDtypeStruct

    hbm = pl.BlockSpec(memory_space=pltpu.HBM)
    smem = pl.BlockSpec(memory_space=pltpu.SMEM)
    width = tokens.shape[1]
    query_width = w_query.shape[2]
    partial = pl.pallas_call(
        project_kernel,
        out_shape=sds((tp_count, 32, LANES), F32),
        in_specs=[hbm] * 5,
        out_specs=whole(1)[0],
        scratch_shapes=[
            pltpu.VMEM((seqs, width), BF16),
            pltpu.VMEM((1, width), F32),
            pltpu.VMEM((query_width, width), BF16),
            pltpu.VMEM((rope_width, width), BF16),
            pltpu.VMEM((rope_width, width), BF16),
            pltpu.VMEM((32, LANES), F32),
            pltpu.SemaphoreType.DMA((5,)),
        ],
    )(tokens, norm_gain[None], w_query[:, 0].T, w_latent.T, w_rotary.T)

    pair = lax.broadcasted_iota(jnp.int32, (1, LANES), 1) % (rope_width // 2)
    frequency = THETA ** (-(2 * pair).astype(F32) / rope_width)
    cosine, sine, limits, key_up, rotary_keys, gain = pl.pallas_call(
        table_kernel,
        out_shape=(
            sds((seqs, LANES), F32),
            sds((seqs, LANES), F32),
            sds((seqs, LANES), jnp.int32),
            sds((w_key_up.shape[2], LANES), BF16),
            sds((seqs, rope_width, pos_dev), BF16),
            sds((1, rank), F32),
        ),
        in_specs=[smem] + whole(4),
        out_specs=tuple(whole(6)),
        compiler_params=SMALL,
    )(
        lengths, frequency, w_key_up[:, 0].T, cache_rotary.transpose(0, 2, 1), latent_gain[None]
    )

    sums = lax.all_to_all(partial, TP, 0, 0, tiled=True)
    block, new_rotary, own_slice, rope_dot = pl.pallas_call(
        functools.partial(query_kernel, float(model_width)),
        out_shape=(
            sds((heads, 32, LANES), BF16),
            sds((seqs, rope_width), BF16),
            sds((seqs, LANES), F32),
            sds((seqs, LANES), F32),
        ),
        in_specs=whole(4),
        out_specs=tuple(whole(4)),
        compiler_params=SMALL,
    )(sums, cosine, sine, key_up)

    got = lax.all_to_all(block, KV, 0, 0, tiled=True)
    mine, side = pl.pallas_call(
        sort_kernel,
        out_shape=(sds((seqs, heads, LANES), BF16),) * 2,
        in_specs=whole(1),
        out_specs=tuple(whole(2)),
        compiler_params=SMALL,
    )(got)
    pieces = [swapped(mine, "tp_0", j) for j in (1, 2, 3)]

    half_shape = (rank // 2, *w_value_up.shape[1:])
    new_latent, fresh_slice, latent_piece, early, cache = pl.pallas_call(
        fresh_kernel,
        out_shape=(
            sds((seqs, rank), BF16),
            sds((seqs, LANES), F32),
            sds((4, seqs), BF16),
            sds(half_shape, BF16),
            sds(cache_latent.shape, BF16),
        ),
        in_specs=whole(2) + [hbm] * 2,
        out_specs=tuple(whole(5)),
        scratch_shapes=[pltpu.VMEM((seqs, rank), F32), pltpu.SemaphoreType.DMA((2,))],
        compiler_params=pltpu.CompilerParams(vmem_limit_bytes=45 * 1024 * 1024),
    )(side, gain, w_value_up, cache_latent)
    pieces, cache = lax.optimization_barrier((pieces, cache))
    pieces = [mine] + pieces
    pieces = pieces + [swapped(piece, "tp_1", 1) for piece in pieces]

    pairs_gap = seqs * (heads + 1)
    values, own_value = pl.pallas_call(
        functools.partial(attend_kernel, score_scale),
        out_shape=(sds((heads, 32, LANES), BF16), sds((seqs, LANES), F32)),
        in_specs=whole(14) + [hbm],
        out_specs=tuple(whole(2)),
        scratch_shapes=[
            pltpu.VMEM((rank // LANES, seqs, heads, LANES), BF16),
            pltpu.VMEM(half_shape, BF16),
            pltpu.VMEM((rank * (heads + 1), LANES), F32),
            pltpu.VMEM((pairs_gap * (rank // LANES), LANES), F32),
            pltpu.VMEM((pairs_gap, LANES), F32),
            pltpu.VMEM((pairs_gap, LANES), F32),
            pltpu.SemaphoreType.DMA((1,)),
        ],
        compiler_params=pltpu.CompilerParams(vmem_limit_bytes=42 * 1024 * 1024),
    )(
        limits, *pieces, side, new_latent, rotary_keys, cache, early, w_value_up
    )

    arrived = lax.all_to_all(values, KV, 0, 0, tiled=True)
    states = pl.pallas_call(
        gather_kernel,
        out_shape=sds((tp_count, 32, LANES), F32),
        in_specs=whole(3),
        out_specs=whole(1)[0],
        scratch_shapes=[pltpu.VMEM((kv_count, 16, LANES), F32)] * 2,
        compiler_params=SMALL,
    )(arrived, own_slice, fresh_slice)
    states = lax.all_to_all(states, TP, 0, 0, tiled=True)
    block_shape = (seqs * out_cols // LANES, LANES)
    term = pl.pallas_call(
        functools.partial(finish_kernel, score_scale),
        out_shape=sds(block_shape, BF16),
        in_specs=whole(4),
        out_specs=whole(1)[0],
        compiler_params=SMALL,
    )(states, rope_dot, own_value, w_out)
    terms = pl.pallas_call(
        ring_kernel,
        out_shape=sds((lax.axis_size("kv_0"), *block_shape), BF16),
        in_specs=whole(4),
        out_specs=whole(1)[0],
        compiler_params=SMALL,
    )(term, *[swapped(term, "kv_1", j) for j in (1, 2, 3)])
    terms = lax.all_to_all(terms, "kv_0", 0, 0, tiled=True)
    mixed_out = pl.pallas_call(
        total_kernel,
        out_shape=sds((seqs, out_cols), BF16),
        in_specs=whole(1),
        out_specs=whole(1)[0],
        compiler_params=SMALL,
    )(terms)
    return (mixed_out, latent_piece.T, new_rotary)


def solution(mesh):
    torus = Mesh(mesh.devices.reshape(8, 4, 4, 2), KV_TP)
    in_specs = (
        P(None, TP),
        P(TP),
        P(TP, KV, None),
        P(TP, KV),
        P(TP, None),
        P(),
        P(TP, KV, None),
        P(),
        P(KV, TP),
        P(None, KV_TP, None),
        P(None, KV_TP, None),
        P(),
    )
    out_specs = (P(None, TP), P(None, KV_TP), P())
    return jax.shard_map(
        shards, mesh=torus, in_specs=in_specs, out_specs=out_specs, check_vma=False
    )
```

```python
import functools

import jax
import jax.numpy as jnp
from jax import lax
from jax.experimental import pallas as pl
from jax.experimental.pallas import tpu as pltpu
from jax.sharding import Mesh
from jax.sharding import PartitionSpec as P

KV = ("kv_0", "kv_1")
TP = ("tp_0", "tp_1")
KV_TP = ("kv_0", "kv_1", "tp_0", "tp_1")


THETA = 10000.0
EPS = 1e-06
F32 = jnp.float32
BF16 = jnp.bfloat16
SMALL = pltpu.CompilerParams(vmem_limit_bytes=4 * 1024 * 1024)
FLOOR = -(2.0**127)
LANES = 128
NT = (((1,), (1,)), ((), ()))


def whole(count):
    return [pl.BlockSpec(memory_space=pltpu.VMEM)] * count


def lane_ids(rows):
    return lax.broadcasted_iota(jnp.int32, (rows, LANES), 1)


def swapped(value, axis, step):
    count = lax.axis_size(axis)
    return lax.ppermute(value, axis, [(i, i ^ step) for i in range(count)])


def fetch(pairs, sems):
    copies = [pltpu.make_async_copy(src, dst, sems.at[i]) for i, (src, dst) in enumerate(pairs)]
    for copy in copies:
        copy.start()
    return copies


def project_kernel(
    tokens_hbm, gain_hbm, query_hbm, latent_hbm, rotary_hbm, out_ref,
    tokens_s, gain_s, query_s, latent_s, rotary_s, sum_s, sems,
):
    copies = fetch(
        [
            (tokens_hbm, tokens_s), (gain_hbm, gain_s), (query_hbm, query_s),
            (latent_hbm, latent_s), (rotary_hbm, rotary_s),
        ],
        sems,
    )
    for copy in copies:
        copy.wait()
    tokens = tokens_s[...].astype(F32)
    scaled = (tokens * gain_s[...]).astype(BF16)
    squares = jnp.sum(tokens * tokens, axis=1, keepdims=True)
    sum_s[0:16, 0:96] = lax.dot_general(scaled, query_s[...], NT, preferred_element_type=F32)
    sum_s[0:16, 96:128] = lax.dot_general(scaled, latent_s[...], NT, preferred_element_type=F32)
    sum_s[16:32, :] = jnp.broadcast_to(squares, (16, LANES))
    sum_s[16:32, 0:32] = lax.dot_general(scaled, rotary_s[...], NT, preferred_element_type=F32)
    out_ref[...] = sum_s[...]


def add_kernel(a_ref, b_ref, out_ref):
    out_ref[...] = a_ref[...] + b_ref[...]


def table_kernel(
    lengths_ref, frequency_ref, key_in_ref, cos_ref, sin_ref, limit_ref, key_ref,
):
    row = lax.broadcasted_iota(jnp.int32, (16, LANES), 0)
    position = jnp.zeros((16, LANES), jnp.int32)
    for b in range(16):
        position = jnp.where(row == b, lengths_ref[b], position)
    angles = position.astype(F32) * frequency_ref[...]
    cos_ref[...] = jnp.cos(angles)
    sin_ref[...] = jnp.sin(angles)
    limit_ref[...] = position
    key_ref[...] = key_in_ref[...]


def query_kernel(
    model_width, a_ref, b_ref, c_ref, d_ref, cos_ref, sin_ref, key_ref,
    block_ref, rotary_ref, slice_ref, dot_ref,
):
    total = (a_ref[...] + b_ref[...]) + (c_ref[...] + d_ref[...])
    lane = lane_ids(16)
    low = (lane & 31) < 16
    first, second = total[0:16], total[16:32]
    squares = jnp.sum(jnp.where(lane == 64, second, 0.0), axis=1, keepdims=True)
    inverse = lax.rsqrt(squares / model_width + EPS)

    def rotated(v):
        turned = jnp.where(low, -pltpu.roll(v, LANES - 16, 1), pltpu.roll(v, 16, 1))
        return v * cos_ref[...] + turned * sin_ref[...]

    query = (first * inverse).astype(BF16)
    query_f = query.astype(F32)
    rope = rotated(query_f)
    fresh = rotated(second * inverse).astype(BF16)
    latent_query = jnp.dot(query[:, 0:64], key_ref[...], preferred_element_type=F32).astype(BF16)
    side = jnp.where(lane < 96, rope, query_f)
    side = pltpu.roll(jnp.where(lane < 64, 0.0, side), 64, 1).astype(BF16)
    for peer in range(block_ref.shape[0]):
        block_ref[peer, 0:16, :] = latent_query
        block_ref[peer, 16:32, :] = side
    rotary_ref[...] = fresh[:, 0:32]
    slice_ref[...] = latent_query.astype(F32)
    both = jnp.where(lane < 32, side.astype(F32) * fresh.astype(F32), 0.0)
    dot_ref[...] = jnp.broadcast_to(jnp.sum(both, axis=1, keepdims=True), (16, LANES))


def sort_kernel(block_ref, mine_ref, side_ref):
    mine_ref[...] = pltpu.einshape("hbr->bhr", block_ref[:, 0:16, :])
    side_ref[...] = pltpu.einshape("hbr->bhr", block_ref[:, 16:32, :])


def fresh_kernel(
    side_ref, gain_ref, rot_hbm, cache_hbm,
    fresh_ref, slice_ref, piece_ref, rot_ref, cache_ref, row_s, sems,
):
    copies = fetch([(cache_hbm, cache_ref), (rot_hbm, rot_ref)], sems)
    heads, width, rank = side_ref.shape[1], 32, gain_ref.shape[1]
    square = jnp.zeros((16, width), F32)
    for k in range(heads):
        block = side_ref[:, k, width : 2 * width].astype(F32)
        row_s[:, k * width : (k + 1) * width] = block
        square += block * block
    mean = jnp.sum(square, axis=1, keepdims=True) / rank
    fresh = (row_s[...] * lax.rsqrt(mean + EPS) * gain_ref[...]).astype(BF16)
    fresh_ref[...] = fresh
    row_s[...] = fresh.astype(F32)
    tp = lax.axis_index("tp_0") * 2 + lax.axis_index("tp_1")
    kv = lax.axis_index("kv_0") * 4 + lax.axis_index("kv_1")
    slice_ref[...] = row_s[:, pl.ds(pl.multiple_of(tp * LANES, LANES), LANES)]
    column = (kv * 8 + tp) * 4
    base = column // LANES
    held = row_s[:, pl.ds(pl.multiple_of(base * LANES, LANES), LANES)]
    held = pltpu.roll(held, (LANES - (column - base * LANES)) % LANES, 1)
    piece_ref[...] = held.T[0:4, :].astype(BF16)
    for copy in copies:
        copy.wait()


def attend_kernel(scale, limit_ref, *refs):
    pieces = refs[0:8]
    (side_ref, fresh_ref, rot_ref, cache_ref, value_hbm, out_ref, own_ref) = refs[8:15]
    (q_s, value_s, spread_s, o_s, m_s, l_s, sems) = refs[15:]
    seqs, heads = 16, 32
    depth, chunks = value_hbm.shape[0], sems.shape[0]
    part = depth // chunks
    cut = lambda ref, i: ref.at[pl.ds(i * part, part)]
    copies = fetch([(cut(value_hbm, i), cut(value_s, i)) for i in range(chunks)], sems)
    blocks, gap = q_s.shape[0], heads + 1

    chip, core = lax.axis_index("tp_0"), lax.axis_index("tp_1")
    kv = lax.axis_index("kv_0") * 4 + lax.axis_index("kv_1")
    first_pos = (kv * 8 + chip * 2 + core) * LANES
    for j in range(4):
        q_s[(chip ^ j) * 2 + core] = pieces[j][...]
        q_s[(chip ^ j) * 2 + 1 - core] = pieces[4 + j][...]
    group = 8
    for first in range(0, seqs, group):
        members = range(first, first + group)
        scores = []
        for b in members:
            query = jnp.concatenate([q_s[n, b] for n in range(blocks)], axis=1)
            term = lax.dot_general(query, cache_ref[b], NT, preferred_element_type=F32)
            term += jnp.dot(side_ref[b][:, 0:32], rot_ref[b], preferred_element_type=F32)
            scores.append(term)
        scores = jnp.concatenate(scores, axis=0) * scale
        limit = jnp.concatenate(
            [jnp.broadcast_to(limit_ref[b : b + 1, :], (heads, LANES)) for b in members], axis=0
        )
        valid = first_pos + lane_ids(heads * group) < limit
        top = jnp.max(jnp.where(valid, scores, FLOOR), axis=1, keepdims=True)
        weights = jnp.where(valid, jnp.exp(scores - top), 0.0)
        total = jnp.sum(weights, axis=1, keepdims=True)
        weights = weights.astype(BF16)
        for k, b in enumerate(members):
            part_rows = slice(k * heads, (k + 1) * heads)
            rows = slice(b * gap, b * gap + heads)
            summed = jnp.dot(weights[part_rows], cache_ref[b], preferred_element_type=F32)
            for n in range(blocks):
                at = (n * seqs + b) * gap
                o_s[at : at + heads, :] = summed[:, n * LANES : (n + 1) * LANES]
            m_s[rows, :] = jnp.broadcast_to(top[part_rows], (heads, LANES))
            l_s[rows, :] = jnp.broadcast_to(total[part_rows], (heads, LANES))
    for i in range(chunks):
        copies[i].wait()

        def spread(step, _):
            for n in range(8):
                r = i * part + step * 8 + n
                spread_s[pl.ds(r * gap, heads), :] = value_s[r].astype(F32)
            return 0

        lax.fori_loop(0, part // 8, spread, 0)
    lane = lane_ids(seqs)
    for h in range(heads):
        latent = jnp.concatenate(
            [o_s[pl.ds(n * seqs * gap + h, seqs, stride=gap), :] for n in range(blocks)], axis=1
        ).astype(BF16)
        weight = spread_s[pl.ds(h, depth, stride=gap), :].astype(BF16)
        out_ref[h, 0:16, :] = jnp.dot(latent, weight, preferred_element_type=F32).astype(BF16)
        stats = jnp.zeros((seqs, LANES), F32)
        for at, ref in ((0, m_s), (3, l_s)):
            left = ref[pl.ds(h, seqs, stride=gap), :]
            for n in range(3):
                piece = left.astype(BF16).astype(F32)
                stats = jnp.where(lane == at + n, piece, stats)
                left = left - piece
        out_ref[h, 16:32, :] = stats.astype(BF16)
    weight = spread_s[pl.ds(kv, depth, stride=gap), :].astype(BF16)
    own_ref[...] = jnp.dot(fresh_ref[...], weight, preferred_element_type=F32)


def gather_kernel(parts_ref, slice_ref, fresh_ref, out_ref, m_s, l_s):
    count = parts_ref.shape[0]
    lane = lane_ids(16)
    top = jnp.full((16, LANES), FLOOR, F32)
    for k in range(count):
        stats = parts_ref[k, 16:32, :].astype(F32)
        m = jnp.sum(jnp.where(lane < 3, stats, 0.0), axis=1, keepdims=True)
        l = jnp.sum(jnp.where((lane >= 3) & (lane < 6), stats, 0.0), axis=1, keepdims=True)
        m = jnp.broadcast_to(m, (16, LANES))
        m_s[k] = m
        l_s[k] = jnp.broadcast_to(l, (16, LANES))
        top = jnp.maximum(top, m)
    total = jnp.zeros((16, LANES), F32)
    summed = jnp.zeros((16, LANES), F32)
    for k in range(count):
        factor = jnp.exp(m_s[k] - top)
        total += factor * l_s[k]
        summed += factor * parts_ref[k, 0:16, :].astype(F32)
    own = jnp.sum(slice_ref[...] * fresh_ref[...], axis=1, keepdims=True)
    stats = jnp.where(lane == 0, top, jnp.where(lane == 1, total, own))
    out_ref[0:16, :] = summed
    out_ref[16:32, :] = stats


def lane_of(stats, n):
    return jnp.sum(jnp.where(lane_ids(stats.shape[0]) == n, stats, 0.0), axis=1, keepdims=True)


def merged(refs):
    stats = [ref[16:32, :] for ref in refs]
    tops = [lane_of(s, 0) for s in stats]
    highest = functools.reduce(jnp.maximum, tops)
    factors = [jnp.exp(top - highest) for top in tops]
    summed = functools.reduce(jnp.add, [f * ref[0:16, :] for f, ref in zip(factors, refs)])
    total = functools.reduce(jnp.add, [f * lane_of(s, 1) for f, s in zip(factors, stats)])
    return summed, highest, total, functools.reduce(jnp.add, [lane_of(s, 2) for s in stats])


def pair_kernel(a_ref, b_ref, out_ref):
    summed, top, total, own = merged((a_ref, b_ref))
    lane = lane_ids(16)
    out_ref[0:16, :] = summed
    out_ref[16:32, :] = jnp.where(lane == 0, top, jnp.where(lane == 1, total, own))


def finish_kernel(scale, a_ref, b_ref, c_ref, d_ref, dot_ref, own_ref, weight_ref, out_ref):
    summed, top, total, own = merged((a_ref, b_ref, c_ref, d_ref))
    own = (own + dot_ref[...]) * scale
    highest = jnp.maximum(top, own)
    factor, own_weight = jnp.exp(top - highest), jnp.exp(own - highest)
    summed = factor * summed + own_weight * own_ref[...]
    head = (summed / (factor * total + own_weight)).astype(BF16)
    term = jnp.dot(head, weight_ref[...], preferred_element_type=F32).astype(BF16)
    for n in range(4):
        out_ref[16 * n : 16 * (n + 1), :] = term[:, LANES * n : LANES * (n + 1)]


def ring_kernel(a_ref, b_ref, c_ref, d_ref, out_ref):
    a, b, c, d = (ref[...].astype(F32) for ref in (a_ref, b_ref, c_ref, d_ref))
    term = ((a + b) + (c + d)).astype(BF16)
    for peer in range(out_ref.shape[0]):
        out_ref[peer] = term


def total_kernel(terms_ref, out_ref):
    for n in range(4):
        rows = slice(16 * n, 16 * (n + 1))
        total = terms_ref[0, rows, :].astype(F32)
        for k in range(1, terms_ref.shape[0]):
            total += terms_ref[k, rows, :].astype(F32)
        out_ref[:, LANES * n : LANES * (n + 1)] = total.astype(BF16)


def shards(
    tokens, norm_gain, w_query, w_latent, w_rotary, latent_gain, w_key_up, w_value_up, w_out,
    cache_latent, cache_rotary, lengths,
):
    seqs = tokens.shape[0]
    kv_count, tp_count = lax.axis_size(KV), lax.axis_size(TP)
    heads = kv_count
    rope_width = cache_rotary.shape[2]
    rank = cache_latent.shape[2]
    pos_dev = cache_latent.shape[1]
    model_width = tokens.shape[1] * tp_count
    out_cols = w_out.shape[1]
    score_scale = w_query.shape[2] ** (-0.5)
    sds = jax.ShapeDtypeStruct

    hbm = pl.BlockSpec(memory_space=pltpu.HBM)
    smem = pl.BlockSpec(memory_space=pltpu.SMEM)
    width = tokens.shape[1]
    query_width = w_query.shape[2]
    partial = pl.pallas_call(
        project_kernel,
        out_shape=sds((32, LANES), F32),
        in_specs=[hbm] * 5,
        out_specs=whole(1)[0],
        scratch_shapes=[
            pltpu.VMEM((seqs, width), BF16),
            pltpu.VMEM((1, width), F32),
            pltpu.VMEM((query_width, width), BF16),
            pltpu.VMEM((rope_width, width), BF16),
            pltpu.VMEM((rope_width, width), BF16),
            pltpu.VMEM((32, LANES), F32),
            pltpu.SemaphoreType.DMA((5,)),
        ],
    )(tokens, norm_gain[None], w_query[:, 0].T, w_latent.T, w_rotary.T)

    pair = lax.broadcasted_iota(jnp.int32, (1, LANES), 1) % (rope_width // 2)
    frequency = THETA ** (-(2 * pair).astype(F32) / rope_width)
    cosine, sine, limits, key_up = pl.pallas_call(
        table_kernel,
        out_shape=(
            sds((seqs, LANES), F32),
            sds((seqs, LANES), F32),
            sds((seqs, LANES), jnp.int32),
            sds((w_key_up.shape[2], LANES), BF16),
        ),
        in_specs=[smem] + whole(2),
        out_specs=tuple(whole(4)),
        compiler_params=SMALL,
    )(lengths, frequency, w_key_up[:, 0].T)

    partial = pl.pallas_call(
        add_kernel,
        out_shape=sds((32, LANES), F32),
        in_specs=whole(2),
        out_specs=whole(1)[0],
        compiler_params=SMALL,
    )(partial, swapped(partial, "tp_1", 1))
    sums = [partial] + [swapped(partial, "tp_0", j) for j in (1, 2, 3)]
    block, new_rotary, own_slice, rope_dot = pl.pallas_call(
        functools.partial(query_kernel, float(model_width)),
        out_shape=(
            sds((heads, 32, LANES), BF16),
            sds((seqs, rope_width), BF16),
            sds((seqs, LANES), F32),
            sds((seqs, LANES), F32),
        ),
        in_specs=whole(7),
        out_specs=tuple(whole(4)),
        compiler_params=SMALL,
    )(*sums, cosine, sine, key_up)

    got = lax.all_to_all(block, KV, 0, 0, tiled=True)
    mine, side = pl.pallas_call(
        sort_kernel,
        out_shape=(sds((seqs, heads, LANES), BF16),) * 2,
        in_specs=whole(1),
        out_specs=tuple(whole(2)),
        compiler_params=SMALL,
    )(got)
    pieces = [swapped(mine, "tp_0", j) for j in (1, 2, 3)]

    rotary_keys = cache_rotary.transpose(0, 2, 1)
    new_latent, fresh_slice, latent_piece, rotary_keys, cache = pl.pallas_call(
        fresh_kernel,
        out_shape=(
            sds((seqs, rank), BF16),
            sds((seqs, LANES), F32),
            sds((4, seqs), BF16),
            sds(rotary_keys.shape, BF16),
            sds(cache_latent.shape, BF16),
        ),
        in_specs=whole(2) + [hbm] * 2,
        out_specs=tuple(whole(5)),
        scratch_shapes=[pltpu.VMEM((seqs, rank), F32), pltpu.SemaphoreType.DMA((2,))],
        compiler_params=pltpu.CompilerParams(vmem_limit_bytes=48 * 1024 * 1024),
    )(side, latent_gain[None], rotary_keys, cache_latent)
    pieces, cache = lax.optimization_barrier((pieces, cache))
    pieces = [mine] + pieces
    pieces = pieces + [swapped(piece, "tp_1", 1) for piece in pieces]

    pairs_gap = seqs * (heads + 1)
    values, own_value = pl.pallas_call(
        functools.partial(attend_kernel, score_scale),
        out_shape=(sds((heads, 32, LANES), BF16), sds((seqs, LANES), F32)),
        in_specs=whole(13) + [hbm],
        out_specs=tuple(whole(2)),
        scratch_shapes=[
            pltpu.VMEM((rank // LANES, seqs, heads, LANES), BF16),
            pltpu.VMEM(w_value_up.shape, BF16),
            pltpu.VMEM((rank * (heads + 1), LANES), F32),
            pltpu.VMEM((pairs_gap * (rank // LANES), LANES), F32),
            pltpu.VMEM((pairs_gap, LANES), F32),
            pltpu.VMEM((pairs_gap, LANES), F32),
            pltpu.SemaphoreType.DMA((4,)),
        ],
        compiler_params=pltpu.CompilerParams(vmem_limit_bytes=46 * 1024 * 1024),
    )(
        limits, *pieces, side, new_latent, rotary_keys, cache, w_value_up
    )

    arrived = lax.all_to_all(values, KV, 0, 0, tiled=True)
    state = pl.pallas_call(
        gather_kernel,
        out_shape=sds((32, LANES), F32),
        in_specs=whole(3),
        out_specs=whole(1)[0],
        scratch_shapes=[pltpu.VMEM((kv_count, 16, LANES), F32)] * 2,
        compiler_params=SMALL,
    )(arrived, own_slice, fresh_slice)
    state = pl.pallas_call(
        pair_kernel,
        out_shape=sds((32, LANES), F32),
        in_specs=whole(2),
        out_specs=whole(1)[0],
        compiler_params=SMALL,
    )(state, swapped(state, "tp_1", 1))
    states = [state] + [swapped(state, "tp_0", j) for j in (1, 2, 3)]
    block_shape = (seqs * out_cols // LANES, LANES)
    term = pl.pallas_call(
        functools.partial(finish_kernel, score_scale),
        out_shape=sds(block_shape, BF16),
        in_specs=whole(7),
        out_specs=whole(1)[0],
        compiler_params=SMALL,
    )(*states, rope_dot, own_value, w_out)
    terms = pl.pallas_call(
        ring_kernel,
        out_shape=sds((lax.axis_size("kv_0"), *block_shape), BF16),
        in_specs=whole(4),
        out_specs=whole(1)[0],
        compiler_params=SMALL,
    )(term, *[swapped(term, "kv_1", j) for j in (1, 2, 3)])
    terms = lax.all_to_all(terms, "kv_0", 0, 0, tiled=True)
    mixed_out = pl.pallas_call(
        total_kernel,
        out_shape=sds((seqs, out_cols), BF16),
        in_specs=whole(1),
        out_specs=whole(1)[0],
        compiler_params=SMALL,
    )(terms)
    return (mixed_out, latent_piece.T, new_rotary)


def solution(mesh):
    torus = Mesh(mesh.devices.reshape(8, 4, 4, 2), KV_TP)
    in_specs = (
        P(None, TP),
        P(TP),
        P(TP, KV, None),
        P(TP, KV),
        P(TP, None),
        P(),
        P(TP, KV, None),
        P(),
        P(KV, TP),
        P(None, KV_TP, None),
        P(None, KV_TP, None),
        P(),
    )
    out_specs = (P(None, TP), P(None, KV_TP), P())
    return jax.shard_map(
        shards, mesh=torus, in_specs=in_specs, out_specs=out_specs, check_vma=False
    )
```

```python
import functools

import jax
import jax.numpy as jnp
from jax import lax
from jax.experimental import pallas as pl
from jax.experimental.pallas import tpu as pltpu
from jax.sharding import Mesh
from jax.sharding import PartitionSpec as P

KV = ("kv_0", "kv_1")
TP = ("tp_0", "tp_1")
KV_TP = ("kv_0", "kv_1", "tp_0", "tp_1")


THETA = 10000.0
EPS = 1e-06
F32 = jnp.float32
BF16 = jnp.bfloat16
SMALL = pltpu.CompilerParams(vmem_limit_bytes=4 * 1024 * 1024)
FLOOR = -(2.0**127)
LANES = 128
NT = (((1,), (1,)), ((), ()))


def whole(count):
    return [pl.BlockSpec(memory_space=pltpu.VMEM)] * count


def lane_ids(rows):
    return lax.broadcasted_iota(jnp.int32, (rows, LANES), 1)


def swapped(value, axis, step):
    count = lax.axis_size(axis)
    return lax.ppermute(value, axis, [(i, i ^ step) for i in range(count)])


def fetch(pairs, sems):
    copies = [pltpu.make_async_copy(src, dst, sems.at[i]) for i, (src, dst) in enumerate(pairs)]
    for copy in copies:
        copy.start()
    return copies


def project_kernel(
    tokens_hbm, gain_hbm, query_hbm, latent_hbm, rotary_hbm, out_ref,
    tokens_s, gain_s, query_s, latent_s, rotary_s, sum_s, sems,
):
    copies = fetch(
        [
            (tokens_hbm, tokens_s), (gain_hbm, gain_s), (query_hbm, query_s),
            (latent_hbm, latent_s), (rotary_hbm, rotary_s),
        ],
        sems,
    )
    for copy in copies:
        copy.wait()
    tokens = tokens_s[...].astype(F32)
    scaled = (tokens * gain_s[...]).astype(BF16)
    squares = jnp.sum(tokens * tokens, axis=1, keepdims=True)
    sum_s[0:16, 0:96] = lax.dot_general(scaled, query_s[...], NT, preferred_element_type=F32)
    sum_s[0:16, 96:128] = lax.dot_general(scaled, latent_s[...], NT, preferred_element_type=F32)
    sum_s[16:32, :] = jnp.broadcast_to(squares, (16, LANES))
    sum_s[16:32, 0:32] = lax.dot_general(scaled, rotary_s[...], NT, preferred_element_type=F32)
    out_ref[...] = sum_s[...]


def add_kernel(a_ref, b_ref, out_ref):
    out_ref[...] = a_ref[...] + b_ref[...]


def table_kernel(
    lengths_ref, frequency_ref, key_in_ref, cos_ref, sin_ref, limit_ref, key_ref,
):
    row = lax.broadcasted_iota(jnp.int32, (16, LANES), 0)
    position = jnp.zeros((16, LANES), jnp.int32)
    for b in range(16):
        position = jnp.where(row == b, lengths_ref[b], position)
    angles = position.astype(F32) * frequency_ref[...]
    cos_ref[...] = jnp.cos(angles)
    sin_ref[...] = jnp.sin(angles)
    limit_ref[...] = position
    key_ref[...] = key_in_ref[...]


def query_kernel(
    model_width, a_ref, b_ref, c_ref, d_ref, cos_ref, sin_ref, key_ref,
    block_ref, rotary_ref, slice_ref, dot_ref,
):
    total = (a_ref[...] + b_ref[...]) + (c_ref[...] + d_ref[...])
    lane = lane_ids(16)
    low = (lane & 31) < 16
    first, second = total[0:16], total[16:32]
    squares = jnp.sum(jnp.where(lane == 64, second, 0.0), axis=1, keepdims=True)
    inverse = lax.rsqrt(squares / model_width + EPS)

    def rotated(v):
        turned = jnp.where(low, -pltpu.roll(v, LANES - 16, 1), pltpu.roll(v, 16, 1))
        return v * cos_ref[...] + turned * sin_ref[...]

    query = (first * inverse).astype(BF16)
    query_f = query.astype(F32)
    rope = rotated(query_f)
    fresh = rotated(second * inverse).astype(BF16)
    latent_query = jnp.dot(query[:, 0:64], key_ref[...], preferred_element_type=F32).astype(BF16)
    side = jnp.where(lane < 96, rope, query_f)
    side = pltpu.roll(jnp.where(lane < 64, 0.0, side), 64, 1).astype(BF16)
    for peer in range(block_ref.shape[0]):
        block_ref[peer, 0:16, :] = latent_query
        block_ref[peer, 16:32, :] = side
    rotary_ref[...] = fresh[:, 0:32]
    slice_ref[...] = latent_query.astype(F32)
    both = jnp.where(lane < 32, side.astype(F32) * fresh.astype(F32), 0.0)
    dot_ref[...] = jnp.broadcast_to(jnp.sum(both, axis=1, keepdims=True), (16, LANES))


def sort_kernel(block_ref, mine_ref, side_ref):
    mine_ref[...] = pltpu.einshape("hbr->bhr", block_ref[:, 0:16, :])
    side_ref[...] = pltpu.einshape("hbr->bhr", block_ref[:, 16:32, :])


def fresh_kernel(
    side_ref, gain_ref, value_hbm, fresh_ref, slice_ref, piece_ref, value_ref, row_s, value_s, sems
):
    chunks = sems.shape[0]
    part = value_s.shape[0] // chunks
    cut = lambda ref, i: ref.at[pl.ds(i * part, part)]
    copies = fetch([(cut(value_hbm, i), cut(value_s, i)) for i in range(chunks)], sems)
    heads, width, rank = side_ref.shape[1], 32, gain_ref.shape[1]
    square = jnp.zeros((16, width), F32)
    for k in range(heads):
        block = side_ref[:, k, width : 2 * width].astype(F32)
        row_s[:, k * width : (k + 1) * width] = block
        square += block * block
    mean = jnp.sum(square, axis=1, keepdims=True) / rank
    fresh = (row_s[...] * lax.rsqrt(mean + EPS) * gain_ref[...]).astype(BF16)
    fresh_ref[...] = fresh
    row_s[...] = fresh.astype(F32)
    tp = lax.axis_index("tp_0") * 2 + lax.axis_index("tp_1")
    kv = lax.axis_index("kv_0") * 4 + lax.axis_index("kv_1")
    slice_ref[...] = row_s[:, pl.ds(pl.multiple_of(tp * LANES, LANES), LANES)]
    column = (kv * 8 + tp) * 4
    base = column // LANES
    held = row_s[:, pl.ds(pl.multiple_of(base * LANES, LANES), LANES)]
    held = pltpu.roll(held, (LANES - (column - base * LANES)) % LANES, 1)
    piece_ref[...] = held.T[0:4, :].astype(BF16)
    step = 64
    for i in range(chunks):
        copies[i].wait()
        for j in range(i * part, (i + 1) * part, step):
            value_ref[:, j : j + step, :] = pltpu.einshape("rhv->hrv", value_s[j : j + step])


def attend_kernel(scale, limit_ref, *refs):
    pieces = refs[0:8]
    (side_ref, fresh_ref, rot_ref, cache_ref, value_ref, out_ref, own_ref) = refs[8:15]
    (q_s, o_s, m_s, l_s) = refs[15:]
    seqs, heads = 16, 32
    blocks, gap = q_s.shape[0], heads + 1

    chip, core = lax.axis_index("tp_0"), lax.axis_index("tp_1")
    kv = lax.axis_index("kv_0") * 4 + lax.axis_index("kv_1")
    first_pos = (kv * 8 + chip * 2 + core) * LANES
    for j in range(4):
        q_s[(chip ^ j) * 2 + core] = pieces[j][...]
        q_s[(chip ^ j) * 2 + 1 - core] = pieces[4 + j][...]
    group = 8
    for first in range(0, seqs, group):
        members = range(first, first + group)
        scores = []
        for b in members:
            query = jnp.concatenate([q_s[n, b] for n in range(blocks)], axis=1)
            term = lax.dot_general(query, cache_ref[b], NT, preferred_element_type=F32)
            term += jnp.dot(side_ref[b][:, 0:32], rot_ref[b], preferred_element_type=F32)
            scores.append(term)
        scores = jnp.concatenate(scores, axis=0) * scale
        limit = jnp.concatenate(
            [jnp.broadcast_to(limit_ref[b : b + 1, :], (heads, LANES)) for b in members], axis=0
        )
        valid = first_pos + lane_ids(heads * group) < limit
        top = jnp.max(jnp.where(valid, scores, FLOOR), axis=1, keepdims=True)
        weights = jnp.where(valid, jnp.exp(scores - top), 0.0)
        total = jnp.sum(weights, axis=1, keepdims=True)
        weights = weights.astype(BF16)
        for k, b in enumerate(members):
            part_rows = slice(k * heads, (k + 1) * heads)
            rows = slice(b * gap, b * gap + heads)
            summed = jnp.dot(weights[part_rows], cache_ref[b], preferred_element_type=F32)
            for n in range(blocks):
                at = (n * seqs + b) * gap
                o_s[at : at + heads, :] = summed[:, n * LANES : (n + 1) * LANES]
            m_s[rows, :] = jnp.broadcast_to(top[part_rows], (heads, LANES))
            l_s[rows, :] = jnp.broadcast_to(total[part_rows], (heads, LANES))
    lane = lane_ids(seqs)
    for h in range(heads):
        latent = jnp.concatenate(
            [o_s[pl.ds(n * seqs * gap + h, seqs, stride=gap), :] for n in range(blocks)], axis=1
        ).astype(BF16)
        out_ref[h, 0:16, :] = jnp.dot(
            latent, value_ref[h], preferred_element_type=F32
        ).astype(BF16)
        stats = jnp.zeros((seqs, LANES), F32)
        for at, ref in ((0, m_s), (3, l_s)):
            left = ref[pl.ds(h, seqs, stride=gap), :]
            for n in range(3):
                piece = left.astype(BF16).astype(F32)
                stats = jnp.where(lane == at + n, piece, stats)
                left = left - piece
        out_ref[h, 16:32, :] = stats.astype(BF16)
    own_ref[...] = jnp.dot(fresh_ref[...], value_ref[kv], preferred_element_type=F32)


def gather_kernel(parts_ref, slice_ref, fresh_ref, out_ref, m_s, l_s):
    count = parts_ref.shape[0]
    lane = lane_ids(16)
    top = jnp.full((16, LANES), FLOOR, F32)
    for k in range(count):
        stats = parts_ref[k, 16:32, :].astype(F32)
        m = jnp.sum(jnp.where(lane < 3, stats, 0.0), axis=1, keepdims=True)
        l = jnp.sum(jnp.where((lane >= 3) & (lane < 6), stats, 0.0), axis=1, keepdims=True)
        m = jnp.broadcast_to(m, (16, LANES))
        m_s[k] = m
        l_s[k] = jnp.broadcast_to(l, (16, LANES))
        top = jnp.maximum(top, m)
    total = jnp.zeros((16, LANES), F32)
    summed = jnp.zeros((16, LANES), F32)
    for k in range(count):
        factor = jnp.exp(m_s[k] - top)
        total += factor * l_s[k]
        summed += factor * parts_ref[k, 0:16, :].astype(F32)
    own = jnp.sum(slice_ref[...] * fresh_ref[...], axis=1, keepdims=True)
    stats = jnp.where(lane == 0, top, jnp.where(lane == 1, total, own))
    out_ref[0:16, :] = summed
    out_ref[16:32, :] = stats


def lane_of(stats, n):
    return jnp.sum(jnp.where(lane_ids(stats.shape[0]) == n, stats, 0.0), axis=1, keepdims=True)


def merged(refs):
    stats = [ref[16:32, :] for ref in refs]
    tops = [lane_of(s, 0) for s in stats]
    highest = functools.reduce(jnp.maximum, tops)
    factors = [jnp.exp(top - highest) for top in tops]
    summed = functools.reduce(jnp.add, [f * ref[0:16, :] for f, ref in zip(factors, refs)])
    total = functools.reduce(jnp.add, [f * lane_of(s, 1) for f, s in zip(factors, stats)])
    return summed, highest, total, functools.reduce(jnp.add, [lane_of(s, 2) for s in stats])


def pair_kernel(a_ref, b_ref, out_ref):
    summed, top, total, own = merged((a_ref, b_ref))
    lane = lane_ids(16)
    out_ref[0:16, :] = summed
    out_ref[16:32, :] = jnp.where(lane == 0, top, jnp.where(lane == 1, total, own))


def finish_kernel(scale, a_ref, b_ref, c_ref, d_ref, dot_ref, own_ref, weight_ref, out_ref):
    summed, top, total, own = merged((a_ref, b_ref, c_ref, d_ref))
    own = (own + dot_ref[...]) * scale
    highest = jnp.maximum(top, own)
    factor, own_weight = jnp.exp(top - highest), jnp.exp(own - highest)
    summed = factor * summed + own_weight * own_ref[...]
    head = (summed / (factor * total + own_weight)).astype(BF16)
    term = jnp.dot(head, weight_ref[...], preferred_element_type=F32).astype(BF16)
    for n in range(4):
        out_ref[16 * n : 16 * (n + 1), :] = term[:, LANES * n : LANES * (n + 1)]


def ring_kernel(a_ref, b_ref, c_ref, d_ref, out_ref):
    a, b, c, d = (ref[...].astype(F32) for ref in (a_ref, b_ref, c_ref, d_ref))
    term = ((a + b) + (c + d)).astype(BF16)
    for peer in range(out_ref.shape[0]):
        out_ref[peer] = term


def total_kernel(terms_ref, out_ref):
    for n in range(4):
        rows = slice(16 * n, 16 * (n + 1))
        total = terms_ref[0, rows, :].astype(F32)
        for k in range(1, terms_ref.shape[0]):
            total += terms_ref[k, rows, :].astype(F32)
        out_ref[:, LANES * n : LANES * (n + 1)] = total.astype(BF16)


def shards(
    tokens, norm_gain, w_query, w_latent, w_rotary, latent_gain, w_key_up, w_value_up, w_out,
    cache_latent, cache_rotary, lengths,
):
    seqs = tokens.shape[0]
    kv_count, tp_count = lax.axis_size(KV), lax.axis_size(TP)
    heads = kv_count
    rope_width = cache_rotary.shape[2]
    rank = cache_latent.shape[2]
    pos_dev = cache_latent.shape[1]
    model_width = tokens.shape[1] * tp_count
    out_cols = w_out.shape[1]
    score_scale = w_query.shape[2] ** (-0.5)
    sds = jax.ShapeDtypeStruct

    hbm = pl.BlockSpec(memory_space=pltpu.HBM)
    smem = pl.BlockSpec(memory_space=pltpu.SMEM)
    width = tokens.shape[1]
    query_width = w_query.shape[2]
    partial = pl.pallas_call(
        project_kernel,
        out_shape=sds((32, LANES), F32),
        in_specs=[hbm] * 5,
        out_specs=whole(1)[0],
        scratch_shapes=[
            pltpu.VMEM((seqs, width), BF16),
            pltpu.VMEM((1, width), F32),
            pltpu.VMEM((query_width, width), BF16),
            pltpu.VMEM((rope_width, width), BF16),
            pltpu.VMEM((rope_width, width), BF16),
            pltpu.VMEM((32, LANES), F32),
            pltpu.SemaphoreType.DMA((5,)),
        ],
    )(tokens, norm_gain[None], w_query[:, 0].T, w_latent.T, w_rotary.T)

    pair = lax.broadcasted_iota(jnp.int32, (1, LANES), 1) % (rope_width // 2)
    frequency = THETA ** (-(2 * pair).astype(F32) / rope_width)
    cosine, sine, limits, key_up = pl.pallas_call(
        table_kernel,
        out_shape=(
            sds((seqs, LANES), F32),
            sds((seqs, LANES), F32),
            sds((seqs, LANES), jnp.int32),
            sds((w_key_up.shape[2], LANES), BF16),
        ),
        in_specs=[smem] + whole(2),
        out_specs=tuple(whole(4)),
        compiler_params=SMALL,
    )(lengths, frequency, w_key_up[:, 0].T)

    partial = pl.pallas_call(
        add_kernel,
        out_shape=sds((32, LANES), F32),
        in_specs=whole(2),
        out_specs=whole(1)[0],
        compiler_params=SMALL,
    )(partial, swapped(partial, "tp_1", 1))
    sums = [partial] + [swapped(partial, "tp_0", j) for j in (1, 2, 3)]
    block, new_rotary, own_slice, rope_dot = pl.pallas_call(
        functools.partial(query_kernel, float(model_width)),
        out_shape=(
            sds((heads, 32, LANES), BF16),
            sds((seqs, rope_width), BF16),
            sds((seqs, LANES), F32),
            sds((seqs, LANES), F32),
        ),
        in_specs=whole(7),
        out_specs=tuple(whole(4)),
        compiler_params=SMALL,
    )(*sums, cosine, sine, key_up)

    got = lax.all_to_all(block, KV, 0, 0, tiled=True)
    mine, side = pl.pallas_call(
        sort_kernel,
        out_shape=(sds((seqs, heads, LANES), BF16),) * 2,
        in_specs=whole(1),
        out_specs=tuple(whole(2)),
        compiler_params=SMALL,
    )(got)
    pieces = [swapped(mine, "tp_0", j) for j in (1, 2, 3)]

    new_latent, fresh_slice, latent_piece, value_up = pl.pallas_call(
        fresh_kernel,
        out_shape=(
            sds((seqs, rank), BF16),
            sds((seqs, LANES), F32),
            sds((4, seqs), BF16),
            sds((heads, rank, LANES), BF16),
        ),
        in_specs=whole(2) + [hbm],
        out_specs=tuple(whole(4)),
        scratch_shapes=[
            pltpu.VMEM((seqs, rank), F32),
            pltpu.VMEM(w_value_up.shape, BF16),
            pltpu.SemaphoreType.DMA((8,)),
        ],
        compiler_params=pltpu.CompilerParams(vmem_limit_bytes=40 * 1024 * 1024),
    )(side, latent_gain[None], w_value_up)
    pieces, value_up = lax.optimization_barrier((pieces, value_up))
    pieces = [mine] + pieces
    pieces = pieces + [swapped(piece, "tp_1", 1) for piece in pieces]

    pairs_gap = seqs * (heads + 1)
    values, own_value = pl.pallas_call(
        functools.partial(attend_kernel, score_scale),
        out_shape=(sds((heads, 32, LANES), BF16), sds((seqs, LANES), F32)),
        in_specs=whole(14),
        out_specs=tuple(whole(2)),
        scratch_shapes=[
            pltpu.VMEM((rank // LANES, seqs, heads, LANES), BF16),
            pltpu.VMEM((pairs_gap * (rank // LANES), LANES), F32),
            pltpu.VMEM((pairs_gap, LANES), F32),
            pltpu.VMEM((pairs_gap, LANES), F32),
        ],
        compiler_params=pltpu.CompilerParams(vmem_limit_bytes=20 * 1024 * 1024),
    )(
        limits, *pieces, side, new_latent, cache_rotary.transpose(0, 2, 1), cache_latent, value_up
    )

    arrived = lax.all_to_all(values, KV, 0, 0, tiled=True)
    state = pl.pallas_call(
        gather_kernel,
        out_shape=sds((32, LANES), F32),
        in_specs=whole(3),
        out_specs=whole(1)[0],
        scratch_shapes=[pltpu.VMEM((kv_count, 16, LANES), F32)] * 2,
        compiler_params=SMALL,
    )(arrived, own_slice, fresh_slice)
    state = pl.pallas_call(
        pair_kernel,
        out_shape=sds((32, LANES), F32),
        in_specs=whole(2),
        out_specs=whole(1)[0],
        compiler_params=SMALL,
    )(state, swapped(state, "tp_1", 1))
    states = [state] + [swapped(state, "tp_0", j) for j in (1, 2, 3)]
    block_shape = (seqs * out_cols // LANES, LANES)
    term = pl.pallas_call(
        functools.partial(finish_kernel, score_scale),
        out_shape=sds(block_shape, BF16),
        in_specs=whole(7),
        out_specs=whole(1)[0],
        compiler_params=SMALL,
    )(*states, rope_dot, own_value, w_out)
    terms = pl.pallas_call(
        ring_kernel,
        out_shape=sds((lax.axis_size("kv_0"), *block_shape), BF16),
        in_specs=whole(4),
        out_specs=whole(1)[0],
        compiler_params=SMALL,
    )(term, *[swapped(term, "kv_1", j) for j in (1, 2, 3)])
    terms = lax.all_to_all(terms, "kv_0", 0, 0, tiled=True)
    mixed_out = pl.pallas_call(
        total_kernel,
        out_shape=sds((seqs, out_cols), BF16),
        in_specs=whole(1),
        out_specs=whole(1)[0],
        compiler_params=SMALL,
    )(terms)
    return (mixed_out, latent_piece.T, new_rotary)


def solution(mesh):
    torus = Mesh(mesh.devices.reshape(8, 4, 4, 2), KV_TP)
    in_specs = (
        P(None, TP),
        P(TP),
        P(TP, KV, None),
        P(TP, KV),
        P(TP, None),
        P(),
        P(TP, KV, None),
        P(),
        P(KV, TP),
        P(None, KV_TP, None),
        P(None, KV_TP, None),
        P(),
    )
    out_specs = (P(None, TP), P(None, KV_TP), P())
    return jax.shard_map(
        shards, mesh=torus, in_specs=in_specs, out_specs=out_specs, check_vma=False
    )
```

```python
import functools

import jax
import jax.numpy as jnp
from jax import lax
from jax.experimental import pallas as pl
from jax.experimental.pallas import tpu as pltpu
from jax.sharding import Mesh
from jax.sharding import PartitionSpec as P

KV = ("kv_0", "kv_1")
TP = ("tp_0", "tp_1")
KV_TP = ("kv_0", "kv_1", "tp_0", "tp_1")


THETA = 10000.0
EPS = 1e-06
F32 = jnp.float32
BF16 = jnp.bfloat16
SMALL = pltpu.CompilerParams(vmem_limit_bytes=4 * 1024 * 1024)
FLOOR = -(2.0**127)
LANES = 128
NT = (((1,), (1,)), ((), ()))


def whole(count):
    return [pl.BlockSpec(memory_space=pltpu.VMEM)] * count


def lane_ids(rows):
    return lax.broadcasted_iota(jnp.int32, (rows, LANES), 1)


def swapped(value, axis, step):
    count = lax.axis_size(axis)
    return lax.ppermute(value, axis, [(i, i ^ step) for i in range(count)])


def fetch(pairs, sems):
    copies = [pltpu.make_async_copy(src, dst, sems.at[i]) for i, (src, dst) in enumerate(pairs)]
    for copy in copies:
        copy.start()
    return copies


def project_kernel(
    tokens_hbm, gain_hbm, query_hbm, latent_hbm, rotary_hbm, out_ref,
    tokens_s, gain_s, query_s, latent_s, rotary_s, sum_s, sems,
):
    copies = fetch(
        [
            (tokens_hbm, tokens_s), (gain_hbm, gain_s), (query_hbm, query_s),
            (latent_hbm, latent_s), (rotary_hbm, rotary_s),
        ],
        sems,
    )
    for copy in copies:
        copy.wait()
    tokens = tokens_s[...].astype(F32)
    scaled = (tokens * gain_s[...]).astype(BF16)
    squares = jnp.sum(tokens * tokens, axis=1, keepdims=True)
    sum_s[0:16, 0:96] = lax.dot_general(scaled, query_s[...], NT, preferred_element_type=F32)
    sum_s[0:16, 96:128] = lax.dot_general(scaled, latent_s[...], NT, preferred_element_type=F32)
    sum_s[16:32, :] = jnp.broadcast_to(squares, (16, LANES))
    sum_s[16:32, 0:32] = lax.dot_general(scaled, rotary_s[...], NT, preferred_element_type=F32)
    out_ref[...] = sum_s[...]


def hold_kernel(in_ref, out_ref):
    out_ref[...] = in_ref[...]


def add_kernel(a_ref, b_ref, out_ref):
    out_ref[...] = a_ref[...] + b_ref[...]


def table_kernel(
    lengths_ref, frequency_ref, key_in_ref, cos_ref, sin_ref, limit_ref, key_ref,
):
    row = lax.broadcasted_iota(jnp.int32, (16, LANES), 0)
    position = jnp.zeros((16, LANES), jnp.int32)
    for b in range(16):
        position = jnp.where(row == b, lengths_ref[b], position)
    angles = position.astype(F32) * frequency_ref[...]
    cos_ref[...] = jnp.cos(angles)
    sin_ref[...] = jnp.sin(angles)
    limit_ref[...] = position
    key_ref[...] = key_in_ref[...]


def query_kernel(
    model_width, a_ref, b_ref, c_ref, d_ref, cos_ref, sin_ref, key_ref,
    block_ref, rotary_ref, slice_ref, dot_ref,
):
    total = (a_ref[...] + b_ref[...]) + (c_ref[...] + d_ref[...])
    lane = lane_ids(16)
    low = (lane & 31) < 16
    first, second = total[0:16], total[16:32]
    squares = jnp.sum(jnp.where(lane == 64, second, 0.0), axis=1, keepdims=True)
    inverse = lax.rsqrt(squares / model_width + EPS)

    def rotated(v):
        turned = jnp.where(low, -pltpu.roll(v, LANES - 16, 1), pltpu.roll(v, 16, 1))
        return v * cos_ref[...] + turned * sin_ref[...]

    query = (first * inverse).astype(BF16)
    query_f = query.astype(F32)
    rope = rotated(query_f)
    fresh = rotated(second * inverse).astype(BF16)
    latent_query = jnp.dot(query[:, 0:64], key_ref[...], preferred_element_type=F32).astype(BF16)
    side = jnp.where(lane < 96, rope, query_f)
    side = pltpu.roll(jnp.where(lane < 64, 0.0, side), 64, 1).astype(BF16)
    for peer in range(block_ref.shape[0]):
        block_ref[peer, 0:16, :] = latent_query
        block_ref[peer, 16:32, :] = side
    rotary_ref[...] = fresh[:, 0:32]
    slice_ref[...] = latent_query.astype(F32)
    both = jnp.where(lane < 32, side.astype(F32) * fresh.astype(F32), 0.0)
    dot_ref[...] = jnp.broadcast_to(jnp.sum(both, axis=1, keepdims=True), (16, LANES))


def sort_kernel(block_ref, mine_ref, side_ref):
    mine_ref[...] = pltpu.einshape("hbr->bhr", block_ref[:, 0:16, :])
    side_ref[...] = pltpu.einshape("hbr->bhr", block_ref[:, 16:32, :])


def fresh_kernel(side_ref, gain_ref, fresh_ref, slice_ref, piece_ref, row_s):
    heads, width, rank = side_ref.shape[1], 32, gain_ref.shape[1]
    square = jnp.zeros((16, width), F32)
    for k in range(heads):
        block = side_ref[:, k, width : 2 * width].astype(F32)
        row_s[:, k * width : (k + 1) * width] = block
        square += block * block
    mean = jnp.sum(square, axis=1, keepdims=True) / rank
    fresh = (row_s[...] * lax.rsqrt(mean + EPS) * gain_ref[...]).astype(BF16)
    fresh_ref[...] = fresh
    row_s[...] = fresh.astype(F32)
    tp = lax.axis_index("tp_0") * 2 + lax.axis_index("tp_1")
    kv = lax.axis_index("kv_0") * 4 + lax.axis_index("kv_1")
    slice_ref[...] = row_s[:, pl.ds(pl.multiple_of(tp * LANES, LANES), LANES)]
    column = (kv * 8 + tp) * 4
    base = column // LANES
    held = row_s[:, pl.ds(pl.multiple_of(base * LANES, LANES), LANES)]
    held = pltpu.roll(held, (LANES - (column - base * LANES)) % LANES, 1)
    piece_ref[...] = held.T[0:4, :].astype(BF16)


def values_kernel(side_ref, value_hbm, value_ref, value_s, sems):
    chunks = sems.shape[0]
    part = value_s.shape[0] // chunks
    cut = lambda ref, i: ref.at[pl.ds(i * part, part)]
    copies = fetch([(cut(value_hbm, i), cut(value_s, i)) for i in range(chunks)], sems)
    step = 64
    for i in range(chunks):
        copies[i].wait()
        for j in range(i * part, (i + 1) * part, step):
            value_ref[:, j : j + step, :] = pltpu.einshape("rhv->hrv", value_s[j : j + step])


def attend_kernel(scale, limit_ref, *refs):
    pieces = refs[0:8]
    (side_ref, fresh_ref, rot_ref, cache_ref, value_ref, out_ref, own_ref) = refs[8:15]
    (q_s, o_s, m_s, l_s) = refs[15:]
    seqs, heads = 16, 32
    blocks, gap = q_s.shape[0], heads + 1

    chip, core = lax.axis_index("tp_0"), lax.axis_index("tp_1")
    kv = lax.axis_index("kv_0") * 4 + lax.axis_index("kv_1")
    first_pos = (kv * 8 + chip * 2 + core) * LANES
    for j in range(4):
        q_s[(chip ^ j) * 2 + core] = pieces[j][...]
        q_s[(chip ^ j) * 2 + 1 - core] = pieces[4 + j][...]
    group = 8
    for first in range(0, seqs, group):
        members = range(first, first + group)
        scores = []
        for b in members:
            query = jnp.concatenate([q_s[n, b] for n in range(blocks)], axis=1)
            term = lax.dot_general(query, cache_ref[b], NT, preferred_element_type=F32)
            term += jnp.dot(side_ref[b][:, 0:32], rot_ref[b], preferred_element_type=F32)
            scores.append(term)
        scores = jnp.concatenate(scores, axis=0) * scale
        limit = jnp.concatenate(
            [jnp.broadcast_to(limit_ref[b : b + 1, :], (heads, LANES)) for b in members], axis=0
        )
        valid = first_pos + lane_ids(heads * group) < limit
        top = jnp.max(jnp.where(valid, scores, FLOOR), axis=1, keepdims=True)
        weights = jnp.where(valid, jnp.exp(scores - top), 0.0)
        total = jnp.sum(weights, axis=1, keepdims=True)
        weights = weights.astype(BF16)
        for k, b in enumerate(members):
            part_rows = slice(k * heads, (k + 1) * heads)
            rows = slice(b * gap, b * gap + heads)
            summed = jnp.dot(weights[part_rows], cache_ref[b], preferred_element_type=F32)
            for n in range(blocks):
                at = (n * seqs + b) * gap
                o_s[at : at + heads, :] = summed[:, n * LANES : (n + 1) * LANES]
            m_s[rows, :] = jnp.broadcast_to(top[part_rows], (heads, LANES))
            l_s[rows, :] = jnp.broadcast_to(total[part_rows], (heads, LANES))
    lane = lane_ids(seqs)
    for h in range(heads):
        latent = jnp.concatenate(
            [o_s[pl.ds(n * seqs * gap + h, seqs, stride=gap), :] for n in range(blocks)], axis=1
        ).astype(BF16)
        out_ref[h, 0:16, :] = jnp.dot(
            latent, value_ref[h], preferred_element_type=F32
        ).astype(BF16)
        stats = jnp.zeros((seqs, LANES), F32)
        for at, ref in ((0, m_s), (3, l_s)):
            left = ref[pl.ds(h, seqs, stride=gap), :]
            for n in range(3):
                piece = left.astype(BF16).astype(F32)
                stats = jnp.where(lane == at + n, piece, stats)
                left = left - piece
        out_ref[h, 16:32, :] = stats.astype(BF16)
    own_ref[...] = jnp.dot(fresh_ref[...], value_ref[kv], preferred_element_type=F32)


def gather_kernel(parts_ref, slice_ref, fresh_ref, out_ref, m_s, l_s):
    count = parts_ref.shape[0]
    lane = lane_ids(16)
    top = jnp.full((16, LANES), FLOOR, F32)
    for k in range(count):
        stats = parts_ref[k, 16:32, :].astype(F32)
        m = jnp.sum(jnp.where(lane < 3, stats, 0.0), axis=1, keepdims=True)
        l = jnp.sum(jnp.where((lane >= 3) & (lane < 6), stats, 0.0), axis=1, keepdims=True)
        m = jnp.broadcast_to(m, (16, LANES))
        m_s[k] = m
        l_s[k] = jnp.broadcast_to(l, (16, LANES))
        top = jnp.maximum(top, m)
    total = jnp.zeros((16, LANES), F32)
    summed = jnp.zeros((16, LANES), F32)
    for k in range(count):
        factor = jnp.exp(m_s[k] - top)
        total += factor * l_s[k]
        summed += factor * parts_ref[k, 0:16, :].astype(F32)
    own = jnp.sum(slice_ref[...] * fresh_ref[...], axis=1, keepdims=True)
    stats = jnp.where(lane == 0, top, jnp.where(lane == 1, total, own))
    out_ref[0:16, :] = summed
    out_ref[16:32, :] = stats


def lane_of(stats, n):
    return jnp.sum(jnp.where(lane_ids(stats.shape[0]) == n, stats, 0.0), axis=1, keepdims=True)


def merged(refs):
    stats = [ref[16:32, :] for ref in refs]
    tops = [lane_of(s, 0) for s in stats]
    highest = functools.reduce(jnp.maximum, tops)
    factors = [jnp.exp(top - highest) for top in tops]
    summed = functools.reduce(jnp.add, [f * ref[0:16, :] for f, ref in zip(factors, refs)])
    total = functools.reduce(jnp.add, [f * lane_of(s, 1) for f, s in zip(factors, stats)])
    return summed, highest, total, functools.reduce(jnp.add, [lane_of(s, 2) for s in stats])


def pair_kernel(a_ref, b_ref, out_ref):
    summed, top, total, own = merged((a_ref, b_ref))
    lane = lane_ids(16)
    out_ref[0:16, :] = summed
    out_ref[16:32, :] = jnp.where(lane == 0, top, jnp.where(lane == 1, total, own))


def finish_kernel(scale, a_ref, b_ref, c_ref, d_ref, dot_ref, own_ref, weight_ref, out_ref):
    summed, top, total, own = merged((a_ref, b_ref, c_ref, d_ref))
    own = (own + dot_ref[...]) * scale
    highest = jnp.maximum(top, own)
    factor, own_weight = jnp.exp(top - highest), jnp.exp(own - highest)
    summed = factor * summed + own_weight * own_ref[...]
    head = (summed / (factor * total + own_weight)).astype(BF16)
    term = jnp.dot(head, weight_ref[...], preferred_element_type=F32).astype(BF16)
    for n in range(4):
        out_ref[16 * n : 16 * (n + 1), :] = term[:, LANES * n : LANES * (n + 1)]


def ring_kernel(a_ref, b_ref, c_ref, d_ref, out_ref):
    a, b, c, d = (ref[...].astype(F32) for ref in (a_ref, b_ref, c_ref, d_ref))
    term = ((a + b) + (c + d)).astype(BF16)
    for peer in range(out_ref.shape[0]):
        out_ref[peer] = term


def total_kernel(terms_ref, out_ref):
    for n in range(4):
        rows = slice(16 * n, 16 * (n + 1))
        total = terms_ref[0, rows, :].astype(F32)
        for k in range(1, terms_ref.shape[0]):
            total += terms_ref[k, rows, :].astype(F32)
        out_ref[:, LANES * n : LANES * (n + 1)] = total.astype(BF16)


def shards(
    tokens, norm_gain, w_query, w_latent, w_rotary, latent_gain, w_key_up, w_value_up, w_out,
    cache_latent, cache_rotary, lengths,
):
    seqs = tokens.shape[0]
    kv_count, tp_count = lax.axis_size(KV), lax.axis_size(TP)
    heads = kv_count
    rope_width = cache_rotary.shape[2]
    rank = cache_latent.shape[2]
    pos_dev = cache_latent.shape[1]
    model_width = tokens.shape[1] * tp_count
    out_cols = w_out.shape[1]
    score_scale = w_query.shape[2] ** (-0.5)
    sds = jax.ShapeDtypeStruct

    hbm = pl.BlockSpec(memory_space=pltpu.HBM)
    smem = pl.BlockSpec(memory_space=pltpu.SMEM)
    width = tokens.shape[1]
    query_width = w_query.shape[2]
    partial = pl.pallas_call(
        project_kernel,
        out_shape=sds((32, LANES), F32),
        in_specs=[hbm] * 5,
        out_specs=whole(1)[0],
        scratch_shapes=[
            pltpu.VMEM((seqs, width), BF16),
            pltpu.VMEM((1, width), F32),
            pltpu.VMEM((query_width, width), BF16),
            pltpu.VMEM((rope_width, width), BF16),
            pltpu.VMEM((rope_width, width), BF16),
            pltpu.VMEM((32, LANES), F32),
            pltpu.SemaphoreType.DMA((5,)),
        ],
    )(tokens, norm_gain[None], w_query[:, 0].T, w_latent.T, w_rotary.T)

    pair = lax.broadcasted_iota(jnp.int32, (1, LANES), 1) % (rope_width // 2)
    frequency = THETA ** (-(2 * pair).astype(F32) / rope_width)
    cosine, sine, limits, key_up = pl.pallas_call(
        table_kernel,
        out_shape=(
            sds((seqs, LANES), F32),
            sds((seqs, LANES), F32),
            sds((seqs, LANES), jnp.int32),
            sds((w_key_up.shape[2], LANES), BF16),
        ),
        in_specs=[smem] + whole(2),
        out_specs=tuple(whole(4)),
        compiler_params=SMALL,
    )(lengths, frequency, w_key_up[:, 0].T)

    other = swapped(partial, "tp_1", 1)
    held = pl.pallas_call(
        hold_kernel,
        out_shape=sds((32, LANES), F32),
        in_specs=whole(1),
        out_specs=whole(1)[0],
        compiler_params=SMALL,
    )(partial)
    partial = pl.pallas_call(
        add_kernel,
        out_shape=sds((32, LANES), F32),
        in_specs=whole(2),
        out_specs=whole(1)[0],
        compiler_params=SMALL,
    )(held, other)
    sums = [partial] + [swapped(partial, "tp_0", j) for j in (1, 2, 3)]
    block, new_rotary, own_slice, rope_dot = pl.pallas_call(
        functools.partial(query_kernel, float(model_width)),
        out_shape=(
            sds((heads, 32, LANES), BF16),
            sds((seqs, rope_width), BF16),
            sds((seqs, LANES), F32),
            sds((seqs, LANES), F32),
        ),
        in_specs=whole(7),
        out_specs=tuple(whole(4)),
        compiler_params=SMALL,
    )(*sums, cosine, sine, key_up)

    got = lax.all_to_all(block, KV, 0, 0, tiled=True)
    mine, side = pl.pallas_call(
        sort_kernel,
        out_shape=(sds((seqs, heads, LANES), BF16),) * 2,
        in_specs=whole(1),
        out_specs=tuple(whole(2)),
        compiler_params=SMALL,
    )(got)
    pieces = [swapped(mine, "tp_0", j) for j in (1, 2, 3)]

    value_up = pl.pallas_call(
        values_kernel,
        out_shape=sds((heads, rank, LANES), BF16),
        in_specs=whole(1) + [hbm],
        out_specs=whole(1)[0],
        scratch_shapes=[pltpu.VMEM(w_value_up.shape, BF16), pltpu.SemaphoreType.DMA((8,))],
        compiler_params=pltpu.CompilerParams(vmem_limit_bytes=40 * 1024 * 1024),
    )(side, w_value_up)
    pieces, value_up, side = lax.optimization_barrier((pieces, value_up, side))
    new_latent, fresh_slice, latent_piece = pl.pallas_call(
        fresh_kernel,
        out_shape=(sds((seqs, rank), BF16), sds((seqs, LANES), F32), sds((4, seqs), BF16)),
        in_specs=whole(2),
        out_specs=tuple(whole(3)),
        scratch_shapes=[pltpu.VMEM((seqs, rank), F32)],
        compiler_params=SMALL,
    )(side, latent_gain[None])
    pieces = [mine] + pieces
    pieces = pieces + [swapped(piece, "tp_1", 1) for piece in pieces]

    pairs_gap = seqs * (heads + 1)
    values, own_value = pl.pallas_call(
        functools.partial(attend_kernel, score_scale),
        out_shape=(sds((heads, 32, LANES), BF16), sds((seqs, LANES), F32)),
        in_specs=whole(14),
        out_specs=tuple(whole(2)),
        scratch_shapes=[
            pltpu.VMEM((rank // LANES, seqs, heads, LANES), BF16),
            pltpu.VMEM((pairs_gap * (rank // LANES), LANES), F32),
            pltpu.VMEM((pairs_gap, LANES), F32),
            pltpu.VMEM((pairs_gap, LANES), F32),
        ],
        compiler_params=pltpu.CompilerParams(vmem_limit_bytes=20 * 1024 * 1024),
    )(
        limits, *pieces, side, new_latent, cache_rotary.transpose(0, 2, 1), cache_latent, value_up
    )

    arrived = lax.all_to_all(values, KV, 0, 0, tiled=True)
    state = pl.pallas_call(
        gather_kernel,
        out_shape=sds((32, LANES), F32),
        in_specs=whole(3),
        out_specs=whole(1)[0],
        scratch_shapes=[pltpu.VMEM((kv_count, 16, LANES), F32)] * 2,
        compiler_params=SMALL,
    )(arrived, own_slice, fresh_slice)
    state = pl.pallas_call(
        pair_kernel,
        out_shape=sds((32, LANES), F32),
        in_specs=whole(2),
        out_specs=whole(1)[0],
        compiler_params=SMALL,
    )(state, swapped(state, "tp_1", 1))
    states = [state] + [swapped(state, "tp_0", j) for j in (1, 2, 3)]
    block_shape = (seqs * out_cols // LANES, LANES)
    term = pl.pallas_call(
        functools.partial(finish_kernel, score_scale),
        out_shape=sds(block_shape, BF16),
        in_specs=whole(7),
        out_specs=whole(1)[0],
        compiler_params=SMALL,
    )(*states, rope_dot, own_value, w_out)
    terms = pl.pallas_call(
        ring_kernel,
        out_shape=sds((lax.axis_size("kv_0"), *block_shape), BF16),
        in_specs=whole(4),
        out_specs=whole(1)[0],
        compiler_params=SMALL,
    )(term, *[swapped(term, "kv_1", j) for j in (1, 2, 3)])
    terms = lax.all_to_all(terms, "kv_0", 0, 0, tiled=True)
    mixed_out = pl.pallas_call(
        total_kernel,
        out_shape=sds((seqs, out_cols), BF16),
        in_specs=whole(1),
        out_specs=whole(1)[0],
        compiler_params=SMALL,
    )(terms)
    return (mixed_out, latent_piece.T, new_rotary)


def solution(mesh):
    torus = Mesh(mesh.devices.reshape(8, 4, 4, 2), KV_TP)
    in_specs = (
        P(None, TP),
        P(TP),
        P(TP, KV, None),
        P(TP, KV),
        P(TP, None),
        P(),
        P(TP, KV, None),
        P(),
        P(KV, TP),
        P(None, KV_TP, None),
        P(None, KV_TP, None),
        P(),
    )
    out_specs = (P(None, TP), P(None, KV_TP), P())
    return jax.shard_map(
        shards, mesh=torus, in_specs=in_specs, out_specs=out_specs, check_vma=False
    )
```

```python
import functools

import jax
import jax.numpy as jnp
from jax import lax
from jax.experimental import pallas as pl
from jax.experimental.pallas import tpu as pltpu
from jax.sharding import Mesh
from jax.sharding import PartitionSpec as P

KV = ("kv_0", "kv_1")
TP = ("tp_0", "tp_1")
KV_TP = ("kv_0", "kv_1", "tp_0", "tp_1")


THETA = 10000.0
EPS = 1e-06
F32 = jnp.float32
BF16 = jnp.bfloat16
SMALL = pltpu.CompilerParams(vmem_limit_bytes=4 * 1024 * 1024)
FLOOR = -(2.0**127)
LANES = 128
NT = (((1,), (1,)), ((), ()))


def whole(count):
    return [pl.BlockSpec(memory_space=pltpu.VMEM)] * count


def lane_ids(rows):
    return lax.broadcasted_iota(jnp.int32, (rows, LANES), 1)


def swapped(value, axis, step):
    count = lax.axis_size(axis)
    return lax.ppermute(value, axis, [(i, i ^ step) for i in range(count)])


def fetch(pairs, sems):
    copies = [pltpu.make_async_copy(src, dst, sems.at[i]) for i, (src, dst) in enumerate(pairs)]
    for copy in copies:
        copy.start()
    return copies


def project_kernel(
    tokens_hbm, gain_hbm, query_hbm, latent_hbm, rotary_hbm, out_ref,
    tokens_s, gain_s, query_s, latent_s, rotary_s, sum_s, sems,
):
    copies = fetch(
        [
            (tokens_hbm, tokens_s), (gain_hbm, gain_s), (query_hbm, query_s),
            (latent_hbm, latent_s), (rotary_hbm, rotary_s),
        ],
        sems,
    )
    for copy in copies:
        copy.wait()
    tokens = tokens_s[...].astype(F32)
    scaled = (tokens * gain_s[...]).astype(BF16)
    squares = jnp.sum(tokens * tokens, axis=1, keepdims=True)
    sum_s[0:16, 0:96] = lax.dot_general(scaled, query_s[...], NT, preferred_element_type=F32)
    sum_s[0:16, 96:128] = lax.dot_general(scaled, latent_s[...], NT, preferred_element_type=F32)
    sum_s[16:32, :] = jnp.broadcast_to(squares, (16, LANES))
    sum_s[16:32, 0:32] = lax.dot_general(scaled, rotary_s[...], NT, preferred_element_type=F32)
    out_ref[...] = sum_s[...]


def hold_kernel(in_ref, out_ref):
    out_ref[...] = in_ref[...]


def add_kernel(a_ref, b_ref, out_ref):
    out_ref[...] = a_ref[...] + b_ref[...]


def table_kernel(
    lengths_ref, frequency_ref, key_in_ref, cos_ref, sin_ref, limit_ref, key_ref,
):
    row = lax.broadcasted_iota(jnp.int32, (16, LANES), 0)
    position = jnp.zeros((16, LANES), jnp.int32)
    for b in range(16):
        position = jnp.where(row == b, lengths_ref[b], position)
    angles = position.astype(F32) * frequency_ref[...]
    cos_ref[...] = jnp.cos(angles)
    sin_ref[...] = jnp.sin(angles)
    limit_ref[...] = position
    key_ref[...] = key_in_ref[...]


def query_kernel(
    model_width, a_ref, b_ref, c_ref, d_ref, cos_ref, sin_ref, key_ref,
    block_ref, rotary_ref, slice_ref, dot_ref,
):
    total = (a_ref[...] + b_ref[...]) + (c_ref[...] + d_ref[...])
    lane = lane_ids(16)
    low = (lane & 31) < 16
    first, second = total[0:16], total[16:32]
    squares = jnp.sum(jnp.where(lane == 64, second, 0.0), axis=1, keepdims=True)
    inverse = lax.rsqrt(squares / model_width + EPS)

    def rotated(v):
        turned = jnp.where(low, -pltpu.roll(v, LANES - 16, 1), pltpu.roll(v, 16, 1))
        return v * cos_ref[...] + turned * sin_ref[...]

    query = (first * inverse).astype(BF16)
    query_f = query.astype(F32)
    rope = rotated(query_f)
    fresh = rotated(second * inverse).astype(BF16)
    latent_query = jnp.dot(query[:, 0:64], key_ref[...], preferred_element_type=F32).astype(BF16)
    side = jnp.where(lane < 96, rope, query_f)
    side = pltpu.roll(jnp.where(lane < 64, 0.0, side), 64, 1).astype(BF16)
    for peer in range(block_ref.shape[0]):
        block_ref[peer, 0:16, :] = latent_query
        block_ref[peer, 16:32, :] = side
    rotary_ref[...] = fresh[:, 0:32]
    slice_ref[...] = latent_query.astype(F32)
    both = jnp.where(lane < 32, side.astype(F32) * fresh.astype(F32), 0.0)
    dot_ref[...] = jnp.broadcast_to(jnp.sum(both, axis=1, keepdims=True), (16, LANES))


def sort_kernel(block_ref, mine_ref, side_ref):
    mine_ref[...] = pltpu.einshape("hbr->bhr", block_ref[:, 0:16, :])
    side_ref[...] = pltpu.einshape("hbr->bhr", block_ref[:, 16:32, :])


def fresh_kernel(side_ref, gain_ref, fresh_ref, slice_ref, piece_ref, row_s):
    heads, width, rank = side_ref.shape[1], 32, gain_ref.shape[1]
    square = jnp.zeros((16, width), F32)
    for k in range(heads):
        block = side_ref[:, k, width : 2 * width].astype(F32)
        row_s[:, k * width : (k + 1) * width] = block
        square += block * block
    mean = jnp.sum(square, axis=1, keepdims=True) / rank
    fresh = (row_s[...] * lax.rsqrt(mean + EPS) * gain_ref[...]).astype(BF16)
    fresh_ref[...] = fresh
    row_s[...] = fresh.astype(F32)
    tp = lax.axis_index("tp_0") * 2 + lax.axis_index("tp_1")
    kv = lax.axis_index("kv_0") * 4 + lax.axis_index("kv_1")
    slice_ref[...] = row_s[:, pl.ds(pl.multiple_of(tp * LANES, LANES), LANES)]
    column = (kv * 8 + tp) * 4
    base = column // LANES
    held = row_s[:, pl.ds(pl.multiple_of(base * LANES, LANES), LANES)]
    held = pltpu.roll(held, (LANES - (column - base * LANES)) % LANES, 1)
    piece_ref[...] = held.T[0:4, :].astype(BF16)


def values_kernel(side_ref, value_hbm, value_ref, value_s, sems):
    chunks = sems.shape[0]
    part = value_s.shape[0] // chunks
    cut = lambda ref, i: ref.at[pl.ds(i * part, part)]
    copies = fetch([(cut(value_hbm, i), cut(value_s, i)) for i in range(chunks)], sems)
    step = 64
    for i in range(chunks):
        copies[i].wait()
        for j in range(i * part, (i + 1) * part, step):
            value_ref[:, j : j + step, :] = pltpu.einshape("rhv->hrv", value_s[j : j + step])


def attend_kernel(scale, limit_ref, *refs):
    pieces = refs[0:8]
    (side_ref, fresh_ref, rot_ref, cache_ref, value_ref, out_ref, own_ref) = refs[8:15]
    (q_s, o_s, m_s, l_s) = refs[15:]
    seqs, heads = 16, 32
    blocks, gap = q_s.shape[0], heads + 1

    chip, core = lax.axis_index("tp_0"), lax.axis_index("tp_1")
    kv = lax.axis_index("kv_0") * 4 + lax.axis_index("kv_1")
    first_pos = (kv * 8 + chip * 2 + core) * LANES
    for j in range(4):
        q_s[(chip ^ j) * 2 + core] = pieces[j][...]
        q_s[(chip ^ j) * 2 + 1 - core] = pieces[4 + j][...]
    group = 8
    for first in range(0, seqs, group):
        members = range(first, first + group)
        scores = []
        for b in members:
            query = jnp.concatenate([q_s[n, b] for n in range(blocks)], axis=1)
            term = lax.dot_general(query, cache_ref[b], NT, preferred_element_type=F32)
            term += jnp.dot(side_ref[b][:, 0:32], rot_ref[b], preferred_element_type=F32)
            scores.append(term)
        scores = jnp.concatenate(scores, axis=0) * scale
        limit = jnp.concatenate(
            [jnp.broadcast_to(limit_ref[b : b + 1, :], (heads, LANES)) for b in members], axis=0
        )
        valid = first_pos + lane_ids(heads * group) < limit
        top = jnp.max(jnp.where(valid, scores, FLOOR), axis=1, keepdims=True)
        weights = jnp.where(valid, jnp.exp(scores - top), 0.0)
        total = jnp.sum(weights, axis=1, keepdims=True)
        weights = weights.astype(BF16)
        for k, b in enumerate(members):
            part_rows = slice(k * heads, (k + 1) * heads)
            rows = slice(b * gap, b * gap + heads)
            summed = jnp.dot(weights[part_rows], cache_ref[b], preferred_element_type=F32)
            for n in range(blocks):
                at = (n * seqs + b) * gap
                o_s[at : at + heads, :] = summed[:, n * LANES : (n + 1) * LANES]
            m_s[rows, :] = jnp.broadcast_to(top[part_rows], (heads, LANES))
            l_s[rows, :] = jnp.broadcast_to(total[part_rows], (heads, LANES))
    lane = lane_ids(seqs)
    for h in range(heads):
        latent = jnp.concatenate(
            [o_s[pl.ds(n * seqs * gap + h, seqs, stride=gap), :] for n in range(blocks)], axis=1
        ).astype(BF16)
        out_ref[h, 0:16, :] = jnp.dot(
            latent, value_ref[h], preferred_element_type=F32
        ).astype(BF16)
        stats = jnp.zeros((seqs, LANES), F32)
        for at, ref in ((0, m_s), (3, l_s)):
            left = ref[pl.ds(h, seqs, stride=gap), :]
            for n in range(3):
                piece = left.astype(BF16).astype(F32)
                stats = jnp.where(lane == at + n, piece, stats)
                left = left - piece
        out_ref[h, 16:32, :] = stats.astype(BF16)
    own_ref[...] = jnp.dot(fresh_ref[...], value_ref[kv], preferred_element_type=F32)


def gather_kernel(parts_ref, slice_ref, fresh_ref, out_ref, m_s, l_s):
    count = parts_ref.shape[0]
    lane = lane_ids(16)
    top = jnp.full((16, LANES), FLOOR, F32)
    for k in range(count):
        stats = parts_ref[k, 16:32, :].astype(F32)
        m = jnp.sum(jnp.where(lane < 3, stats, 0.0), axis=1, keepdims=True)
        l = jnp.sum(jnp.where((lane >= 3) & (lane < 6), stats, 0.0), axis=1, keepdims=True)
        m = jnp.broadcast_to(m, (16, LANES))
        m_s[k] = m
        l_s[k] = jnp.broadcast_to(l, (16, LANES))
        top = jnp.maximum(top, m)
    total = jnp.zeros((16, LANES), F32)
    summed = jnp.zeros((16, LANES), F32)
    for k in range(count):
        factor = jnp.exp(m_s[k] - top)
        total += factor * l_s[k]
        summed += factor * parts_ref[k, 0:16, :].astype(F32)
    own = jnp.sum(slice_ref[...] * fresh_ref[...], axis=1, keepdims=True)
    stats = jnp.where(lane == 0, top, jnp.where(lane == 1, total, own))
    out_ref[0:16, :] = summed
    out_ref[16:32, :] = stats


def lane_of(stats, n):
    return jnp.sum(jnp.where(lane_ids(stats.shape[0]) == n, stats, 0.0), axis=1, keepdims=True)


def merged(refs):
    stats = [ref[16:32, :] for ref in refs]
    tops = [lane_of(s, 0) for s in stats]
    highest = functools.reduce(jnp.maximum, tops)
    factors = [jnp.exp(top - highest) for top in tops]
    summed = functools.reduce(jnp.add, [f * ref[0:16, :] for f, ref in zip(factors, refs)])
    total = functools.reduce(jnp.add, [f * lane_of(s, 1) for f, s in zip(factors, stats)])
    return summed, highest, total, functools.reduce(jnp.add, [lane_of(s, 2) for s in stats])


def pair_kernel(a_ref, b_ref, out_ref):
    summed, top, total, own = merged((a_ref, b_ref))
    lane = lane_ids(16)
    out_ref[0:16, :] = summed
    out_ref[16:32, :] = jnp.where(lane == 0, top, jnp.where(lane == 1, total, own))


def finish_kernel(scale, a_ref, b_ref, c_ref, d_ref, dot_ref, own_ref, weight_ref, out_ref):
    summed, top, total, own = merged((a_ref, b_ref, c_ref, d_ref))
    own = (own + dot_ref[...]) * scale
    highest = jnp.maximum(top, own)
    factor, own_weight = jnp.exp(top - highest), jnp.exp(own - highest)
    summed = factor * summed + own_weight * own_ref[...]
    head = (summed / (factor * total + own_weight)).astype(BF16)
    term = jnp.dot(head, weight_ref[...], preferred_element_type=F32).astype(BF16)
    for n in range(4):
        out_ref[16 * n : 16 * (n + 1), :] = term[:, LANES * n : LANES * (n + 1)]


def ring_kernel(a_ref, b_ref, c_ref, d_ref, out_ref):
    a, b, c, d = (ref[...].astype(F32) for ref in (a_ref, b_ref, c_ref, d_ref))
    term = ((a + b) + (c + d)).astype(BF16)
    for peer in range(out_ref.shape[0]):
        out_ref[peer] = term


def total_kernel(terms_ref, out_ref):
    for n in range(4):
        rows = slice(16 * n, 16 * (n + 1))
        total = terms_ref[0, rows, :].astype(F32)
        for k in range(1, terms_ref.shape[0]):
            total += terms_ref[k, rows, :].astype(F32)
        out_ref[:, LANES * n : LANES * (n + 1)] = total.astype(BF16)


def shards(
    tokens, norm_gain, w_query, w_latent, w_rotary, latent_gain, w_key_up, w_value_up, w_out,
    cache_latent, cache_rotary, lengths,
):
    seqs = tokens.shape[0]
    kv_count, tp_count = lax.axis_size(KV), lax.axis_size(TP)
    heads = kv_count
    rope_width = cache_rotary.shape[2]
    rank = cache_latent.shape[2]
    pos_dev = cache_latent.shape[1]
    model_width = tokens.shape[1] * tp_count
    out_cols = w_out.shape[1]
    score_scale = w_query.shape[2] ** (-0.5)
    sds = jax.ShapeDtypeStruct

    hbm = pl.BlockSpec(memory_space=pltpu.HBM)
    smem = pl.BlockSpec(memory_space=pltpu.SMEM)
    width = tokens.shape[1]
    query_width = w_query.shape[2]
    partial = pl.pallas_call(
        project_kernel,
        out_shape=sds((32, LANES), F32),
        in_specs=[hbm] * 5,
        out_specs=whole(1)[0],
        scratch_shapes=[
            pltpu.VMEM((seqs, width), BF16),
            pltpu.VMEM((1, width), F32),
            pltpu.VMEM((query_width, width), BF16),
            pltpu.VMEM((rope_width, width), BF16),
            pltpu.VMEM((rope_width, width), BF16),
            pltpu.VMEM((32, LANES), F32),
            pltpu.SemaphoreType.DMA((5,)),
        ],
    )(tokens, norm_gain[None], w_query[:, 0].T, w_latent.T, w_rotary.T)

    pair = lax.broadcasted_iota(jnp.int32, (1, LANES), 1) % (rope_width // 2)
    frequency = THETA ** (-(2 * pair).astype(F32) / rope_width)
    cosine, sine, limits, key_up = pl.pallas_call(
        table_kernel,
        out_shape=(
            sds((seqs, LANES), F32),
            sds((seqs, LANES), F32),
            sds((seqs, LANES), jnp.int32),
            sds((w_key_up.shape[2], LANES), BF16),
        ),
        in_specs=[smem] + whole(2),
        out_specs=tuple(whole(4)),
        compiler_params=SMALL,
    )(lengths, frequency, w_key_up[:, 0].T)

    other = swapped(partial, "tp_1", 1)
    held = pl.pallas_call(
        hold_kernel,
        out_shape=sds((32, LANES), F32),
        in_specs=whole(1),
        out_specs=whole(1)[0],
        compiler_params=SMALL,
    )(partial)
    partial = pl.pallas_call(
        add_kernel,
        out_shape=sds((32, LANES), F32),
        in_specs=whole(2),
        out_specs=whole(1)[0],
        compiler_params=SMALL,
    )(held, other)
    sums = [partial] + [swapped(partial, "tp_0", j) for j in (1, 2, 3)]
    block, new_rotary, own_slice, rope_dot = pl.pallas_call(
        functools.partial(query_kernel, float(model_width)),
        out_shape=(
            sds((heads, 32, LANES), BF16),
            sds((seqs, rope_width), BF16),
            sds((seqs, LANES), F32),
            sds((seqs, LANES), F32),
        ),
        in_specs=whole(7),
        out_specs=tuple(whole(4)),
        compiler_params=SMALL,
    )(*sums, cosine, sine, key_up)

    got = lax.all_to_all(block, KV, 0, 0, tiled=True)
    mine, side = pl.pallas_call(
        sort_kernel,
        out_shape=(sds((seqs, heads, LANES), BF16),) * 2,
        in_specs=whole(1),
        out_specs=tuple(whole(2)),
        compiler_params=SMALL,
    )(got)
    pieces = [swapped(mine, "tp_0", j) for j in (1, 2, 3)]

    value_up = pl.pallas_call(
        values_kernel,
        out_shape=sds((heads, rank, LANES), BF16),
        in_specs=whole(1) + [hbm],
        out_specs=whole(1)[0],
        scratch_shapes=[pltpu.VMEM(w_value_up.shape, BF16), pltpu.SemaphoreType.DMA((8,))],
        compiler_params=pltpu.CompilerParams(vmem_limit_bytes=40 * 1024 * 1024),
    )(side, w_value_up)
    pieces, value_up, side, mine = lax.optimization_barrier((pieces, value_up, side, mine))
    new_latent, fresh_slice, latent_piece = pl.pallas_call(
        fresh_kernel,
        out_shape=(sds((seqs, rank), BF16), sds((seqs, LANES), F32), sds((4, seqs), BF16)),
        in_specs=whole(2),
        out_specs=tuple(whole(3)),
        scratch_shapes=[pltpu.VMEM((seqs, rank), F32)],
        compiler_params=SMALL,
    )(side, latent_gain[None])
    pieces = [mine] + pieces
    pieces = pieces + [swapped(piece, "tp_1", 1) for piece in pieces]

    pairs_gap = seqs * (heads + 1)
    values, own_value = pl.pallas_call(
        functools.partial(attend_kernel, score_scale),
        out_shape=(sds((heads, 32, LANES), BF16), sds((seqs, LANES), F32)),
        in_specs=whole(14),
        out_specs=tuple(whole(2)),
        scratch_shapes=[
            pltpu.VMEM((rank // LANES, seqs, heads, LANES), BF16),
            pltpu.VMEM((pairs_gap * (rank // LANES), LANES), F32),
            pltpu.VMEM((pairs_gap, LANES), F32),
            pltpu.VMEM((pairs_gap, LANES), F32),
        ],
        compiler_params=pltpu.CompilerParams(vmem_limit_bytes=20 * 1024 * 1024),
    )(
        limits, *pieces, side, new_latent, cache_rotary.transpose(0, 2, 1), cache_latent, value_up
    )

    arrived = lax.all_to_all(values, KV, 0, 0, tiled=True)
    state = pl.pallas_call(
        gather_kernel,
        out_shape=sds((32, LANES), F32),
        in_specs=whole(3),
        out_specs=whole(1)[0],
        scratch_shapes=[pltpu.VMEM((kv_count, 16, LANES), F32)] * 2,
        compiler_params=SMALL,
    )(arrived, own_slice, fresh_slice)
    state = pl.pallas_call(
        pair_kernel,
        out_shape=sds((32, LANES), F32),
        in_specs=whole(2),
        out_specs=whole(1)[0],
        compiler_params=SMALL,
    )(state, swapped(state, "tp_1", 1))
    states = [state] + [swapped(state, "tp_0", j) for j in (1, 2, 3)]
    block_shape = (seqs * out_cols // LANES, LANES)
    term = pl.pallas_call(
        functools.partial(finish_kernel, score_scale),
        out_shape=sds(block_shape, BF16),
        in_specs=whole(7),
        out_specs=whole(1)[0],
        compiler_params=SMALL,
    )(*states, rope_dot, own_value, w_out)
    terms = pl.pallas_call(
        ring_kernel,
        out_shape=sds((lax.axis_size("kv_0"), *block_shape), BF16),
        in_specs=whole(4),
        out_specs=whole(1)[0],
        compiler_params=SMALL,
    )(term, *[swapped(term, "kv_1", j) for j in (1, 2, 3)])
    terms = lax.all_to_all(terms, "kv_0", 0, 0, tiled=True)
    mixed_out = pl.pallas_call(
        total_kernel,
        out_shape=sds((seqs, out_cols), BF16),
        in_specs=whole(1),
        out_specs=whole(1)[0],
        compiler_params=SMALL,
    )(terms)
    return (mixed_out, latent_piece.T, new_rotary)


def solution(mesh):
    torus = Mesh(mesh.devices.reshape(8, 4, 4, 2), KV_TP)
    in_specs = (
        P(None, TP),
        P(TP),
        P(TP, KV, None),
        P(TP, KV),
        P(TP, None),
        P(),
        P(TP, KV, None),
        P(),
        P(KV, TP),
        P(None, KV_TP, None),
        P(None, KV_TP, None),
        P(),
    )
    out_specs = (P(None, TP), P(None, KV_TP), P())
    return jax.shard_map(
        shards, mesh=torus, in_specs=in_specs, out_specs=out_specs, check_vma=False
    )
```

```python
import functools

import jax
import jax.numpy as jnp
from jax import lax
from jax.experimental import pallas as pl
from jax.experimental.pallas import tpu as pltpu
from jax.sharding import Mesh
from jax.sharding import PartitionSpec as P

KV = ("kv_0", "kv_1")
TP = ("tp_0", "tp_1")
KV_TP = ("kv_0", "kv_1", "tp_0", "tp_1")


THETA = 10000.0
EPS = 1e-06
F32 = jnp.float32
BF16 = jnp.bfloat16
SMALL = pltpu.CompilerParams(vmem_limit_bytes=4 * 1024 * 1024)
FLOOR = -(2.0**127)
LANES = 128
NT = (((1,), (1,)), ((), ()))


def whole(count):
    return [pl.BlockSpec(memory_space=pltpu.VMEM)] * count


def lane_ids(rows):
    return lax.broadcasted_iota(jnp.int32, (rows, LANES), 1)


def swapped(value, axis, step):
    count = lax.axis_size(axis)
    return lax.ppermute(value, axis, [(i, i ^ step) for i in range(count)])


def fetch(pairs, sems):
    copies = [pltpu.make_async_copy(src, dst, sems.at[i]) for i, (src, dst) in enumerate(pairs)]
    for copy in copies:
        copy.start()
    return copies


def project_kernel(
    tokens_hbm, gain_hbm, query_hbm, latent_hbm, rotary_hbm, out_ref,
    tokens_s, gain_s, query_s, latent_s, rotary_s, sum_s, sems,
):
    copies = fetch(
        [
            (tokens_hbm, tokens_s), (gain_hbm, gain_s), (query_hbm, query_s),
            (latent_hbm, latent_s), (rotary_hbm, rotary_s),
        ],
        sems,
    )
    for copy in copies:
        copy.wait()
    tokens = tokens_s[...].astype(F32)
    scaled = (tokens * gain_s[...]).astype(BF16)
    squares = jnp.sum(tokens * tokens, axis=1, keepdims=True)
    sum_s[0:16, 0:96] = lax.dot_general(scaled, query_s[...], NT, preferred_element_type=F32)
    sum_s[0:16, 96:128] = lax.dot_general(scaled, latent_s[...], NT, preferred_element_type=F32)
    sum_s[16:32, :] = jnp.broadcast_to(squares, (16, LANES))
    sum_s[16:32, 0:32] = lax.dot_general(scaled, rotary_s[...], NT, preferred_element_type=F32)
    out_ref[...] = sum_s[...]


def hold_kernel(in_ref, out_ref):
    out_ref[...] = in_ref[...]


def add_kernel(a_ref, b_ref, out_ref):
    out_ref[...] = a_ref[...] + b_ref[...]


def table_kernel(
    lengths_ref, frequency_ref, key_in_ref, cos_ref, sin_ref, limit_ref, key_ref,
):
    row = lax.broadcasted_iota(jnp.int32, (16, LANES), 0)
    position = jnp.zeros((16, LANES), jnp.int32)
    for b in range(16):
        position = jnp.where(row == b, lengths_ref[b], position)
    angles = position.astype(F32) * frequency_ref[...]
    cos_ref[...] = jnp.cos(angles)
    sin_ref[...] = jnp.sin(angles)
    limit_ref[...] = position
    key_ref[...] = key_in_ref[...]


def query_kernel(
    model_width, a_ref, b_ref, c_ref, d_ref, cos_ref, sin_ref, key_ref,
    block_ref, rotary_ref, slice_ref, dot_ref,
):
    total = (a_ref[...] + b_ref[...]) + (c_ref[...] + d_ref[...])
    lane = lane_ids(16)
    low = (lane & 31) < 16
    first, second = total[0:16], total[16:32]
    squares = jnp.sum(jnp.where(lane == 64, second, 0.0), axis=1, keepdims=True)
    inverse = lax.rsqrt(squares / model_width + EPS)

    def rotated(v):
        turned = jnp.where(low, -pltpu.roll(v, LANES - 16, 1), pltpu.roll(v, 16, 1))
        return v * cos_ref[...] + turned * sin_ref[...]

    query = (first * inverse).astype(BF16)
    query_f = query.astype(F32)
    rope = rotated(query_f)
    fresh = rotated(second * inverse).astype(BF16)
    latent_query = jnp.dot(query[:, 0:64], key_ref[...], preferred_element_type=F32).astype(BF16)
    side = jnp.where(lane < 96, rope, query_f)
    side = pltpu.roll(jnp.where(lane < 64, 0.0, side), 64, 1).astype(BF16)
    for peer in range(block_ref.shape[0]):
        block_ref[peer, 0:16, :] = latent_query
        block_ref[peer, 16:32, :] = side
    rotary_ref[...] = fresh[:, 0:32]
    slice_ref[...] = latent_query.astype(F32)
    both = jnp.where(lane < 32, side.astype(F32) * fresh.astype(F32), 0.0)
    dot_ref[...] = jnp.broadcast_to(jnp.sum(both, axis=1, keepdims=True), (16, LANES))


def sort_kernel(block_ref, mine_ref, side_ref):
    mine_ref[...] = pltpu.einshape("hbr->bhr", block_ref[:, 0:16, :])
    side_ref[...] = pltpu.einshape("hbr->bhr", block_ref[:, 16:32, :])


def fresh_kernel(side_ref, gain_ref, fresh_ref, slice_ref, piece_ref, row_s):
    heads, width, rank = side_ref.shape[1], 32, gain_ref.shape[1]
    square = jnp.zeros((16, width), F32)
    for k in range(heads):
        block = side_ref[:, k, width : 2 * width].astype(F32)
        row_s[:, k * width : (k + 1) * width] = block
        square += block * block
    mean = jnp.sum(square, axis=1, keepdims=True) / rank
    fresh = (row_s[...] * lax.rsqrt(mean + EPS) * gain_ref[...]).astype(BF16)
    fresh_ref[...] = fresh
    row_s[...] = fresh.astype(F32)
    tp = lax.axis_index("tp_0") * 2 + lax.axis_index("tp_1")
    kv = lax.axis_index("kv_0") * 4 + lax.axis_index("kv_1")
    slice_ref[...] = row_s[:, pl.ds(pl.multiple_of(tp * LANES, LANES), LANES)]
    column = (kv * 8 + tp) * 4
    base = column // LANES
    held = row_s[:, pl.ds(pl.multiple_of(base * LANES, LANES), LANES)]
    held = pltpu.roll(held, (LANES - (column - base * LANES)) % LANES, 1)
    piece_ref[...] = held.T[0:4, :].astype(BF16)


def values_kernel(side_ref, value_hbm, value_ref, value_s, sems):
    chunks = sems.shape[0]
    part = value_s.shape[0] // chunks
    cut = lambda ref, i: ref.at[pl.ds(i * part, part)]
    copies = fetch([(cut(value_hbm, i), cut(value_s, i)) for i in range(chunks)], sems)
    step = 64
    for i in range(chunks):
        copies[i].wait()
        for j in range(i * part, (i + 1) * part, step):
            value_ref[:, j : j + step, :] = pltpu.einshape("rhv->hrv", value_s[j : j + step])


def attend_kernel(scale, limit_ref, *refs):
    pieces = refs[0:8]
    (side_ref, fresh_ref, rot_ref, cache_ref, value_ref, out_ref, own_ref) = refs[8:15]
    (q_s, o_s, m_s, l_s) = refs[15:]
    seqs, heads = 16, 32
    blocks, gap = q_s.shape[0], heads + 1

    chip, core = lax.axis_index("tp_0"), lax.axis_index("tp_1")
    kv = lax.axis_index("kv_0") * 4 + lax.axis_index("kv_1")
    first_pos = (kv * 8 + chip * 2 + core) * LANES
    for j in range(4):
        q_s[(chip ^ j) * 2 + core] = pieces[j][...]
        q_s[(chip ^ j) * 2 + 1 - core] = pieces[4 + j][...]
    group = 16
    for first in range(0, seqs, group):
        members = range(first, first + group)
        scores = []
        for b in members:
            query = jnp.concatenate([q_s[n, b] for n in range(blocks)], axis=1)
            term = lax.dot_general(query, cache_ref[b], NT, preferred_element_type=F32)
            term += jnp.dot(side_ref[b][:, 0:32], rot_ref[b], preferred_element_type=F32)
            scores.append(term)
        scores = jnp.concatenate(scores, axis=0) * scale
        limit = jnp.concatenate(
            [jnp.broadcast_to(limit_ref[b : b + 1, :], (heads, LANES)) for b in members], axis=0
        )
        valid = first_pos + lane_ids(heads * group) < limit
        top = jnp.max(jnp.where(valid, scores, FLOOR), axis=1, keepdims=True)
        weights = jnp.where(valid, jnp.exp(scores - top), 0.0)
        total = jnp.sum(weights, axis=1, keepdims=True)
        weights = weights.astype(BF16)
        for k, b in enumerate(members):
            part_rows = slice(k * heads, (k + 1) * heads)
            rows = slice(b * gap, b * gap + heads)
            summed = jnp.dot(weights[part_rows], cache_ref[b], preferred_element_type=F32)
            for n in range(blocks):
                at = (n * seqs + b) * gap
                o_s[at : at + heads, :] = summed[:, n * LANES : (n + 1) * LANES]
            m_s[rows, :] = jnp.broadcast_to(top[part_rows], (heads, LANES))
            l_s[rows, :] = jnp.broadcast_to(total[part_rows], (heads, LANES))
    lane = lane_ids(seqs)
    for h in range(heads):
        latent = jnp.concatenate(
            [o_s[pl.ds(n * seqs * gap + h, seqs, stride=gap), :] for n in range(blocks)], axis=1
        ).astype(BF16)
        out_ref[h, 0:16, :] = jnp.dot(
            latent, value_ref[h], preferred_element_type=F32
        ).astype(BF16)
        stats = jnp.zeros((seqs, LANES), F32)
        for at, ref in ((0, m_s), (3, l_s)):
            left = ref[pl.ds(h, seqs, stride=gap), :]
            for n in range(3):
                piece = left.astype(BF16).astype(F32)
                stats = jnp.where(lane == at + n, piece, stats)
                left = left - piece
        out_ref[h, 16:32, :] = stats.astype(BF16)
    own_ref[...] = jnp.dot(fresh_ref[...], value_ref[kv], preferred_element_type=F32)


def gather_kernel(parts_ref, slice_ref, fresh_ref, out_ref, m_s, l_s):
    count = parts_ref.shape[0]
    lane = lane_ids(16)
    top = jnp.full((16, LANES), FLOOR, F32)
    for k in range(count):
        stats = parts_ref[k, 16:32, :].astype(F32)
        m = jnp.sum(jnp.where(lane < 3, stats, 0.0), axis=1, keepdims=True)
        l = jnp.sum(jnp.where((lane >= 3) & (lane < 6), stats, 0.0), axis=1, keepdims=True)
        m = jnp.broadcast_to(m, (16, LANES))
        m_s[k] = m
        l_s[k] = jnp.broadcast_to(l, (16, LANES))
        top = jnp.maximum(top, m)
    total = jnp.zeros((16, LANES), F32)
    summed = jnp.zeros((16, LANES), F32)
    for k in range(count):
        factor = jnp.exp(m_s[k] - top)
        total += factor * l_s[k]
        summed += factor * parts_ref[k, 0:16, :].astype(F32)
    own = jnp.sum(slice_ref[...] * fresh_ref[...], axis=1, keepdims=True)
    stats = jnp.where(lane == 0, top, jnp.where(lane == 1, total, own))
    out_ref[0:16, :] = summed
    out_ref[16:32, :] = stats


def lane_of(stats, n):
    return jnp.sum(jnp.where(lane_ids(stats.shape[0]) == n, stats, 0.0), axis=1, keepdims=True)


def merged(refs):
    stats = [ref[16:32, :] for ref in refs]
    tops = [lane_of(s, 0) for s in stats]
    highest = functools.reduce(jnp.maximum, tops)
    factors = [jnp.exp(top - highest) for top in tops]
    summed = functools.reduce(jnp.add, [f * ref[0:16, :] for f, ref in zip(factors, refs)])
    total = functools.reduce(jnp.add, [f * lane_of(s, 1) for f, s in zip(factors, stats)])
    return summed, highest, total, functools.reduce(jnp.add, [lane_of(s, 2) for s in stats])


def pair_kernel(a_ref, b_ref, out_ref):
    summed, top, total, own = merged((a_ref, b_ref))
    lane = lane_ids(16)
    out_ref[0:16, :] = summed
    out_ref[16:32, :] = jnp.where(lane == 0, top, jnp.where(lane == 1, total, own))


def finish_kernel(scale, a_ref, b_ref, c_ref, d_ref, dot_ref, own_ref, weight_ref, out_ref):
    summed, top, total, own = merged((a_ref, b_ref, c_ref, d_ref))
    own = (own + dot_ref[...]) * scale
    highest = jnp.maximum(top, own)
    factor, own_weight = jnp.exp(top - highest), jnp.exp(own - highest)
    summed = factor * summed + own_weight * own_ref[...]
    head = (summed / (factor * total + own_weight)).astype(BF16)
    term = jnp.dot(head, weight_ref[...], preferred_element_type=F32).astype(BF16)
    for n in range(4):
        out_ref[16 * n : 16 * (n + 1), :] = term[:, LANES * n : LANES * (n + 1)]


def ring_kernel(a_ref, b_ref, c_ref, d_ref, out_ref):
    a, b, c, d = (ref[...].astype(F32) for ref in (a_ref, b_ref, c_ref, d_ref))
    term = ((a + b) + (c + d)).astype(BF16)
    for peer in range(out_ref.shape[0]):
        out_ref[peer] = term


def total_kernel(terms_ref, out_ref):
    for n in range(4):
        rows = slice(16 * n, 16 * (n + 1))
        total = terms_ref[0, rows, :].astype(F32)
        for k in range(1, terms_ref.shape[0]):
            total += terms_ref[k, rows, :].astype(F32)
        out_ref[:, LANES * n : LANES * (n + 1)] = total.astype(BF16)


def shards(
    tokens, norm_gain, w_query, w_latent, w_rotary, latent_gain, w_key_up, w_value_up, w_out,
    cache_latent, cache_rotary, lengths,
):
    seqs = tokens.shape[0]
    kv_count, tp_count = lax.axis_size(KV), lax.axis_size(TP)
    heads = kv_count
    rope_width = cache_rotary.shape[2]
    rank = cache_latent.shape[2]
    pos_dev = cache_latent.shape[1]
    model_width = tokens.shape[1] * tp_count
    out_cols = w_out.shape[1]
    score_scale = w_query.shape[2] ** (-0.5)
    sds = jax.ShapeDtypeStruct

    hbm = pl.BlockSpec(memory_space=pltpu.HBM)
    smem = pl.BlockSpec(memory_space=pltpu.SMEM)
    width = tokens.shape[1]
    query_width = w_query.shape[2]
    partial = pl.pallas_call(
        project_kernel,
        out_shape=sds((32, LANES), F32),
        in_specs=[hbm] * 5,
        out_specs=whole(1)[0],
        scratch_shapes=[
            pltpu.VMEM((seqs, width), BF16),
            pltpu.VMEM((1, width), F32),
            pltpu.VMEM((query_width, width), BF16),
            pltpu.VMEM((rope_width, width), BF16),
            pltpu.VMEM((rope_width, width), BF16),
            pltpu.VMEM((32, LANES), F32),
            pltpu.SemaphoreType.DMA((5,)),
        ],
    )(tokens, norm_gain[None], w_query[:, 0].T, w_latent.T, w_rotary.T)

    pair = lax.broadcasted_iota(jnp.int32, (1, LANES), 1) % (rope_width // 2)
    frequency = THETA ** (-(2 * pair).astype(F32) / rope_width)
    cosine, sine, limits, key_up = pl.pallas_call(
        table_kernel,
        out_shape=(
            sds((seqs, LANES), F32),
            sds((seqs, LANES), F32),
            sds((seqs, LANES), jnp.int32),
            sds((w_key_up.shape[2], LANES), BF16),
        ),
        in_specs=[smem] + whole(2),
        out_specs=tuple(whole(4)),
        compiler_params=SMALL,
    )(lengths, frequency, w_key_up[:, 0].T)

    other = swapped(partial, "tp_1", 1)
    held = pl.pallas_call(
        hold_kernel,
        out_shape=sds((32, LANES), F32),
        in_specs=whole(1),
        out_specs=whole(1)[0],
        compiler_params=SMALL,
    )(partial)
    partial = pl.pallas_call(
        add_kernel,
        out_shape=sds((32, LANES), F32),
        in_specs=whole(2),
        out_specs=whole(1)[0],
        compiler_params=SMALL,
    )(held, other)
    sums = [partial] + [swapped(partial, "tp_0", j) for j in (1, 2, 3)]
    block, new_rotary, own_slice, rope_dot = pl.pallas_call(
        functools.partial(query_kernel, float(model_width)),
        out_shape=(
            sds((heads, 32, LANES), BF16),
            sds((seqs, rope_width), BF16),
            sds((seqs, LANES), F32),
            sds((seqs, LANES), F32),
        ),
        in_specs=whole(7),
        out_specs=tuple(whole(4)),
        compiler_params=SMALL,
    )(*sums, cosine, sine, key_up)

    got = lax.all_to_all(block, KV, 0, 0, tiled=True)
    mine, side = pl.pallas_call(
        sort_kernel,
        out_shape=(sds((seqs, heads, LANES), BF16),) * 2,
        in_specs=whole(1),
        out_specs=tuple(whole(2)),
        compiler_params=SMALL,
    )(got)
    pieces = [swapped(mine, "tp_0", j) for j in (1, 2, 3)]

    value_up = pl.pallas_call(
        values_kernel,
        out_shape=sds((heads, rank, LANES), BF16),
        in_specs=whole(1) + [hbm],
        out_specs=whole(1)[0],
        scratch_shapes=[pltpu.VMEM(w_value_up.shape, BF16), pltpu.SemaphoreType.DMA((8,))],
        compiler_params=pltpu.CompilerParams(vmem_limit_bytes=40 * 1024 * 1024),
    )(side, w_value_up)
    pieces, value_up, side = lax.optimization_barrier((pieces, value_up, side))
    new_latent, fresh_slice, latent_piece = pl.pallas_call(
        fresh_kernel,
        out_shape=(sds((seqs, rank), BF16), sds((seqs, LANES), F32), sds((4, seqs), BF16)),
        in_specs=whole(2),
        out_specs=tuple(whole(3)),
        scratch_shapes=[pltpu.VMEM((seqs, rank), F32)],
        compiler_params=SMALL,
    )(side, latent_gain[None])
    pieces = [mine] + pieces
    pieces = pieces + [swapped(piece, "tp_1", 1) for piece in pieces]

    pairs_gap = seqs * (heads + 1)
    values, own_value = pl.pallas_call(
        functools.partial(attend_kernel, score_scale),
        out_shape=(sds((heads, 32, LANES), BF16), sds((seqs, LANES), F32)),
        in_specs=whole(14),
        out_specs=tuple(whole(2)),
        scratch_shapes=[
            pltpu.VMEM((rank // LANES, seqs, heads, LANES), BF16),
            pltpu.VMEM((pairs_gap * (rank // LANES), LANES), F32),
            pltpu.VMEM((pairs_gap, LANES), F32),
            pltpu.VMEM((pairs_gap, LANES), F32),
        ],
        compiler_params=pltpu.CompilerParams(vmem_limit_bytes=20 * 1024 * 1024),
    )(
        limits, *pieces, side, new_latent, cache_rotary.transpose(0, 2, 1), cache_latent, value_up
    )

    arrived = lax.all_to_all(values, KV, 0, 0, tiled=True)
    state = pl.pallas_call(
        gather_kernel,
        out_shape=sds((32, LANES), F32),
        in_specs=whole(3),
        out_specs=whole(1)[0],
        scratch_shapes=[pltpu.VMEM((kv_count, 16, LANES), F32)] * 2,
        compiler_params=SMALL,
    )(arrived, own_slice, fresh_slice)
    state = pl.pallas_call(
        pair_kernel,
        out_shape=sds((32, LANES), F32),
        in_specs=whole(2),
        out_specs=whole(1)[0],
        compiler_params=SMALL,
    )(state, swapped(state, "tp_1", 1))
    states = [state] + [swapped(state, "tp_0", j) for j in (1, 2, 3)]
    block_shape = (seqs * out_cols // LANES, LANES)
    term = pl.pallas_call(
        functools.partial(finish_kernel, score_scale),
        out_shape=sds(block_shape, BF16),
        in_specs=whole(7),
        out_specs=whole(1)[0],
        compiler_params=SMALL,
    )(*states, rope_dot, own_value, w_out)
    terms = pl.pallas_call(
        ring_kernel,
        out_shape=sds((lax.axis_size("kv_0"), *block_shape), BF16),
        in_specs=whole(4),
        out_specs=whole(1)[0],
        compiler_params=SMALL,
    )(term, *[swapped(term, "kv_1", j) for j in (1, 2, 3)])
    terms = lax.all_to_all(terms, "kv_0", 0, 0, tiled=True)
    mixed_out = pl.pallas_call(
        total_kernel,
        out_shape=sds((seqs, out_cols), BF16),
        in_specs=whole(1),
        out_specs=whole(1)[0],
        compiler_params=SMALL,
    )(terms)
    return (mixed_out, latent_piece.T, new_rotary)


def solution(mesh):
    torus = Mesh(mesh.devices.reshape(8, 4, 4, 2), KV_TP)
    in_specs = (
        P(None, TP),
        P(TP),
        P(TP, KV, None),
        P(TP, KV),
        P(TP, None),
        P(),
        P(TP, KV, None),
        P(),
        P(KV, TP),
        P(None, KV_TP, None),
        P(None, KV_TP, None),
        P(),
    )
    out_specs = (P(None, TP), P(None, KV_TP), P())
    return jax.shard_map(
        shards, mesh=torus, in_specs=in_specs, out_specs=out_specs, check_vma=False
    )
```
